512 devices in a mesh: grp: 2 (over y), sp: 32 (over z), tp: 8 (over x, core).
Axes of the slice: x: 4, y: 2, z: 32, core: 2. Of those that a mesh axis runs over, the one named last changes fastest.
The devices are a block of a 4x8x32 slice.
Arguments:
- latent: bfloat16 [32768, 4096], P(('grp', 'sp', 'tp')), parts along dimension 0, may hold values from -260 to 260
- context: bfloat16 [1536, 4096], P(('grp', 'sp')), parts along dimension 0, may hold values from -6 to 6
- conditioning: bfloat16 [8192], P(('grp', 'sp')), parts along dimension 0, may hold values from -6 to 6
- norm_gain: float32 [4096], replicated, may hold values from 0.1 to 1.9
- shift_weight: bfloat16 [4096, 4096], P('sp', 'tp'), may hold values from -0.09375 to 0.09375
- scale_weight: bfloat16 [4096, 4096], P('sp', 'tp'), may hold values from -0.09375 to 0.09375
- gate_weight: bfloat16 [4096, 4096], P('sp', 'tp'), may hold values from -0.09375 to 0.09375
- query_weight: bfloat16 [4096, 1024], P(None, 'tp'), may hold values from -3 to 3
- key_weight: bfloat16 [4096, 512], P(None, 'tp'), may hold values from -3 to 3
- value_weight: bfloat16 [4096, 512], P(None, 'tp'), may hold values from -0.09375 to 0.09375
- out_weight: bfloat16 [1024, 4096], P(None, 'tp'), may hold values from -1.5 to 1.5
- sink_logit: float32 [16], P('tp'), may hold values from 3 to 7
Outputs:
- mixed: bfloat16 [32768, 4096], P(('grp', 'sp', 'tp')), parts along dimension 0
The draws below stay inside these ranges and needn't reach their ends.
There are 2 independent parts, one for each index of `grp`. The reference program is written for one: setup_inputs(seed, part) draws one part's arguments, and reference() takes and returns one part's arrays. A program takes and returns all parts, laid end to end along the dimension named above; an argument that names none is the same for every part. Nothing has to cross between parts.
All inputs are finite; a program needn't handle non-finite values.
Results may differ from the reference program's by a relative error of at most 0.012.
The reference program's roundings to bfloat16 on the way count: a program that leaves them out, or rounds other values in their place, can miss the bound.
Values may be sent and summed in bfloat16 or wider, within the bound.
A program may use at most 64 MiB of HBM per device.

```python
import math
import jax
import jax.numpy as jnp
from jax import lax

D = 4096
HEADS = 16
KV_HEADS = 8
HD = 64
GRID_W = 64
WIN = 128
CTX = 768
SEQ = 16384


def paired_projections(seed_key):
    query_rows = jax.random.truncated_normal(jax.random.fold_in(seed_key, 11), -4.0, 4.0, (D, HEADS * HD), jnp.float32) / math.sqrt(D)
    key_rows = jax.random.truncated_normal(jax.random.fold_in(seed_key, 12), -4.0, 4.0, (D, KV_HEADS * HD), jnp.float32) / math.sqrt(D)
    return (query_rows, key_rows)


def draw_query_weight(key, part):
    return paired_projections(key)[0].astype(jnp.bfloat16)


def draw_key_weight(key, part):
    return paired_projections(key)[1].astype(jnp.bfloat16)


def draw_latent(key, part):
    values_drawn = jax.random.truncated_normal(jax.random.fold_in(key, 1), -6.0, 6.0, (SEQ, D), jnp.float32)
    return values_drawn.astype(jnp.bfloat16)


def block_scale(rng, extent, cuts, least, high):
    factor_of, own = 1.0, jax.random.fold_in(rng, 6)
    for dim, blocks in cuts:
        draws = jnp.exp(jax.random.uniform(jax.random.fold_in(own, dim), (blocks,), jnp.float32, least / len(cuts), high / len(cuts)))
        factor_of = factor_of * jnp.repeat(draws, extent[dim] // blocks).reshape([-1 if axis == dim else 1 for axis in range(len(extent))])
    return factor_of


def scatter_about(stream_key, dims, width, most, shards=(), kind=jnp.bfloat16):
    level = block_scale(stream_key, dims, shards, -0.22, 0.18) if shards else 1.0
    values = jax.random.normal(stream_key, dims, jnp.float32) * width * level
    return jnp.minimum(jnp.maximum(values, -most), most).astype(kind)


def setup_inputs(seed: int = 0, part: int = 0) -> dict:
    splits = jax.random.split(jax.random.key(seed), 13)
    own_keys = jax.random.split(jax.random.fold_in(splits[12], part), 13)
    return {
        "latent": draw_latent(jax.random.fold_in(jax.random.fold_in(splits[12], part), 71), part),
        "context": scatter_about(own_keys[1], (CTX, D), 1.0, 6.0, ((0, 32),)),
        "conditioning": scatter_about(own_keys[2], (D,), 1.5, 6.0, ((0, 32),)),
        "norm_gain": jnp.clip(1.0 + 0.18 * jax.random.normal(splits[3], (D,), jnp.float32), 0.1, 1.9),
        "shift_weight": scatter_about(splits[4], (D, D), D ** -0.5, 0.09375, ((0, 32), (1, 8))),
        "scale_weight": scatter_about(splits[5], (D, D), D ** -0.5, 0.09375, ((0, 32), (1, 8))),
        "gate_weight": scatter_about(splits[6], (D, D), D ** -0.5, 0.09375, ((0, 32), (1, 8))),
        "query_weight": draw_query_weight(jax.random.fold_in(splits[12], 71), part),
        "key_weight": draw_key_weight(jax.random.fold_in(splits[12], 71), part),
        "value_weight": scatter_about(splits[9], (D, KV_HEADS * HD), D ** -0.5, 0.09375, ((1, 8),)),
        "out_weight": scatter_about(splits[10], (HEADS * HD, D), (HD // 4) ** -0.5, 1.5, ((1, 8),)),
        "sink_logit": jnp.clip(3.0 + 4.0 * jax.random.uniform(splits[11], (HEADS,), jnp.float32) ** block_scale(splits[11], (HEADS,), ((0, 8),), -0.2, 0.2), 3.0, 7.0),
    }


epsilon = 1e-06
rope_base = 10000.0
neg_large = -1e+30

def row_norm(matrix, norm_gain):
    values = matrix.astype(jnp.float32)
    return values * lax.rsqrt(lax.optimization_barrier(jnp.mean(values * values, axis=-1, keepdims=True)) + epsilon) * norm_gain

def axial_turn(values, position):
    half_dim = values.shape[-1] // 2
    quarter = half_dim // 2
    inverse = rope_base ** (-jnp.arange(quarter, dtype=jnp.float32) / quarter)

    def turn(section, coordinate):
        angles = coordinate.astype(jnp.float32)[:, None] * inverse[None, :]
        cosine = jnp.cos(angles)[:, None, :]
        sine_part = jnp.sin(angles)[:, None, :]
        leading = section[..., :quarter]
        trailing = section[..., quarter:]
        return jnp.concatenate([leading * cosine - trailing * sine_part, leading * sine_part + trailing * cosine], axis=-1)
    return jnp.concatenate([turn(values[..., :half_dim], position // GRID_W), turn(values[..., half_dim:], position % GRID_W)], axis=-1)

def reference(latent, context, conditioning, norm_gain, shift_weight, scale_weight, gate_weight, query_weight, key_weight, value_weight, out_weight, sink_logit):
    lifted = jax.nn.silu(conditioning.astype(jnp.float32)).astype(jnp.bfloat16)[None, :]
    shift_vec = jnp.dot(lifted, shift_weight, preferred_element_type=jnp.float32)[0]
    scale_vec = jnp.dot(lifted, scale_weight, preferred_element_type=jnp.float32)[0]
    gate_vec = jnp.dot(lifted, gate_weight, preferred_element_type=jnp.float32)[0]
    normed = (row_norm(latent, norm_gain) * (1.0 + scale_vec) + shift_vec).astype(jnp.bfloat16)
    position = jnp.arange(SEQ, dtype=jnp.int32)
    queries = axial_turn(jnp.dot(normed, query_weight, preferred_element_type=jnp.float32).reshape(SEQ, HEADS, HD), position).astype(jnp.bfloat16)
    latent_keys = axial_turn(jnp.dot(normed, key_weight, preferred_element_type=jnp.float32).reshape(SEQ, KV_HEADS, HD), position).astype(jnp.bfloat16)
    latent_values = jnp.dot(normed, value_weight, preferred_element_type=jnp.float32).astype(jnp.bfloat16).reshape(SEQ, KV_HEADS, HD)
    prepared = row_norm(context, norm_gain).astype(jnp.bfloat16)
    context_keys = jnp.dot(prepared, key_weight, preferred_element_type=jnp.float32).astype(jnp.bfloat16).reshape(CTX, KV_HEADS, HD).astype(jnp.float32)
    context_values = jnp.dot(prepared, value_weight, preferred_element_type=jnp.float32).astype(jnp.bfloat16).reshape(CTX, KV_HEADS, HD).astype(jnp.float32)
    group_size = HEADS // KV_HEADS
    factor = HD ** (-0.5)
    padded_keys = jnp.pad(latent_keys, ((WIN, WIN), (0, 0), (0, 0)))
    padded_values = jnp.pad(latent_values, ((WIN, WIN), (0, 0), (0, 0)))
    sink_values = sink_logit.astype(jnp.float32).reshape(KV_HEADS, group_size)[:, :, None, None]

    def one_block(block_index):
        first_row = block_index * WIN
        block_queries = lax.dynamic_slice_in_dim(queries, first_row, WIN, 0).reshape(WIN, KV_HEADS, group_size, HD).astype(jnp.float32)
        block_keys = lax.dynamic_slice_in_dim(padded_keys, first_row, 3 * WIN, 0).astype(jnp.float32)
        block_values = lax.dynamic_slice_in_dim(padded_values, first_row, 3 * WIN, 0).astype(jnp.float32)
        local_scores = jnp.einsum('qhgd,khd->hgqk', block_queries, block_keys) * factor
        query_pos = first_row + jnp.arange(WIN, dtype=jnp.int32)
        key_pos = first_row - WIN + jnp.arange(3 * WIN, dtype=jnp.int32)
        allowed = (jnp.abs(key_pos[None, :] - query_pos[:, None]) <= WIN) & (key_pos[None, :] >= 0) & (key_pos[None, :] < SEQ)
        local_scores = jnp.where(allowed, local_scores, neg_large)
        context_scores = jnp.einsum('qhgd,thd->hgqt', block_queries, context_keys) * factor
        joined = jnp.concatenate([local_scores, context_scores, jnp.broadcast_to(sink_values, local_scores.shape[:-1] + (1,))], axis=-1)
        highest = lax.optimization_barrier(jnp.max(joined, axis=-1, keepdims=True))
        exponent = jnp.exp(joined - highest)
        weights = (exponent / lax.optimization_barrier(jnp.sum(exponent, axis=-1, keepdims=True))).astype(jnp.bfloat16)
        weights = lax.optimization_barrier(weights).astype(jnp.float32)
        out_block = jnp.einsum('hgqk,khd->qhgd', weights[..., :3 * WIN], block_values) + jnp.einsum('hgqt,thd->qhgd', weights[..., 3 * WIN:3 * WIN + CTX], context_values)
        return out_block.reshape(WIN, HEADS * HD).astype(jnp.bfloat16)
    attended = lax.map(one_block, jnp.arange(SEQ // WIN, dtype=jnp.int32)).reshape(SEQ, HEADS * HD)
    blended = jnp.dot(attended, out_weight, preferred_element_type=jnp.float32).astype(jnp.bfloat16)
    blended = lax.optimization_barrier(blended).astype(jnp.float32)
    return (latent.astype(jnp.float32) + gate_vec * blended).astype(jnp.bfloat16)
```

```python
import functools

import jax
import jax.numpy as jnp
import numpy as np
from jax import lax
from jax.experimental import pallas as pl
from jax.experimental.pallas import tpu as pltpu
from jax.sharding import PartitionSpec as P

HEADS = 16
KV_HEADS = 8
HD = 64
GRID_W = 64
WIN = 128
REACH = 4
LANES = 128
COLS = 512

epsilon = 1e-06
rope_base = 10000.0
neg_large = -1e30
MESH = pl.DeviceIdType.MESH
f32 = jnp.float32
bf16 = jnp.bfloat16


def rope_tables(grid_rows):
    lane = np.arange(LANES)
    d = lane % HD
    freq = rope_base ** (-(d % 16) / 16.0)
    is_row = d < HD // 2
    sign = np.where(d % 32 < 16, -1.0, 1.0)
    is_key = lane < HD

    def table(count, own):
        angle = np.arange(count)[:, None] * freq[None, :]
        c = np.where(own, np.cos(angle), 0.0)
        s = np.where(own, np.sin(angle) * sign, 0.0)
        scale = HD**-0.5
        ck = np.where(is_key, c, 0.0)
        sk = np.where(is_key, s, 0.0)
        return np.concatenate([c * scale, s * scale, ck, sk], axis=1)

    rows = table(grid_rows, is_row)
    cols = table(GRID_W, ~is_row)
    cols[:, 2 * LANES : 3 * LANES] += np.where(is_key, 0.0, 1.0)
    return rows.astype(np.float32), cols.astype(np.float32)


def kernel(
    n_sp,
    n_tp,
    latent,
    context,
    cond,
    gain,
    shift_w,
    scale_w,
    gate_w,
    q_w,
    k_w,
    v_w,
    o_w,
    sink,
    row_tab,
    col_tab,
    out,
    rows,
    w,
    kw,
    vw,
    ow,
    mw,
    ctx_rows,
    cg,
    mpart,
    chain_l,
    chain_r,
    mtot,
    inv,
    a_vec,
    s_vec,
    g_vec,
    qrot,
    kv,
    ctx,
    att,
    ysend,
    yrecv,
    rt,
    ct,
    load_sem,
    m_send,
    m_recv,
    c_send,
    c_recv,
    x_send,
    x_recv,
    ag_send,
    ag_recv,
    fw_send,
    sib_send,
    sib_recv,
    h_send,
    h_recv,
    t_send,
    t_recv,
    tf_send,
    tsib_send,
    tsib_recv,
    y_send,
    y_recv,
):
    n_x = n_tp // 2
    z = lax.axis_index("sp")
    t = lax.axis_index("tp")
    x = t // 2
    c = t % 2
    xr = (x + 1) % n_x
    xl = (x + n_x - 1) % n_x
    xo = (x + 2) % n_x
    sib = x * 2 + (1 - c)
    t_r, t_l, t_o = xr * 2 + c, xl * 2 + c, xo * 2 + c
    fw_src = ((x + n_x - 1 + 2 * c) % n_x) * 2 + c
    fw_dst = ((x + 1 + n_x - 2 * c) % n_x) * 2 + c
    group = latent.shape[0]
    count = n_tp * group
    depth = latent.shape[1]
    chunks = group // 16
    width = shift_w.shape[1]
    per = width // LANES

    def up(k):
        return {"sp": (z + k) % n_sp}

    def down(k):
        return {"sp": (z + n_sp - k) % n_sp}

    def other(k):
        return {"tp": (t + k) % n_tp}

    started = []

    def send(src, dst, ss, rs, dev):
        copy = pltpu.make_async_remote_copy(
            src_ref=src, dst_ref=dst, send_sem=ss, recv_sem=rs, device_id=dev, device_id_type=MESH
        )
        copy.start()
        started.append(copy)

    def recv(dst, rs, dev):
        pltpu.make_async_remote_copy(
            src_ref=dst, dst_ref=dst, send_sem=rs, recv_sem=rs, device_id=dev, device_id_type=MESH
        ).wait_recv()

    barrier = pltpu.get_barrier_semaphore()
    for k in range(1, n_tp):
        pl.semaphore_signal(barrier, inc=1, device_id=other(k), device_id_type=MESH)
    for k in range(1, REACH + 1):
        pl.semaphore_signal(barrier, inc=1, device_id=up(k), device_id_type=MESH)
        pl.semaphore_signal(barrier, inc=1, device_id=down(k), device_id_type=MESH)

    grid_rows = count // GRID_W
    loads = {}

    def load(name, src, dst):
        copy = pltpu.make_async_copy(src, dst, load_sem.at[len(loads)])
        copy.start()
        loads[name] = copy

    load("m0", shift_w, mw.at[0])
    load("m1", scale_w, mw.at[1])
    load("m2", gate_w, mw.at[2])
    load("rows", latent, rows.at[t])
    load("kw", k_w, kw)
    load("vw", v_w, vw)
    load("ctx", context, ctx_rows)
    load("qw", q_w, w.at[:, pl.ds(0, LANES)])
    load("rt", row_tab.at[pl.ds(pl.multiple_of(z * grid_rows, 8), grid_rows)], rt)
    load("ct", col_tab, ct)
    load("ow", o_w, ow)

    cv = cond[...].astype(f32)
    lifted = jnp.broadcast_to((cv / (1.0 + jnp.exp(-cv))).astype(bf16), (16, cv.shape[1]))
    for i in range(3):
        loads["m%d" % i].wait()
        part = jnp.dot(lifted, mw[i], preferred_element_type=f32)
        for j in range(per):
            mpart[0, per * i + j : per * i + j + 1, :] = part[0:1, j * LANES : (j + 1) * LANES]
    mpart[0, 3 * per : 16, :] = jnp.zeros((16 - 3 * per, LANES), f32)

    loads["kw"].wait()
    loads["vw"].wait()
    for i in range(depth // COLS):
        part = pl.ds(i * COLS, COLS)
        w[part, LANES : 2 * LANES] = jnp.concatenate([kw[part, :], vw[part, :]], axis=1)
    loads["ctx"].wait()
    n_ctx = ctx_rows.shape[0]
    sq = jnp.zeros((n_ctx, LANES), f32)
    for i in range(depth // LANES):
        v = ctx_rows[:, i * LANES : (i + 1) * LANES].astype(f32)
        sq = sq + v * v
    cinv = lax.rsqrt(jnp.sum(sq, axis=1, keepdims=True) * (1.0 / depth) + epsilon)
    acc = jnp.zeros((n_ctx, LANES), f32)
    for i in range(depth // COLS):
        part = slice(i * COLS, (i + 1) * COLS)
        v = ctx_rows[:, part].astype(f32) * cinv * gain[:, part]
        acc = acc + jnp.dot(v.astype(bf16), w[part, LANES : 2 * LANES], preferred_element_type=f32)
    cg[0] = acc.astype(bf16)

    loads["rows"].wait()
    pl.semaphore_wait(barrier, n_tp - 1 + 2 * REACH)
    for k in range(1, REACH + 1):
        if k < REACH:
            send(mpart.at[0], mpart.at[k], m_send.at[k - 1], m_recv.at[k - 1], up(k))
        send(mpart.at[0], mpart.at[3 + k], m_send.at[2 + k], m_recv.at[2 + k], down(k))
    for q in range(chunks):
        piece = rows.at[t, pl.ds(16 * q, 16)]
        send(piece, piece, ag_send.at[0, q], ag_recv.at[0, q], {"tp": t_r})
        send(piece, piece, ag_send.at[1, q], ag_recv.at[1, q], {"tp": t_l})
    for q in range(chunks):
        piece = rows.at[t, pl.ds(16 * q, 16)]
        send(piece, piece, sib_send.at[0, q], sib_recv.at[0, q], {"tp": sib})
    half = n_sp // 2
    for k in range(1, REACH + 1):
        if k < REACH:
            send(cg.at[0], cg.at[k], c_send.at[k - 1], c_recv.at[k - 1], up(k))
        send(cg.at[0], cg.at[half + k - 1], c_send.at[2 + k], c_recv.at[2 + k], down(k))

    def row_stats(g):
        sq = jnp.zeros((group, LANES), f32)
        for i in range(depth // LANES):
            v = rows[g, :, i * LANES : (i + 1) * LANES].astype(f32)
            sq = sq + v * v
        r = lax.rsqrt(jnp.sum(sq, axis=1, keepdims=True) * (1.0 / depth) + epsilon)
        inv[g] = jnp.broadcast_to(r, (group, LANES))

    def chunk_step(q, relay):
        piece_l = rows.at[t_l, pl.ds(16 * q, 16)]
        piece_r = rows.at[t_r, pl.ds(16 * q, 16)]
        recv(piece_l, ag_recv.at[0, q], {"tp": t_l})
        recv(piece_r, ag_recv.at[1, q], {"tp": t_r})
        if relay:
            chunk_relay(q)
        send(piece_l, piece_l, sib_send.at[1, q], sib_recv.at[1, q], {"tp": sib})
        send(piece_r, piece_r, sib_send.at[2, q], sib_recv.at[2, q], {"tp": sib})

    def chunk_relay(q):
        piece = rows.at[fw_src, pl.ds(16 * q, 16)]
        send(piece, piece, fw_send.at[q], ag_recv.at[2, q], {"tp": fw_dst})

    stages = half // REACH

    def mod_step(s):
        if s == 0:
            for k in range(1, REACH + 1):
                if k < REACH:
                    recv(mpart.at[k], m_recv.at[k - 1], down(k))
                recv(mpart.at[3 + k], m_recv.at[2 + k], up(k))
            chain_l[0] = (mpart[0] + mpart[1]) + (mpart[2] + mpart[3])
            chain_r[0] = (mpart[4] + mpart[5]) + (mpart[6] + mpart[7])
        else:
            recv(chain_l.at[s], m_recv.at[5 + 2 * s], down(REACH))
            recv(chain_r.at[s], m_recv.at[6 + 2 * s], up(REACH))
        if s + 1 < stages:
            send(chain_l.at[s], chain_l.at[s + 1], m_send.at[7 + 2 * s], m_recv.at[7 + 2 * s], up(REACH))
            send(chain_r.at[s], chain_r.at[s + 1], m_send.at[8 + 2 * s], m_recv.at[8 + 2 * s], down(REACH))

    def ctx_step(s):
        if s == 0:
            for k in range(1, REACH + 1):
                if k < REACH:
                    recv(cg.at[k], c_recv.at[k - 1], down(k))
                recv(cg.at[half + k - 1], c_recv.at[2 + k], up(k))
        else:
            recv(cg.at[pl.ds(REACH * s, REACH)], c_recv.at[5 + 2 * s], down(REACH))
            recv(cg.at[pl.ds(half + REACH * s, REACH)], c_recv.at[6 + 2 * s], up(REACH))
        if s + 1 < stages:
            for base, j, dev in ((0, 7, up(REACH)), (half, 8, down(REACH))):
                send(
                    cg.at[pl.ds(base + REACH * s, REACH)],
                    cg.at[pl.ds(base + REACH * (s + 1), REACH)],
                    c_send.at[j + 2 * s],
                    c_recv.at[j + 2 * s],
                    dev,
                )

    row_stats(t)
    mod_step(0)
    chunk_step(0, True)
    ctx_step(0)
    chunk_step(1, True)
    mod_step(1)
    ctx_step(1)
    chunk_step(2, True)
    mod_step(2)
    ctx_step(2)
    chunk_step(3, False)
    row_stats(t_l)
    row_stats(t_r)
    mod_step(3)

    mtot[t] = ((chain_l[0] + chain_l[1]) + (chain_l[2] + chain_l[3])) + (
        (chain_r[0] + chain_r[1]) + (chain_r[2] + chain_r[3])
    )
    for k in range(1, n_tp):
        send(mtot.at[t], mtot.at[t], x_send.at[k - 1], x_recv.at[k - 1], other(k))
    chunk_relay(3)
    ctx_step(3)
    for j in range(n_sp):
        ctx[pl.ds(j * n_ctx, n_ctx), :] = cg[j]

    for name in ("rt", "ct", "qw", "ow"):
        loads[name].wait()
    for q in range(chunks):
        for role, src in ((0, sib), (1, xl * 2 + 1 - c), (2, xr * 2 + 1 - c)):
            recv(rows.at[src, pl.ds(16 * q, 16)], sib_recv.at[role, q], {"tp": sib})
    row_stats(sib)
    row_stats(xl * 2 + 1 - c)
    row_stats(xr * 2 + 1 - c)
    for q in range(chunks):
        piece = rows.at[t_o, pl.ds(16 * q, 16)]
        recv(piece, ag_recv.at[2, q], {"tp": t_o})
        send(piece, piece, sib_send.at[3, q], sib_recv.at[3, q], {"tp": sib})
    row_stats(t_o)
    for k in range(1, n_tp):
        src = (t + n_tp - k) % n_tp
        recv(mtot.at[src], x_recv.at[k - 1], {"tp": src})
    for j in range(n_tp):
        for i in range(per):
            part = slice(j * width + i * LANES, j * width + (i + 1) * LANES)
            s_vec[:, part] = mtot[j, i : i + 1, :]
            a_vec[:, part] = gain[:, part] * (1.0 + mtot[j, per + i : per + i + 1, :])
            g_vec[:, part] = mtot[j, 2 * per + i : 2 * per + i + 1, :]
    for q in range(chunks):
        src = xo * 2 + 1 - c
        recv(rows.at[src, pl.ds(16 * q, 16)], sib_recv.at[3, q], {"tp": sib})
    row_stats(xo * 2 + 1 - c)

    lane = lax.broadcasted_iota(jnp.int32, (1, LANES), 1)
    first = lane % 32 < 16

    def swapped(v):
        return jnp.where(first, pltpu.roll(v, LANES - 16, 1), pltpu.roll(v, 16, 1))

    def project(gs):
        acc = jnp.zeros((len(gs) * group, 2 * LANES), f32)
        for i in range(depth // COLS):
            part = slice(i * COLS, (i + 1) * COLS)
            a = a_vec[:, part]
            s = s_vec[:, part]
            tiles = []
            for g in gs:
                r = jnp.concatenate([inv[g]] * (COLS // LANES), axis=1)
                tiles.append((rows[g, :, part].astype(f32) * r * a + s).astype(bf16))
            acc = acc + jnp.dot(jnp.concatenate(tiles, axis=0), w[part, :], preferred_element_type=f32)
        for n, g in enumerate(gs):
            fac = rt[g : g + 1, :] + ct[...]
            vq = acc[n * group : (n + 1) * group, :LANES]
            vk = acc[n * group : (n + 1) * group, LANES:]
            q2 = vq * fac[:, :LANES] + swapped(vq) * fac[:, LANES : 2 * LANES]
            k2 = vk * fac[:, 2 * LANES : 3 * LANES] + swapped(vk) * fac[:, 3 * LANES :]
            qrot[g * group : (g + 1) * group, :] = q2.astype(bf16)
            kv[WIN + g * group : WIN + (g + 1) * group, :] = k2.astype(bf16)

    project((0, 1, n_tp - 2, n_tp - 1))
    send(kv.at[pl.ds(WIN, WIN)], kv.at[pl.ds(WIN + count, WIN)], h_send.at[0], h_recv.at[0], down(1))
    send(kv.at[pl.ds(count, WIN)], kv.at[pl.ds(0, WIN)], h_send.at[1], h_recv.at[1], up(1))
    project(tuple(range(2, n_tp - 2)))

    rows2 = 2 * WIN
    qi = lax.broadcasted_iota(jnp.int32, (rows2, WIN), 0) % WIN
    ki = lax.broadcasted_iota(jnp.int32, (rows2, WIN), 1)
    head1 = lax.broadcasted_iota(jnp.int32, (rows2, 1), 0) >= WIN
    sink_col = jnp.where(head1, sink[1], sink[0])
    is_key = lane < HD
    contract = (((1,), (1,)), ((), ()))
    blocks = count // WIN

    def attend(b):
        qb = qrot[b * WIN : (b + 1) * WIN, :].astype(f32)
        q0 = jnp.where(is_key, qb, 0.0).astype(bf16)
        q1 = jnp.where(is_key, pltpu.roll(qb, HD, 1), 0.0).astype(bf16)
        qq = jnp.concatenate([q0, q1], axis=0)
        band = kv[b * WIN : (b + 3) * WIN, :]
        whole = ctx[...]
        s_band = lax.dot_general(qq, band, contract, preferred_element_type=f32)
        s_ctx = lax.dot_general(qq, whole, contract, preferred_element_type=f32)
        left = ki >= qi
        right = ki <= qi
        if b == 0:
            left = left & (z > 0)
        if b == blocks - 1:
            right = right & (z < n_sp - 1)
        s0 = jnp.where(left, s_band[:, :WIN], neg_large)
        s1 = s_band[:, WIN : 2 * WIN]
        s2 = jnp.where(right, s_band[:, 2 * WIN :], neg_large)
        top = jnp.maximum(jnp.maximum(s0, s1), s2)
        for i in range(whole.shape[0] // LANES):
            top = jnp.maximum(top, s_ctx[:, i * LANES : (i + 1) * LANES])
        m = jnp.maximum(jnp.max(top, axis=1, keepdims=True), sink_col)
        e0 = jnp.exp(s0 - m)
        e1 = jnp.exp(s1 - m)
        e2 = jnp.exp(s2 - m)
        ec = jnp.exp(s_ctx - m)
        tot = e0 + e1 + e2
        for i in range(whole.shape[0] // LANES):
            tot = tot + ec[:, i * LANES : (i + 1) * LANES]
        den = jnp.sum(tot, axis=1, keepdims=True) + jnp.exp(sink_col - m)
        r = 1.0 / den
        p_band = jnp.concatenate([e0, e1, e2], axis=1) * r
        o = jnp.dot(p_band.astype(bf16), band, preferred_element_type=f32) + jnp.dot(
            (ec * r).astype(bf16), whole, preferred_element_type=f32
        )
        res = jnp.where(is_key, pltpu.roll(o[:WIN], HD, 1), o[WIN:]).astype(bf16)
        att[t, b * WIN : (b + 1) * WIN, :] = res

    def att_piece(who, b):
        return att.at[who, pl.ds(b * WIN, WIN)]

    def att_send(b):
        piece = att_piece(t, b)
        send(piece, piece, t_send.at[0, b], t_recv.at[0, b], {"tp": t_r})
        send(piece, piece, t_send.at[1, b], t_recv.at[1, b], {"tp": t_l})
        send(piece, piece, tsib_send.at[0, b], tsib_recv.at[0, b], {"tp": sib})

    def att_near(b):
        piece_l, piece_r = att_piece(t_l, b), att_piece(t_r, b)
        recv(piece_l, t_recv.at[0, b], {"tp": t_l})
        recv(piece_r, t_recv.at[1, b], {"tp": t_r})
        piece = att_piece(fw_src, b)
        send(piece, piece, tf_send.at[b], t_recv.at[2, b], {"tp": fw_dst})
        send(piece_l, piece_l, tsib_send.at[1, b], tsib_recv.at[1, b], {"tp": sib})
        send(piece_r, piece_r, tsib_send.at[2, b], tsib_recv.at[2, b], {"tp": sib})

    def att_far(b):
        piece = att_piece(t_o, b)
        recv(piece, t_recv.at[2, b], {"tp": t_o})
        send(piece, piece, tsib_send.at[3, b], tsib_recv.at[3, b], {"tp": sib})

    order = [*range(1, blocks - 1), 0, blocks - 1]
    for n, b in enumerate(order):
        if n == blocks - 2:
            recv(kv.at[pl.ds(WIN + count, WIN)], h_recv.at[0], up(1))
            recv(kv.at[pl.ds(0, WIN)], h_recv.at[1], down(1))
        attend(b)
        att_send(b)
        if n >= 1:
            att_near(order[n - 1])
        if n >= 2:
            att_far(order[n - 2])
    att_near(order[-1])
    att_far(order[-2])
    att_far(order[-1])
    for b in order:
        for role, xx in ((0, x), (1, xl), (2, xr), (3, xo)):
            recv(att_piece(xx * 2 + 1 - c, b), tsib_recv.at[role, b], {"tp": sib})

    here = pl.ds(pl.multiple_of(t * width, LANES), width)
    for n, xx in enumerate((xo, xr, xl, x)):
        part = pl.ds(pl.multiple_of(xx * WIN, WIN), WIN)
        y = jnp.zeros((WIN, width), f32)
        for i in range(n_x):
            lhs = jnp.concatenate([att[2 * i, part, :], att[2 * i + 1, part, :]], axis=1)
            y = y + jnp.dot(lhs, ow[2 * i * LANES : 2 * (i + 1) * LANES, :], preferred_element_type=f32)
        ysend[2 * n] = y[:group].astype(bf16)
        ysend[2 * n + 1] = y[group:].astype(bf16)
        if n < 3:
            for k in range(2):
                send(ysend.at[2 * n + k], yrecv.at[:, here], y_send.at[2 * n + k], y_recv.at[2 * n + c], {"tp": xx * 2 + k})
        else:
            send(ysend.at[2 * n + 1 - c], yrecv.at[:, here], y_send.at[6], y_recv.at[6], {"tp": sib})
            yrecv[:, here] = ysend[2 * n + c]
    for n, xx in enumerate((xo, xl, xr)):
        for k in range(2):
            cols = pl.ds(pl.multiple_of((xx * 2 + k) * width, LANES), width)
            recv(yrecv.at[:, cols], y_recv.at[2 * n + k], {"tp": xx * 2 + k})
    recv(yrecv.at[:, pl.ds(pl.multiple_of(sib * width, LANES), width)], y_recv.at[6], {"tp": sib})
    for i in range(depth // COLS):
        part = slice(i * COLS, (i + 1) * COLS)
        out[:, part] = (
            rows[t, :, part].astype(f32) + g_vec[:, part] * yrecv[:, part].astype(f32)
        ).astype(bf16)
    for copy in started:
        copy.wait_send()


def local(n_sp, n_tp, latent, context, conditioning, norm_gain, *rest):
    shift_w, scale_w, gate_w, q_w, k_w, v_w, o_w, sink = rest
    group, depth = latent.shape
    n_ctx = context.shape[0]
    count = n_tp * group
    width = shift_w.shape[1]
    blocks = count // WIN
    chunks = group // 16
    row_tab, col_tab = rope_tables(n_sp * count // GRID_W)
    any_space = pl.BlockSpec(memory_space=pl.ANY)
    vmem = pl.BlockSpec(memory_space=pltpu.VMEM)
    dma = pltpu.SemaphoreType.DMA
    return pl.pallas_call(
        functools.partial(kernel, n_sp, n_tp),
        out_shape=jax.ShapeDtypeStruct((group, depth), bf16),
        in_specs=[any_space, any_space, vmem, vmem]
        + [any_space] * 7
        + [pl.BlockSpec(memory_space=pltpu.SMEM), any_space, any_space],
        out_specs=vmem,
        scratch_shapes=[
            pltpu.VMEM((n_tp, group, depth), bf16),
            pltpu.VMEM((depth, 2 * LANES), bf16),
            pltpu.VMEM(k_w.shape, bf16),
            pltpu.VMEM(v_w.shape, bf16),
            pltpu.VMEM(o_w.shape, bf16),
            pltpu.VMEM((3, *shift_w.shape), bf16),
            pltpu.VMEM((n_ctx, depth), bf16),
            pltpu.VMEM((n_sp, n_ctx, LANES), bf16),
            pltpu.VMEM((2 * REACH, 16, LANES), f32),
            pltpu.VMEM((n_sp // 2 // REACH, 16, LANES), f32),
            pltpu.VMEM((n_sp // 2 // REACH, 16, LANES), f32),
            pltpu.VMEM((n_tp, 16, LANES), f32),
            pltpu.VMEM((n_tp, group, LANES), f32),
            pltpu.VMEM((1, depth), f32),
            pltpu.VMEM((1, depth), f32),
            pltpu.VMEM((1, depth), f32),
            pltpu.VMEM((count, LANES), bf16),
            pltpu.VMEM((count + 2 * WIN, LANES), bf16),
            pltpu.VMEM((n_sp * n_ctx, LANES), bf16),
            pltpu.VMEM((n_tp, count, LANES), bf16),
            pltpu.VMEM((n_tp, group, width), bf16),
            pltpu.VMEM((group, depth), bf16),
            pltpu.VMEM((count // GRID_W, 4 * LANES), f32),
            pltpu.VMEM((GRID_W, 4 * LANES), f32),
            dma((16,)),
            dma((16,)),
            dma((16,)),
            dma((16,)),
            dma((16,)),
            dma((n_tp,)),
            dma((n_tp,)),
            dma((2, chunks)),
            dma((3, chunks)),
            dma((chunks,)),
            dma((4, chunks)),
            dma((4, chunks)),
            dma((2,)),
            dma((2,)),
            dma((2, blocks)),
            dma((3, blocks)),
            dma((blocks,)),
            dma((4, blocks)),
            dma((4, blocks)),
            dma((8,)),
            dma((8,)),
        ],
        compiler_params=pltpu.CompilerParams(
            collective_id=0, has_side_effects=True, vmem_limit_bytes=56 * 1024 * 1024
        ),
    )(
        latent,
        context,
        conditioning.reshape(1, -1),
        norm_gain.reshape(1, -1),
        shift_w,
        scale_w,
        gate_w,
        q_w,
        k_w,
        v_w,
        o_w,
        sink,
        jnp.asarray(row_tab),
        jnp.asarray(col_tab),
    )


def solution(mesh):
    in_specs = (
        P(("grp", "sp", "tp"), None),
        P(("grp", "sp"), None),
        P(("grp", "sp")),
        P(),
        P("sp", "tp"),
        P("sp", "tp"),
        P("sp", "tp"),
        P(None, "tp"),
        P(None, "tp"),
        P(None, "tp"),
        P(None, "tp"),
        P("tp"),
    )
    return jax.shard_map(
        functools.partial(local, mesh.shape["sp"], mesh.shape["tp"]),
        mesh=mesh,
        in_specs=in_specs,
        out_specs=P(("grp", "sp", "tp"), None),
        check_vma=False,
    )
```

```python
import functools

import jax
import jax.numpy as jnp
import numpy as np
from jax import lax
from jax.experimental import pallas as pl
from jax.experimental.pallas import tpu as pltpu
from jax.sharding import PartitionSpec as P

HEADS = 16
KV_HEADS = 8
HD = 64
GRID_W = 64
WIN = 128
LANES = 128
COLS = 512

epsilon = 1e-06
rope_base = 10000.0
neg_large = -1e30
MESH = pl.DeviceIdType.MESH
f32 = jnp.float32
bf16 = jnp.bfloat16


def rope_tables(grid_rows):
    lane = np.arange(LANES)
    d = lane % HD
    freq = rope_base ** (-(d % 16) / 16.0)
    is_row = d < HD // 2
    sign = np.where(d % 32 < 16, -1.0, 1.0)
    is_key = lane < HD

    def table(count, own):
        angle = np.arange(count)[:, None] * freq[None, :]
        c = np.where(own, np.cos(angle), 0.0)
        s = np.where(own, np.sin(angle) * sign, 0.0)
        scale = HD**-0.5
        ck = np.where(is_key, c, 0.0)
        sk = np.where(is_key, s, 0.0)
        return np.concatenate([c * scale, s * scale, ck, sk], axis=1)

    rows = table(grid_rows, is_row)
    cols = table(GRID_W, ~is_row)
    cols[:, 2 * LANES : 3 * LANES] += np.where(is_key, 0.0, 1.0)
    return rows.astype(np.float32), cols.astype(np.float32)


def kernel(
    n_sp,
    n_tp,
    latent,
    context,
    cond_in,
    gain_in,
    shift_w,
    scale_w,
    gate_w,
    q_w,
    k_t,
    v_t,
    o_w,
    sink_in,
    row_tab,
    col_tab,
    out,
    rows,
    w,
    kvt,
    ow,
    mw,
    ctx_rows,
    cg,
    cown,
    mpair,
    mall,
    msum,
    mt,
    inv,
    a_vec,
    s_vec,
    g_vec,
    qrot,
    kv,
    ctx,
    att,
    ysend,
    yrecv,
    rt,
    ct,
    cond,
    gain,
    sink,
    hello,
    load_sem,
    pair_send,
    pair_recv,
    m_send,
    m_recv,
    tot_send,
    tot_recv,
    c_send,
    c_recv,
    ag_send,
    ag_recv,
    sib_send,
    sib_recv,
    x_send,
    x_recv,
    xs_send,
    xs_recv,
    h_send,
    h_recv,
    t_send,
    t_recv,
    tsib_send,
    tsib_recv,
    y_send,
    y_recv,
):
    n_x = n_tp // 2
    z = lax.axis_index("sp")
    t = lax.axis_index("tp")
    x = t // 2
    c = t % 2
    xr = (x + 1) % n_x
    xl = (x + n_x - 1) % n_x
    xo = (x + 2) % n_x
    sib = x * 2 + (1 - c)
    t_r, t_l, t_o = xr * 2 + c, xl * 2 + c, xo * 2 + c
    group = latent.shape[0]
    count = n_tp * group
    depth = latent.shape[1]
    chunks = group // 16
    width = shift_w.shape[1]
    per = width // LANES

    late = (z == 0) & (x == 0)
    center = 1

    started = []

    def send(src, dst, ss, rs, dev, keep=True):
        copy = pltpu.make_async_remote_copy(
            src_ref=src, dst_ref=dst, send_sem=ss, recv_sem=rs, device_id=dev, device_id_type=MESH
        )
        copy.start()
        if keep:
            started.append(copy)

    def recv(dst, rs, dev):
        pltpu.make_async_remote_copy(
            src_ref=dst, dst_ref=dst, send_sem=rs, recv_sem=rs, device_id=dev, device_id_type=MESH
        ).wait_recv()

    def sent(src, ss, dev):
        pltpu.make_async_remote_copy(
            src_ref=src, dst_ref=src, send_sem=ss, recv_sem=ss, device_id=dev, device_id_type=MESH
        ).wait_send()

    def each(lo, hi, body):
        def step(i, carry):
            body(i)
            return carry

        lax.fori_loop(lo, hi, step, 0)

    barrier = pltpu.get_barrier_semaphore()

    def greet(dev):
        pl.semaphore_signal(barrier, inc=1, device_id=dev, device_id_type=MESH)

    @pl.when(c == 1)
    def _():
        for who in (sib, t_r, t_l, t_o):
            greet({"tp": who})

    @pl.when(c == 0)
    def _():
        each(z + 1, n_sp, lambda i: greet({"sp": i}))

    @pl.when((c == 0) & (z == center))
    def _():
        each(0, center, lambda i: greet({"sp": i}))

    grid_rows = count // GRID_W
    loads = {}

    def load(name, src, dst):
        copy = pltpu.make_async_copy(src, dst, load_sem.at[len(loads)])
        copy.start()
        loads[name] = copy

    load("cond", cond_in, cond)
    load("m0", shift_w, mw.at[0])
    load("m1", scale_w, mw.at[1])
    load("m2", gate_w, mw.at[2])
    load("rows", latent, rows.at[t])
    load("gain", gain_in, gain)
    load("kw", k_t, kvt.at[pl.ds(0, HD)])
    load("vw", v_t, kvt.at[pl.ds(HD, HD)])
    load("ctx", context, ctx_rows)
    load("qw", q_w, w.at[:, pl.ds(0, LANES)])
    load("rt", row_tab.at[pl.ds(pl.multiple_of(z * grid_rows, 8), grid_rows)], rt)
    load("ct", col_tab, ct)
    load("sink", sink_in, sink)
    load("ow", o_w, ow)

    def contact():
        pl.semaphore_wait(barrier, c * 3 + (1 - c) * (1 + z + jnp.where(z < center, 1, 0)))

    def modulation():
        loads["cond"].wait()
        cv = cond[...].astype(f32)
        lifted = jnp.broadcast_to((cv / (1.0 + jnp.exp(-cv))).astype(bf16), (16, cv.shape[1]))
        for i in range(3):
            loads["m%d" % i].wait()
            part = jnp.dot(lifted, mw[i], preferred_element_type=f32)
            for j in range(per):
                mpair[c, per * i + j : per * i + j + 1, :] = part[0:1, j * LANES : (j + 1) * LANES]
        mpair[c, 3 * per : 16, :] = jnp.zeros((16 - 3 * per, LANES), f32)

    n_ctx = ctx_rows.shape[0]

    def own_context():
        for name in ("kw", "vw", "gain", "ctx"):
            loads[name].wait()
        for i in range(depth // COLS):
            w[i * COLS : (i + 1) * COLS, LANES : 2 * LANES] = kvt[:, i * COLS : (i + 1) * COLS].T
        sq = jnp.zeros((n_ctx, LANES), f32)
        for i in range(depth // LANES):
            v = ctx_rows[:, i * LANES : (i + 1) * LANES].astype(f32)
            sq = sq + v * v
        cinv = lax.rsqrt(jnp.sum(sq, axis=1, keepdims=True) * (1.0 / depth) + epsilon)
        acc = jnp.zeros((n_ctx, LANES), f32)
        for i in range(depth // COLS):
            part = slice(i * COLS, (i + 1) * COLS)
            v = ctx_rows[:, part].astype(f32) * cinv * gain[:, part]
            acc = acc + jnp.dot(v.astype(bf16), w[part, LANES : 2 * LANES], preferred_element_type=f32)
        cown[...] = acc.astype(bf16)

    def row_stats(g):
        sq = jnp.zeros((group, LANES), f32)
        for i in range(depth // LANES):
            v = rows[g, :, i * LANES : (i + 1) * LANES].astype(f32)
            sq = sq + v * v
        r = lax.rsqrt(jnp.sum(sq, axis=1, keepdims=True) * (1.0 / depth) + epsilon)
        inv[g] = jnp.broadcast_to(r, (group, LANES))

    @pl.when(z == 0)
    def _():
        kv[:WIN, :] = jnp.zeros((WIN, LANES), bf16)

    @pl.when(z == n_sp - 1)
    def _():
        kv[WIN + count :, :] = jnp.zeros((WIN, LANES), bf16)

    def piece(g, q):
        return rows.at[g, pl.ds(16 * q, 16)]

    zero_l, zero_r, zero_o = t_l - c, t_r - c, t_o - c

    def meet():
        pl.semaphore_wait(hello, 1)
        send(mpair.at[1], mpair.at[1], pair_send.at[0], pair_recv.at[0], {"tp": sib}, False)

    def hand_context():
        send(cown, cg.at[z, 1], pair_send.at[1], pair_recv.at[1], {"tp": sib}, False)

    def sibling_rows():
        recv(rows.at[sib], sib_recv.at[sib], {"tp": sib})
        for q in range(chunks):
            send(piece(sib, q), piece(sib, q), ag_send.at[2, q], ag_recv.at[2, q], {"tp": t_r}, False)
            send(piece(sib, q), piece(sib, q), ag_send.at[3, q], ag_recv.at[3, q], {"tp": t_l}, False)

    def hand(groups):
        for g in groups:
            send(rows.at[g], rows.at[g], sib_send.at[g], sib_recv.at[g], {"tp": sib}, False)

    @pl.when(c == 1)
    def _():
        loads["rows"].wait()
        contact()
        for q in range(chunks):
            send(piece(t, q), piece(t, q), ag_send.at[0, q], ag_recv.at[0, q], {"tp": t_r}, False)
            send(piece(t, q), piece(t, q), ag_send.at[1, q], ag_recv.at[1, q], {"tp": t_l}, False)
        modulation()
        pl.when(~late)(meet)
        own_context()
        pl.when(~late)(hand_context)
        pl.when(~late)(sibling_rows)
        for q in range(chunks):
            recv(piece(t_r, q), ag_recv.at[1, q], {"tp": t_r})
            send(piece(t_r, q), piece(t_r, q), ag_send.at[4, q], ag_recv.at[4, q], {"tp": t_l}, False)
        for q in range(chunks):
            recv(piece(t_l, q), ag_recv.at[0, q], {"tp": t_l})
        pl.when(~late)(functools.partial(hand, (t, t_r, t_l)))
        row_stats(t)
        row_stats(t_l)
        row_stats(t_r)
        for q in range(chunks):
            recv(piece(zero_l, q), ag_recv.at[2, q], {"tp": t_l})
            send(piece(zero_l, q), piece(zero_l, q), ag_send.at[5, q], ag_recv.at[5, q], {"tp": t_r}, False)
        for q in range(chunks):
            recv(piece(zero_r, q), ag_recv.at[3, q], {"tp": t_r})
        pl.when(~late)(functools.partial(hand, (zero_l, zero_r)))
        row_stats(zero_l)
        row_stats(zero_r)
        for q in range(chunks):
            recv(piece(t_o, q), ag_recv.at[4, q], {"tp": t_r})
        pl.when(~late)(functools.partial(hand, (t_o,)))
        row_stats(t_o)
        for q in range(chunks):
            recv(piece(zero_o, q), ag_recv.at[5, q], {"tp": t_l})
        pl.when(~late)(functools.partial(hand, (zero_o,)))
        row_stats(zero_o)

        @pl.when(late)
        def _():
            meet()
            hand_context()
            sibling_rows()
            hand((t, t_r, t_l, zero_l, zero_r, t_o, zero_o))

        row_stats(sib)
        recv(mt.at[x], xs_recv.at[x], {"tp": sib})
        for n, (who, xx) in enumerate(((t_r, xr), (t_l, xl), (t_o, xo))):
            send(mt.at[x], mt.at[x], x_send.at[n], x_recv.at[x], {"tp": who}, False)
        for who, xx in ((t_r, xr), (t_l, xl), (t_o, xo)):
            recv(mt.at[xx], x_recv.at[xx], {"tp": who})
            send(mt.at[xx], mt.at[xx], xs_send.at[xx], xs_recv.at[xx], {"tp": sib}, False)
        recv(cg.at[:, 1], pair_recv.at[2], {"tp": sib})

    @pl.when(c == 0)
    def _():
        modulation()
        loads["rows"].wait()
        contact()
        pl.semaphore_signal(hello, inc=1, device_id={"tp": sib}, device_id_type=MESH)
        send(rows.at[t], rows.at[t], sib_send.at[t], sib_recv.at[t], {"tp": sib}, False)
        recv(mpair.at[1], pair_recv.at[0], {"tp": sib})

        @pl.when(z != center)
        def _():
            send(mpair, mall.at[z], m_send.at[0], m_recv.at[z], {"sp": center}, False)

        @pl.when(z == center)
        def _():
            mall[center] = mpair[...]

        own_context()
        cg[z, 0] = cown[...]
        row_stats(t)
        recv(cg.at[z, 1], pair_recv.at[1], {"tp": sib})

        def give(i):
            send(cg.at[z], cg.at[z], c_send.at[i], c_recv.at[z], {"sp": i}, False)

        def answer(i):
            recv(cg.at[i], c_recv.at[i], {"sp": i})
            give(i)

        each(0, z, give)
        each(z + 1, n_sp, answer)

        @pl.when(z == center)
        def _():
            def take(i):
                @pl.when(i != center)
                def _():
                    recv(mall.at[i], m_recv.at[i], {"sp": i})

            each(0, n_sp, take)
            tot = mall[0]
            for i in range(1, n_sp):
                tot = tot + mall[i]
            msum[...] = tot

            def tell(i):
                @pl.when(i != center)
                def _():
                    send(msum, mt.at[x], tot_send.at[i], tot_recv, {"sp": i}, False)

            each(0, n_sp, tell)
            mt[x] = tot

        @pl.when(z != center)
        def _():
            recv(mt.at[x], tot_recv, {"sp": center})

        send(mt.at[x], mt.at[x], xs_send.at[x], xs_recv.at[x], {"tp": sib}, False)
        each(0, z, lambda i: recv(cg.at[i], c_recv.at[i], {"sp": i}))
        send(cg.at[:, 1], cg.at[:, 1], pair_send.at[2], pair_recv.at[2], {"tp": sib}, False)
        for g in (sib, t_r + 1, t_l + 1, t_r, t_l, t_o + 1, t_o):
            recv(rows.at[g], sib_recv.at[g], {"tp": sib})
            row_stats(g)
        for xx in (xr, xl, xo):
            recv(mt.at[xx], xs_recv.at[xx], {"tp": sib})

    for j in range(n_sp):
        ctx[pl.ds(j * n_ctx, n_ctx), :] = cg[j, c]
    for j in range(n_tp):
        for i in range(per):
            part = slice(j * width + i * LANES, j * width + (i + 1) * LANES)
            s_vec[:, part] = mt[j // 2, j % 2, i : i + 1, :]
            a_vec[:, part] = gain[:, part] * (1.0 + mt[j // 2, j % 2, per + i : per + i + 1, :])
            g_vec[:, part] = mt[j // 2, j % 2, 2 * per + i : 2 * per + i + 1, :]
    for name in ("rt", "ct", "qw", "ow", "sink"):
        loads[name].wait()

    lane = lax.broadcasted_iota(jnp.int32, (1, LANES), 1)
    first = lane % 32 < 16

    def swapped(v):
        return jnp.where(first, pltpu.roll(v, LANES - 16, 1), pltpu.roll(v, 16, 1))

    def project(gs):
        acc = jnp.zeros((len(gs) * group, 2 * LANES), f32)
        for i in range(depth // COLS):
            part = slice(i * COLS, (i + 1) * COLS)
            a = a_vec[:, part]
            s = s_vec[:, part]
            tiles = []
            for g in gs:
                r = jnp.concatenate([inv[g]] * (COLS // LANES), axis=1)
                tiles.append((rows[g, :, part].astype(f32) * r * a + s).astype(bf16))
            acc = acc + jnp.dot(jnp.concatenate(tiles, axis=0), w[part, :], preferred_element_type=f32)
        for n, g in enumerate(gs):
            fac = rt[g : g + 1, :] + ct[...]
            vq = acc[n * group : (n + 1) * group, :LANES]
            vk = acc[n * group : (n + 1) * group, LANES:]
            q2 = vq * fac[:, :LANES] + swapped(vq) * fac[:, LANES : 2 * LANES]
            k2 = vk * fac[:, 2 * LANES : 3 * LANES] + swapped(vk) * fac[:, 3 * LANES :]
            qrot[g * group : (g + 1) * group, :] = q2.astype(bf16)
            kv[WIN + g * group : WIN + (g + 1) * group, :] = k2.astype(bf16)

    project((0, 1, n_tp - 2, n_tp - 1))

    @pl.when(z > 0)
    def _():
        send(kv.at[pl.ds(WIN, WIN)], kv.at[pl.ds(WIN + count, WIN)], h_send.at[0], h_recv.at[0], {"sp": z - 1}, False)

    @pl.when(z < n_sp - 1)
    def _():
        send(kv.at[pl.ds(count, WIN)], kv.at[pl.ds(0, WIN)], h_send.at[1], h_recv.at[1], {"sp": z + 1}, False)

    project(tuple(range(2, n_tp - 2)))

    rows2 = 2 * WIN
    qi = lax.broadcasted_iota(jnp.int32, (rows2, WIN), 0) % WIN
    ki = lax.broadcasted_iota(jnp.int32, (rows2, WIN), 1)
    head1 = lax.broadcasted_iota(jnp.int32, (rows2, 1), 0) >= WIN
    sink_col = jnp.where(head1, sink[0:1, 1:2], sink[0:1, 0:1])
    is_key = lane < HD
    contract = (((1,), (1,)), ((), ()))
    blocks = count // WIN

    def attend(b):
        qb = qrot[b * WIN : (b + 1) * WIN, :].astype(f32)
        q0 = jnp.where(is_key, qb, 0.0).astype(bf16)
        q1 = jnp.where(is_key, pltpu.roll(qb, HD, 1), 0.0).astype(bf16)
        qq = jnp.concatenate([q0, q1], axis=0)
        band = kv[b * WIN : (b + 3) * WIN, :]
        whole = ctx[...]
        s_band = lax.dot_general(qq, band, contract, preferred_element_type=f32)
        s_ctx = lax.dot_general(qq, whole, contract, preferred_element_type=f32)
        left = ki >= qi
        right = ki <= qi
        if b == 0:
            left = left & (z > 0)
        if b == blocks - 1:
            right = right & (z < n_sp - 1)
        s0 = jnp.where(left, s_band[:, :WIN], neg_large)
        s1 = s_band[:, WIN : 2 * WIN]
        s2 = jnp.where(right, s_band[:, 2 * WIN :], neg_large)
        top = jnp.maximum(jnp.maximum(s0, s1), s2)
        for i in range(whole.shape[0] // LANES):
            top = jnp.maximum(top, s_ctx[:, i * LANES : (i + 1) * LANES])
        m = jnp.maximum(jnp.max(top, axis=1, keepdims=True), sink_col)
        e0 = jnp.exp(s0 - m)
        e1 = jnp.exp(s1 - m)
        e2 = jnp.exp(s2 - m)
        ec = jnp.exp(s_ctx - m)
        tot = e0 + e1 + e2
        for i in range(whole.shape[0] // LANES):
            tot = tot + ec[:, i * LANES : (i + 1) * LANES]
        den = jnp.sum(tot, axis=1, keepdims=True) + jnp.exp(sink_col - m)
        r = 1.0 / den
        p_band = jnp.concatenate([e0, e1, e2], axis=1) * r
        o = jnp.dot(p_band.astype(bf16), band, preferred_element_type=f32) + jnp.dot(
            (ec * r).astype(bf16), whole, preferred_element_type=f32
        )
        res = jnp.where(is_key, pltpu.roll(o[:WIN], HD, 1), o[WIN:]).astype(bf16)
        att[t, b * WIN : (b + 1) * WIN, :] = res

    def att_piece(who, b):
        return att.at[who, pl.ds(b * WIN, WIN)]

    def att_send(b):
        mine = att_piece(t, b)
        send(mine, mine, t_send.at[2, b], t_recv.at[2, b], {"tp": t_o})
        send(mine, mine, t_send.at[0, b], t_recv.at[0, b], {"tp": t_r})
        send(mine, mine, t_send.at[1, b], t_recv.at[1, b], {"tp": t_l})
        send(mine, mine, tsib_send.at[0, b], tsib_recv.at[0, b], {"tp": sib})

    def att_take(b):
        for role, who in ((0, t_l), (1, t_r), (2, t_o)):
            got = att_piece(who, b)
            recv(got, t_recv.at[role, b], {"tp": who})
            send(got, got, tsib_send.at[1 + role, b], tsib_recv.at[1 + role, b], {"tp": sib})

    order = [*range(1, blocks - 1), 0, blocks - 1]
    for n, b in enumerate(order):
        if n == blocks - 2:
            @pl.when(z < n_sp - 1)
            def _():
                recv(kv.at[pl.ds(WIN + count, WIN)], h_recv.at[0], {"sp": z + 1})

            @pl.when(z > 0)
            def _():
                recv(kv.at[pl.ds(0, WIN)], h_recv.at[1], {"sp": z - 1})

        attend(b)
        att_send(b)
        if n >= 2:
            att_take(order[n - 2])
    att_take(order[-2])
    att_take(order[-1])
    for b in order:
        for role, xx in ((0, x), (1, xl), (2, xr), (3, xo)):
            recv(att_piece(xx * 2 + 1 - c, b), tsib_recv.at[role, b], {"tp": sib})

    here = pl.ds(pl.multiple_of(t * width, LANES), width)
    for n, xx in enumerate((xo, xr, xl, x)):
        part = pl.ds(pl.multiple_of(xx * WIN, WIN), WIN)
        y = jnp.zeros((WIN, width), f32)
        for i in range(n_x):
            lhs = jnp.concatenate([att[2 * i, part, :], att[2 * i + 1, part, :]], axis=1)
            y = y + jnp.dot(lhs, ow[2 * i * LANES : 2 * (i + 1) * LANES, :], preferred_element_type=f32)
        ysend[2 * n] = y[:group].astype(bf16)
        ysend[2 * n + 1] = y[group:].astype(bf16)
        if n < 3:
            for k in range(2):
                send(ysend.at[2 * n + k], yrecv.at[:, here], y_send.at[2 * n + k], y_recv.at[2 * n + c], {"tp": xx * 2 + k})
        else:
            send(ysend.at[2 * n + 1 - c], yrecv.at[:, here], y_send.at[6], y_recv.at[6], {"tp": sib})
            yrecv[:, here] = ysend[2 * n + c]
    for n, xx in enumerate((xo, xl, xr)):
        for k in range(2):
            cols = pl.ds(pl.multiple_of((xx * 2 + k) * width, LANES), width)
            recv(yrecv.at[:, cols], y_recv.at[2 * n + k], {"tp": xx * 2 + k})
    recv(yrecv.at[:, pl.ds(pl.multiple_of(sib * width, LANES), width)], y_recv.at[6], {"tp": sib})
    for i in range(depth // COLS):
        part = slice(i * COLS, (i + 1) * COLS)
        out[:, part] = (
            rows[t, :, part].astype(f32) + g_vec[:, part] * yrecv[:, part].astype(f32)
        ).astype(bf16)
    for copy in started:
        copy.wait_send()

    @pl.when(z > 0)
    def _():
        sent(kv.at[pl.ds(WIN, WIN)], h_send.at[0], {"sp": z - 1})

    @pl.when(z < n_sp - 1)
    def _():
        sent(kv.at[pl.ds(count, WIN)], h_send.at[1], {"sp": z + 1})

    @pl.when(c == 1)
    def _():
        sent(mpair.at[1], pair_send.at[0], {"tp": sib})
        sent(cown, pair_send.at[1], {"tp": sib})
        for q in range(chunks):
            for n, (g, who) in enumerate(
                ((t, t_r), (t, t_l), (sib, t_r), (sib, t_l), (t_r, t_l), (zero_l, t_r))
            ):
                sent(piece(g, q), ag_send.at[n, q], {"tp": who})
        for g in (t, t_r, t_l, zero_l, zero_r, t_o, zero_o):
            sent(rows.at[g], sib_send.at[g], {"tp": sib})
        for n, who in enumerate((t_r, t_l, t_o)):
            sent(mt.at[x], x_send.at[n], {"tp": who})
        for xx in (xr, xl, xo):
            sent(mt.at[xx], xs_send.at[xx], {"tp": sib})

    @pl.when(c == 0)
    def _():
        sent(rows.at[t], sib_send.at[t], {"tp": sib})
        sent(mt.at[x], xs_send.at[x], {"tp": sib})
        sent(cg.at[:, 1], pair_send.at[2], {"tp": sib})

        def gone(i):
            @pl.when(i != z)
            def _():
                sent(cg.at[z], c_send.at[i], {"sp": i})

            @pl.when((z == center) & (i != z))
            def _():
                sent(msum, tot_send.at[i], {"sp": i})

        each(0, n_sp, gone)

        @pl.when(z != center)
        def _():
            sent(mpair, m_send.at[0], {"sp": center})


def local(n_sp, n_tp, latent, context, conditioning, norm_gain, *rest):
    shift_w, scale_w, gate_w, q_w, k_w, v_w, o_w, sink = rest
    group, depth = latent.shape
    n_ctx = context.shape[0]
    count = n_tp * group
    width = shift_w.shape[1]
    blocks = count // WIN
    chunks = group // 16
    row_tab, col_tab = rope_tables(n_sp * count // GRID_W)
    any_space = pl.BlockSpec(memory_space=pl.ANY)
    vmem = pl.BlockSpec(memory_space=pltpu.VMEM)
    dma = pltpu.SemaphoreType.DMA
    return pl.pallas_call(
        functools.partial(kernel, n_sp, n_tp),
        out_shape=jax.ShapeDtypeStruct((group, depth), bf16),
        in_specs=[any_space] * 14,
        out_specs=vmem,
        scratch_shapes=[
            pltpu.VMEM((n_tp, group, depth), bf16),
            pltpu.VMEM((depth, 2 * LANES), bf16),
            pltpu.VMEM((2 * HD, depth), bf16),
            pltpu.VMEM(o_w.shape, bf16),
            pltpu.VMEM((3, *shift_w.shape), bf16),
            pltpu.VMEM((n_ctx, depth), bf16),
            pltpu.VMEM((n_sp, 2, n_ctx, LANES), bf16),
            pltpu.VMEM((n_ctx, LANES), bf16),
            pltpu.VMEM((2, 16, LANES), f32),
            pltpu.VMEM((n_sp, 2, 16, LANES), f32),
            pltpu.VMEM((2, 16, LANES), f32),
            pltpu.VMEM((n_tp // 2, 2, 16, LANES), f32),
            pltpu.VMEM((n_tp, group, LANES), f32),
            pltpu.VMEM((1, depth), f32),
            pltpu.VMEM((1, depth), f32),
            pltpu.VMEM((1, depth), f32),
            pltpu.VMEM((count, LANES), bf16),
            pltpu.VMEM((count + 2 * WIN, LANES), bf16),
            pltpu.VMEM((n_sp * n_ctx, LANES), bf16),
            pltpu.VMEM((n_tp, count, LANES), bf16),
            pltpu.VMEM((n_tp, group, width), bf16),
            pltpu.VMEM((group, depth), bf16),
            pltpu.VMEM((count // GRID_W, 4 * LANES), f32),
            pltpu.VMEM((GRID_W, 4 * LANES), f32),
            pltpu.VMEM((1, conditioning.shape[0]), bf16),
            pltpu.VMEM((1, depth), f32),
            pltpu.VMEM((1, sink.shape[0]), f32),
            pltpu.SemaphoreType.REGULAR,
            dma((16,)),
            dma((3,)),
            dma((3,)),
            dma((1,)),
            dma((n_sp,)),
            dma((n_sp,)),
            dma,
            dma((n_sp,)),
            dma((n_sp,)),
            dma((6, chunks)),
            dma((6, chunks)),
            dma((n_tp,)),
            dma((n_tp,)),
            dma((3,)),
            dma((n_tp // 2,)),
            dma((n_tp // 2,)),
            dma((n_tp // 2,)),
            dma((2,)),
            dma((2,)),
            dma((3, blocks)),
            dma((3, blocks)),
            dma((4, blocks)),
            dma((4, blocks)),
            dma((8,)),
            dma((8,)),
        ],
        compiler_params=pltpu.CompilerParams(
            collective_id=0, has_side_effects=True, vmem_limit_bytes=56 * 1024 * 1024
        ),
    )(
        latent,
        context,
        conditioning.reshape(1, -1),
        norm_gain.reshape(1, -1),
        shift_w,
        scale_w,
        gate_w,
        q_w,
        k_w.T,
        v_w.T,
        o_w,
        sink.reshape(1, -1),
        jnp.asarray(row_tab),
        jnp.asarray(col_tab),
    )


def solution(mesh):
    in_specs = (
        P(("grp", "sp", "tp"), None),
        P(("grp", "sp"), None),
        P(("grp", "sp")),
        P(),
        P("sp", "tp"),
        P("sp", "tp"),
        P("sp", "tp"),
        P(None, "tp"),
        P(None, "tp"),
        P(None, "tp"),
        P(None, "tp"),
        P("tp"),
    )
    return jax.shard_map(
        functools.partial(local, mesh.shape["sp"], mesh.shape["tp"]),
        mesh=mesh,
        in_specs=in_specs,
        out_specs=P(("grp", "sp", "tp"), None),
        check_vma=False,
    )
```

```python
import functools

import jax
import jax.numpy as jnp
import numpy as np
from jax import lax
from jax.experimental import pallas as pl
from jax.experimental.pallas import tpu as pltpu
from jax.sharding import PartitionSpec as P

HEADS = 16
KV_HEADS = 8
HD = 64
GRID_W = 64
WIN = 128
SPAN = 4
LANES = 128
COLS = 512

epsilon = 1e-06
rope_base = 10000.0
neg_large = -1e30
MESH = pl.DeviceIdType.MESH
f32 = jnp.float32
bf16 = jnp.bfloat16


def rope_tables(grid_rows):
    lane = np.arange(LANES)
    d = lane % HD
    freq = rope_base ** (-(d % 16) / 16.0)
    is_row = d < HD // 2
    sign = np.where(d % 32 < 16, -1.0, 1.0)
    is_key = lane < HD

    def table(count, own):
        angle = np.arange(count)[:, None] * freq[None, :]
        c = np.where(own, np.cos(angle), 0.0)
        s = np.where(own, np.sin(angle) * sign, 0.0)
        scale = HD**-0.5
        ck = np.where(is_key, c, 0.0)
        sk = np.where(is_key, s, 0.0)
        return np.concatenate([c * scale, s * scale, ck, sk], axis=1)

    rows = table(grid_rows, is_row)
    cols = table(GRID_W, ~is_row)
    cols[:, 2 * LANES : 3 * LANES] += np.where(is_key, 0.0, 1.0)
    return rows.astype(np.float32), cols.astype(np.float32)


def kernel(
    n_sp,
    n_tp,
    latent,
    context,
    cond_in,
    gain_in,
    shift_w,
    scale_w,
    gate_w,
    q_w,
    k_t,
    v_t,
    o_w,
    sink_in,
    row_tab,
    col_tab,
    out,
    rows,
    w,
    kvt,
    ow,
    mw,
    ctx_rows,
    cg,
    cown,
    cpair,
    mpair,
    mall,
    msum,
    mt,
    inv,
    a_vec,
    s_vec,
    g_vec,
    qrot,
    kv,
    ctx,
    att,
    ysend,
    yrecv,
    rt,
    ct,
    cond,
    gain,
    sink,
    hello,
    load_sem,
    pair_send,
    pair_recv,
    m_send,
    m_recv,
    tot_send,
    tot_recv,
    c_send,
    p_recv,
    b_recv,
    bl_send,
    bm_send,
    ag_send,
    ag_recv,
    sib_send,
    sib_recv,
    x_send,
    x_recv,
    xs_send,
    xs_recv,
    h_send,
    h_recv,
    t_send,
    t_recv,
    tsib_send,
    tsib_recv,
    y_send,
    y_recv,
):
    n_x = n_tp // 2
    z = lax.axis_index("sp")
    t = lax.axis_index("tp")
    x = t // 2
    c = t % 2
    xr = (x + 1) % n_x
    xl = (x + n_x - 1) % n_x
    xo = (x + 2) % n_x
    sib = x * 2 + (1 - c)
    t_r, t_l, t_o = xr * 2 + c, xl * 2 + c, xo * 2 + c
    group = latent.shape[0]
    count = n_tp * group
    depth = latent.shape[1]
    chunks = group // 16
    width = shift_w.shape[1]
    per = width // LANES

    late = (z == 0) & (x == 0)
    center = 1

    started = []

    def send(src, dst, ss, rs, dev, keep=True):
        copy = pltpu.make_async_remote_copy(
            src_ref=src, dst_ref=dst, send_sem=ss, recv_sem=rs, device_id=dev, device_id_type=MESH
        )
        copy.start()
        if keep:
            started.append(copy)

    def recv(dst, rs, dev):
        pltpu.make_async_remote_copy(
            src_ref=dst, dst_ref=dst, send_sem=rs, recv_sem=rs, device_id=dev, device_id_type=MESH
        ).wait_recv()

    def sent(src, ss, dev):
        pltpu.make_async_remote_copy(
            src_ref=src, dst_ref=src, send_sem=ss, recv_sem=ss, device_id=dev, device_id_type=MESH
        ).wait_send()

    def each(lo, hi, body):
        def step(i, carry):
            body(i)
            return carry

        lax.fori_loop(lo, hi, step, 0)

    barrier = pltpu.get_barrier_semaphore()

    def greet(dev):
        pl.semaphore_signal(barrier, inc=1, device_id=dev, device_id_type=MESH)

    @pl.when(c == 1)
    def _():
        for who in (sib, t_r, t_l, t_o):
            greet({"tp": who})

    lead = SPAN * (z // SPAN) + center
    members = [(z // SPAN) * SPAN + j for j in range(SPAN) if j != center]
    teams = n_sp // SPAN
    team = z // SPAN

    @pl.when((c == 0) & (z == center))
    def _():
        each(0, center, lambda i: greet({"sp": i}))
        each(center + 1, n_sp, lambda i: greet({"sp": i}))

    @pl.when((c == 0) & (z == lead))
    def _():
        for i in members:
            greet({"sp": i})
        each(team + 1, teams, lambda i: greet({"sp": SPAN * i + center}))

    grid_rows = count // GRID_W
    loads = {}

    def load(name, src, dst):
        copy = pltpu.make_async_copy(src, dst, load_sem.at[len(loads)])
        copy.start()
        loads[name] = copy

    load("cond", cond_in, cond)
    load("m0", shift_w, mw.at[0])
    load("m1", scale_w, mw.at[1])
    load("m2", gate_w, mw.at[2])
    load("rows", latent, rows.at[t])
    load("gain", gain_in, gain)
    load("kw", k_t, kvt.at[pl.ds(0, HD)])
    load("vw", v_t, kvt.at[pl.ds(HD, HD)])
    load("ctx", context, ctx_rows)
    load("qw", q_w, w.at[:, pl.ds(0, LANES)])
    load("rt", row_tab.at[pl.ds(pl.multiple_of(z * grid_rows, 8), grid_rows)], rt)
    load("ct", col_tab, ct)
    load("sink", sink_in, sink)
    load("ow", o_w, ow)

    def contact():
        pl.semaphore_wait(barrier, c * 3 + (1 - c) * (1 + jnp.where(z == center, 0, 1) + jnp.where(z == lead, team, 1)))

    def modulation():
        loads["cond"].wait()
        cv = cond[...].astype(f32)
        lifted = jnp.broadcast_to((cv / (1.0 + jnp.exp(-cv))).astype(bf16), (16, cv.shape[1]))
        for i in range(3):
            loads["m%d" % i].wait()
            part = jnp.dot(lifted, mw[i], preferred_element_type=f32)
            for j in range(per):
                mpair[c, per * i + j : per * i + j + 1, :] = part[0:1, j * LANES : (j + 1) * LANES]
        mpair[c, 3 * per : 16, :] = jnp.zeros((16 - 3 * per, LANES), f32)

    n_ctx = ctx_rows.shape[0]

    def own_context():
        for name in ("kw", "vw", "gain", "ctx"):
            loads[name].wait()
        for i in range(depth // COLS):
            w[i * COLS : (i + 1) * COLS, LANES : 2 * LANES] = kvt[:, i * COLS : (i + 1) * COLS].T
        sq = jnp.zeros((n_ctx, LANES), f32)
        for i in range(depth // LANES):
            v = ctx_rows[:, i * LANES : (i + 1) * LANES].astype(f32)
            sq = sq + v * v
        cinv = lax.rsqrt(jnp.sum(sq, axis=1, keepdims=True) * (1.0 / depth) + epsilon)
        acc = jnp.zeros((n_ctx, LANES), f32)
        for i in range(depth // COLS):
            part = slice(i * COLS, (i + 1) * COLS)
            v = ctx_rows[:, part].astype(f32) * cinv * gain[:, part]
            acc = acc + jnp.dot(v.astype(bf16), w[part, LANES : 2 * LANES], preferred_element_type=f32)
        cown[...] = acc.astype(bf16)

    def row_stats(g):
        sq = jnp.zeros((group, LANES), f32)
        for i in range(depth // LANES):
            v = rows[g, :, i * LANES : (i + 1) * LANES].astype(f32)
            sq = sq + v * v
        r = lax.rsqrt(jnp.sum(sq, axis=1, keepdims=True) * (1.0 / depth) + epsilon)
        inv[g] = jnp.broadcast_to(r, (group, LANES))

    @pl.when(z == 0)
    def _():
        kv[:WIN, :] = jnp.zeros((WIN, LANES), bf16)

    @pl.when(z == n_sp - 1)
    def _():
        kv[WIN + count :, :] = jnp.zeros((WIN, LANES), bf16)

    def piece(g, q):
        return rows.at[g, pl.ds(16 * q, 16)]

    zero_l, zero_r, zero_o = t_l - c, t_r - c, t_o - c

    def meet():
        pl.semaphore_wait(hello, 1)
        send(mpair.at[1], mpair.at[1], pair_send.at[0], pair_recv.at[0], {"tp": sib}, False)

    def hand_context():
        send(cown, cpair.at[1], pair_send.at[1], pair_recv.at[1], {"tp": sib}, False)

    def sibling_rows():
        recv(rows.at[sib], sib_recv.at[sib], {"tp": sib})
        for q in range(chunks):
            send(piece(sib, q), piece(sib, q), ag_send.at[2, q], ag_recv.at[2, q], {"tp": t_r}, False)
            send(piece(sib, q), piece(sib, q), ag_send.at[3, q], ag_recv.at[3, q], {"tp": t_l}, False)

    def hand(groups):
        for g in groups:
            send(rows.at[g], rows.at[g], sib_send.at[g], sib_recv.at[g], {"tp": sib}, False)

    @pl.when(c == 1)
    def _():
        loads["rows"].wait()
        contact()
        for q in range(chunks):
            send(piece(t, q), piece(t, q), ag_send.at[0, q], ag_recv.at[0, q], {"tp": t_r}, False)
            send(piece(t, q), piece(t, q), ag_send.at[1, q], ag_recv.at[1, q], {"tp": t_l}, False)
        modulation()
        pl.when(~late)(meet)
        own_context()
        pl.when(~late)(hand_context)
        pl.when(~late)(sibling_rows)
        for q in range(chunks):
            recv(piece(t_r, q), ag_recv.at[1, q], {"tp": t_r})
            send(piece(t_r, q), piece(t_r, q), ag_send.at[4, q], ag_recv.at[4, q], {"tp": t_l}, False)
        for q in range(chunks):
            recv(piece(t_l, q), ag_recv.at[0, q], {"tp": t_l})
        pl.when(~late)(functools.partial(hand, (t, t_r, t_l)))
        row_stats(t)
        row_stats(t_l)
        row_stats(t_r)
        for q in range(chunks):
            recv(piece(zero_l, q), ag_recv.at[2, q], {"tp": t_l})
            send(piece(zero_l, q), piece(zero_l, q), ag_send.at[5, q], ag_recv.at[5, q], {"tp": t_r}, False)
        for q in range(chunks):
            recv(piece(zero_r, q), ag_recv.at[3, q], {"tp": t_r})
        pl.when(~late)(functools.partial(hand, (zero_l, zero_r)))
        row_stats(zero_l)
        row_stats(zero_r)
        for q in range(chunks):
            recv(piece(t_o, q), ag_recv.at[4, q], {"tp": t_r})
        pl.when(~late)(functools.partial(hand, (t_o,)))
        row_stats(t_o)
        for q in range(chunks):
            recv(piece(zero_o, q), ag_recv.at[5, q], {"tp": t_l})
        pl.when(~late)(functools.partial(hand, (zero_o,)))
        row_stats(zero_o)

        @pl.when(late)
        def _():
            meet()
            hand_context()
            sibling_rows()
            hand((t, t_r, t_l, zero_l, zero_r, t_o, zero_o))

        row_stats(sib)
        recv(mt.at[x], xs_recv.at[x], {"tp": sib})
        for n, (who, xx) in enumerate(((t_r, xr), (t_l, xl), (t_o, xo))):
            send(mt.at[x], mt.at[x], x_send.at[n], x_recv.at[x], {"tp": who}, False)
        for who, xx in ((t_r, xr), (t_l, xl), (t_o, xo)):
            recv(mt.at[xx], x_recv.at[xx], {"tp": who})
            send(mt.at[xx], mt.at[xx], xs_send.at[xx], xs_recv.at[xx], {"tp": sib}, False)
        recv(cg.at[:, 1], pair_recv.at[2], {"tp": sib})

    @pl.when(c == 0)
    def _():
        modulation()
        loads["rows"].wait()
        contact()
        pl.semaphore_signal(hello, inc=1, device_id={"tp": sib}, device_id_type=MESH)
        send(rows.at[t], rows.at[t], sib_send.at[t], sib_recv.at[t], {"tp": sib}, False)
        recv(mpair.at[1], pair_recv.at[0], {"tp": sib})

        @pl.when(z != center)
        def _():
            send(mpair, mall.at[z], m_send.at[0], m_recv.at[z], {"sp": center}, False)

        @pl.when(z == center)
        def _():
            mall[center] = mpair[...]

        own_context()
        cpair[0] = cown[...]
        row_stats(t)
        recv(cpair.at[1], pair_recv.at[1], {"tp": sib})

        def block(i):
            return cg.at[pl.ds(SPAN * i, SPAN)]

        def tell_sum():
            def take(i):
                recv(mall.at[i], m_recv.at[i], {"sp": i})

            each(0, center, take)
            each(center + 1, n_sp, take)
            tot = mall[0]
            for i in range(1, n_sp):
                tot = tot + mall[i]
            msum[...] = tot

            def tell(i):
                send(msum, mt.at[x], tot_send.at[i], tot_recv, {"sp": i}, False)

            each(0, center, tell)
            each(center + 1, n_sp, tell)
            mt[x] = tot

        def pass_sum():
            send(mt.at[x], mt.at[x], xs_send.at[x], xs_recv.at[x], {"tp": sib}, False)

        def sum_in():
            recv(mt.at[x], tot_recv, {"sp": center})
            pass_sum()

        @pl.when(z != lead)
        def _():
            send(cpair, cg.at[z], c_send.at[0], p_recv.at[z % SPAN], {"sp": lead}, False)
            sum_in()
            each(0, teams, lambda i: recv(block(i), b_recv.at[i], {"sp": lead}))

        @pl.when(z == lead)
        def _():
            cg[z] = cpair[...]

            @pl.when(z == center)
            def _():
                tell_sum()
                pass_sum()

            for n, i in enumerate(members):
                recv(cg.at[i], p_recv.at[n + (1 if n >= center else 0)], {"sp": i})

            def hand_block(i):
                for n, who in enumerate(members):
                    send(block(i), block(i), bm_send.at[n, i], b_recv.at[i], {"sp": who}, False)

            def give(i):
                send(block(team), block(team), bl_send.at[i], b_recv.at[team], {"sp": SPAN * i + center}, False)

            def got(i):
                recv(block(i), b_recv.at[i], {"sp": SPAN * i + center})

            def answer(i):
                got(i)
                give(i)
                hand_block(i)

            def follow(i):
                got(i)
                hand_block(i)

            each(0, team, give)
            hand_block(team)
            each(team + 1, teams, answer)
            pl.when(z != center)(sum_in)
            each(0, team, follow)

        send(cg.at[:, 1], cg.at[:, 1], pair_send.at[2], pair_recv.at[2], {"tp": sib}, False)
        for g in (sib, t_r + 1, t_l + 1, t_r, t_l, t_o + 1, t_o):
            recv(rows.at[g], sib_recv.at[g], {"tp": sib})
            row_stats(g)
        for xx in (xr, xl, xo):
            recv(mt.at[xx], xs_recv.at[xx], {"tp": sib})

    for j in range(n_sp):
        ctx[pl.ds(j * n_ctx, n_ctx), :] = cg[j, c]
    for j in range(n_tp):
        for i in range(per):
            part = slice(j * width + i * LANES, j * width + (i + 1) * LANES)
            s_vec[:, part] = mt[j // 2, j % 2, i : i + 1, :]
            a_vec[:, part] = gain[:, part] * (1.0 + mt[j // 2, j % 2, per + i : per + i + 1, :])
            g_vec[:, part] = mt[j // 2, j % 2, 2 * per + i : 2 * per + i + 1, :]
    for name in ("rt", "ct", "qw", "ow", "sink"):
        loads[name].wait()

    lane = lax.broadcasted_iota(jnp.int32, (1, LANES), 1)
    first = lane % 32 < 16

    def swapped(v):
        return jnp.where(first, pltpu.roll(v, LANES - 16, 1), pltpu.roll(v, 16, 1))

    def project(gs):
        acc = jnp.zeros((len(gs) * group, 2 * LANES), f32)
        for i in range(depth // COLS):
            part = slice(i * COLS, (i + 1) * COLS)
            a = a_vec[:, part]
            s = s_vec[:, part]
            tiles = []
            for g in gs:
                r = jnp.concatenate([inv[g]] * (COLS // LANES), axis=1)
                tiles.append((rows[g, :, part].astype(f32) * r * a + s).astype(bf16))
            acc = acc + jnp.dot(jnp.concatenate(tiles, axis=0), w[part, :], preferred_element_type=f32)
        for n, g in enumerate(gs):
            fac = rt[g : g + 1, :] + ct[...]
            vq = acc[n * group : (n + 1) * group, :LANES]
            vk = acc[n * group : (n + 1) * group, LANES:]
            q2 = vq * fac[:, :LANES] + swapped(vq) * fac[:, LANES : 2 * LANES]
            k2 = vk * fac[:, 2 * LANES : 3 * LANES] + swapped(vk) * fac[:, 3 * LANES :]
            qrot[g * group : (g + 1) * group, :] = q2.astype(bf16)
            kv[WIN + g * group : WIN + (g + 1) * group, :] = k2.astype(bf16)

    project((0, 1, n_tp - 2, n_tp - 1))

    @pl.when(z > 0)
    def _():
        send(kv.at[pl.ds(WIN, WIN)], kv.at[pl.ds(WIN + count, WIN)], h_send.at[0], h_recv.at[0], {"sp": z - 1}, False)

    @pl.when(z < n_sp - 1)
    def _():
        send(kv.at[pl.ds(count, WIN)], kv.at[pl.ds(0, WIN)], h_send.at[1], h_recv.at[1], {"sp": z + 1}, False)

    project(tuple(range(2, n_tp - 2)))

    rows2 = 2 * WIN
    qi = lax.broadcasted_iota(jnp.int32, (rows2, WIN), 0) % WIN
    ki = lax.broadcasted_iota(jnp.int32, (rows2, WIN), 1)
    head1 = lax.broadcasted_iota(jnp.int32, (rows2, 1), 0) >= WIN
    sink_col = jnp.where(head1, sink[0:1, 1:2], sink[0:1, 0:1])
    is_key = lane < HD
    contract = (((1,), (1,)), ((), ()))
    blocks = count // WIN

    def attend(b):
        qb = qrot[b * WIN : (b + 1) * WIN, :].astype(f32)
        q0 = jnp.where(is_key, qb, 0.0).astype(bf16)
        q1 = jnp.where(is_key, pltpu.roll(qb, HD, 1), 0.0).astype(bf16)
        qq = jnp.concatenate([q0, q1], axis=0)
        band = kv[b * WIN : (b + 3) * WIN, :]
        whole = ctx[...]
        s_band = lax.dot_general(qq, band, contract, preferred_element_type=f32)
        s_ctx = lax.dot_general(qq, whole, contract, preferred_element_type=f32)
        left = ki >= qi
        right = ki <= qi
        if b == 0:
            left = left & (z > 0)
        if b == blocks - 1:
            right = right & (z < n_sp - 1)
        s0 = jnp.where(left, s_band[:, :WIN], neg_large)
        s1 = s_band[:, WIN : 2 * WIN]
        s2 = jnp.where(right, s_band[:, 2 * WIN :], neg_large)
        top = jnp.maximum(jnp.maximum(s0, s1), s2)
        for i in range(whole.shape[0] // LANES):
            top = jnp.maximum(top, s_ctx[:, i * LANES : (i + 1) * LANES])
        m = jnp.maximum(jnp.max(top, axis=1, keepdims=True), sink_col)
        e0 = jnp.exp(s0 - m)
        e1 = jnp.exp(s1 - m)
        e2 = jnp.exp(s2 - m)
        ec = jnp.exp(s_ctx - m)
        tot = e0 + e1 + e2
        for i in range(whole.shape[0] // LANES):
            tot = tot + ec[:, i * LANES : (i + 1) * LANES]
        den = jnp.sum(tot, axis=1, keepdims=True) + jnp.exp(sink_col - m)
        r = 1.0 / den
        p_band = jnp.concatenate([e0, e1, e2], axis=1) * r
        o = jnp.dot(p_band.astype(bf16), band, preferred_element_type=f32) + jnp.dot(
            (ec * r).astype(bf16), whole, preferred_element_type=f32
        )
        res = jnp.where(is_key, pltpu.roll(o[:WIN], HD, 1), o[WIN:]).astype(bf16)
        att[t, b * WIN : (b + 1) * WIN, :] = res

    def att_piece(who, b):
        return att.at[who, pl.ds(b * WIN, WIN)]

    def att_send(b):
        mine = att_piece(t, b)
        send(mine, mine, t_send.at[2, b], t_recv.at[2, b], {"tp": t_o})
        send(mine, mine, t_send.at[0, b], t_recv.at[0, b], {"tp": t_r})
        send(mine, mine, t_send.at[1, b], t_recv.at[1, b], {"tp": t_l})
        send(mine, mine, tsib_send.at[0, b], tsib_recv.at[0, b], {"tp": sib})

    def att_take(b):
        for role, who in ((0, t_l), (1, t_r), (2, t_o)):
            got = att_piece(who, b)
            recv(got, t_recv.at[role, b], {"tp": who})
            send(got, got, tsib_send.at[1 + role, b], tsib_recv.at[1 + role, b], {"tp": sib})

    order = [*range(1, blocks - 1), 0, blocks - 1]
    for n, b in enumerate(order):
        if n == blocks - 2:
            @pl.when(z < n_sp - 1)
            def _():
                recv(kv.at[pl.ds(WIN + count, WIN)], h_recv.at[0], {"sp": z + 1})

            @pl.when(z > 0)
            def _():
                recv(kv.at[pl.ds(0, WIN)], h_recv.at[1], {"sp": z - 1})

        attend(b)
        att_send(b)
        if n >= 2:
            att_take(order[n - 2])
    att_take(order[-2])
    att_take(order[-1])
    for b in order:
        for role, xx in ((0, x), (1, xl), (2, xr), (3, xo)):
            recv(att_piece(xx * 2 + 1 - c, b), tsib_recv.at[role, b], {"tp": sib})

    here = pl.ds(pl.multiple_of(t * width, LANES), width)
    for n, xx in enumerate((xo, xr, xl, x)):
        part = pl.ds(pl.multiple_of(xx * WIN, WIN), WIN)
        y = jnp.zeros((WIN, width), f32)
        for i in range(n_x):
            lhs = jnp.concatenate([att[2 * i, part, :], att[2 * i + 1, part, :]], axis=1)
            y = y + jnp.dot(lhs, ow[2 * i * LANES : 2 * (i + 1) * LANES, :], preferred_element_type=f32)
        ysend[2 * n] = y[:group].astype(bf16)
        ysend[2 * n + 1] = y[group:].astype(bf16)
        if n < 3:
            for k in range(2):
                send(ysend.at[2 * n + k], yrecv.at[:, here], y_send.at[2 * n + k], y_recv.at[2 * n + c], {"tp": xx * 2 + k})
        else:
            send(ysend.at[2 * n + 1 - c], yrecv.at[:, here], y_send.at[6], y_recv.at[6], {"tp": sib})
            yrecv[:, here] = ysend[2 * n + c]
    for n, xx in enumerate((xo, xl, xr)):
        for k in range(2):
            cols = pl.ds(pl.multiple_of((xx * 2 + k) * width, LANES), width)
            recv(yrecv.at[:, cols], y_recv.at[2 * n + k], {"tp": xx * 2 + k})
    recv(yrecv.at[:, pl.ds(pl.multiple_of(sib * width, LANES), width)], y_recv.at[6], {"tp": sib})
    for i in range(depth // COLS):
        part = slice(i * COLS, (i + 1) * COLS)
        out[:, part] = (
            rows[t, :, part].astype(f32) + g_vec[:, part] * yrecv[:, part].astype(f32)
        ).astype(bf16)
    for copy in started:
        copy.wait_send()

    @pl.when(z > 0)
    def _():
        sent(kv.at[pl.ds(WIN, WIN)], h_send.at[0], {"sp": z - 1})

    @pl.when(z < n_sp - 1)
    def _():
        sent(kv.at[pl.ds(count, WIN)], h_send.at[1], {"sp": z + 1})

    @pl.when(c == 1)
    def _():
        sent(mpair.at[1], pair_send.at[0], {"tp": sib})
        sent(cown, pair_send.at[1], {"tp": sib})
        for q in range(chunks):
            for n, (g, who) in enumerate(
                ((t, t_r), (t, t_l), (sib, t_r), (sib, t_l), (t_r, t_l), (zero_l, t_r))
            ):
                sent(piece(g, q), ag_send.at[n, q], {"tp": who})
        for g in (t, t_r, t_l, zero_l, zero_r, t_o, zero_o):
            sent(rows.at[g], sib_send.at[g], {"tp": sib})
        for n, who in enumerate((t_r, t_l, t_o)):
            sent(mt.at[x], x_send.at[n], {"tp": who})
        for xx in (xr, xl, xo):
            sent(mt.at[xx], xs_send.at[xx], {"tp": sib})

    @pl.when(c == 0)
    def _():
        sent(rows.at[t], sib_send.at[t], {"tp": sib})
        sent(mt.at[x], xs_send.at[x], {"tp": sib})
        sent(cg.at[:, 1], pair_send.at[2], {"tp": sib})

        def told(i):
            sent(msum, tot_send.at[i], {"sp": i})

        @pl.when(z == center)
        def _():
            each(0, center, told)
            each(center + 1, n_sp, told)

        @pl.when(z != lead)
        def _():
            sent(cpair, c_send.at[0], {"sp": lead})

        @pl.when(z == lead)
        def _():
            def given(i):
                sent(cg.at[pl.ds(SPAN * team, SPAN)], bl_send.at[i], {"sp": SPAN * i + center})

            each(0, team, given)
            each(team + 1, teams, given)

            def handed(i):
                for n, who in enumerate(members):
                    sent(cg.at[pl.ds(SPAN * i, SPAN)], bm_send.at[n, i], {"sp": who})

            each(0, teams, handed)

        @pl.when(z != center)
        def _():
            sent(mpair, m_send.at[0], {"sp": center})


def local(n_sp, n_tp, latent, context, conditioning, norm_gain, *rest):
    shift_w, scale_w, gate_w, q_w, k_w, v_w, o_w, sink = rest
    group, depth = latent.shape
    n_ctx = context.shape[0]
    count = n_tp * group
    width = shift_w.shape[1]
    blocks = count // WIN
    chunks = group // 16
    row_tab, col_tab = rope_tables(n_sp * count // GRID_W)
    any_space = pl.BlockSpec(memory_space=pl.ANY)
    vmem = pl.BlockSpec(memory_space=pltpu.VMEM)
    dma = pltpu.SemaphoreType.DMA
    return pl.pallas_call(
        functools.partial(kernel, n_sp, n_tp),
        out_shape=jax.ShapeDtypeStruct((group, depth), bf16),
        in_specs=[any_space] * 14,
        out_specs=vmem,
        scratch_shapes=[
            pltpu.VMEM((n_tp, group, depth), bf16),
            pltpu.VMEM((depth, 2 * LANES), bf16),
            pltpu.VMEM((2 * HD, depth), bf16),
            pltpu.VMEM(o_w.shape, bf16),
            pltpu.VMEM((3, *shift_w.shape), bf16),
            pltpu.VMEM((n_ctx, depth), bf16),
            pltpu.VMEM((n_sp, 2, n_ctx, LANES), bf16),
            pltpu.VMEM((n_ctx, LANES), bf16),
            pltpu.VMEM((2, n_ctx, LANES), bf16),
            pltpu.VMEM((2, 16, LANES), f32),
            pltpu.VMEM((n_sp, 2, 16, LANES), f32),
            pltpu.VMEM((2, 16, LANES), f32),
            pltpu.VMEM((n_tp // 2, 2, 16, LANES), f32),
            pltpu.VMEM((n_tp, group, LANES), f32),
            pltpu.VMEM((1, depth), f32),
            pltpu.VMEM((1, depth), f32),
            pltpu.VMEM((1, depth), f32),
            pltpu.VMEM((count, LANES), bf16),
            pltpu.VMEM((count + 2 * WIN, LANES), bf16),
            pltpu.VMEM((n_sp * n_ctx, LANES), bf16),
            pltpu.VMEM((n_tp, count, LANES), bf16),
            pltpu.VMEM((n_tp, group, width), bf16),
            pltpu.VMEM((group, depth), bf16),
            pltpu.VMEM((count // GRID_W, 4 * LANES), f32),
            pltpu.VMEM((GRID_W, 4 * LANES), f32),
            pltpu.VMEM((1, conditioning.shape[0]), bf16),
            pltpu.VMEM((1, depth), f32),
            pltpu.VMEM((1, sink.shape[0]), f32),
            pltpu.SemaphoreType.REGULAR,
            dma((16,)),
            dma((3,)),
            dma((3,)),
            dma((1,)),
            dma((n_sp,)),
            dma((n_sp,)),
            dma,
            dma((1,)),
            dma((SPAN,)),
            dma((n_sp // SPAN,)),
            dma((n_sp // SPAN,)),
            dma((SPAN - 1, n_sp // SPAN)),
            dma((6, chunks)),
            dma((6, chunks)),
            dma((n_tp,)),
            dma((n_tp,)),
            dma((3,)),
            dma((n_tp // 2,)),
            dma((n_tp // 2,)),
            dma((n_tp // 2,)),
            dma((2,)),
            dma((2,)),
            dma((3, blocks)),
            dma((3, blocks)),
            dma((4, blocks)),
            dma((4, blocks)),
            dma((8,)),
            dma((8,)),
        ],
        compiler_params=pltpu.CompilerParams(
            collective_id=0, has_side_effects=True, vmem_limit_bytes=56 * 1024 * 1024
        ),
    )(
        latent,
        context,
        conditioning.reshape(1, -1),
        norm_gain.reshape(1, -1),
        shift_w,
        scale_w,
        gate_w,
        q_w,
        k_w.T,
        v_w.T,
        o_w,
        sink.reshape(1, -1),
        jnp.asarray(row_tab),
        jnp.asarray(col_tab),
    )


def solution(mesh):
    in_specs = (
        P(("grp", "sp", "tp"), None),
        P(("grp", "sp"), None),
        P(("grp", "sp")),
        P(),
        P("sp", "tp"),
        P("sp", "tp"),
        P("sp", "tp"),
        P(None, "tp"),
        P(None, "tp"),
        P(None, "tp"),
        P(None, "tp"),
        P("tp"),
    )
    return jax.shard_map(
        functools.partial(local, mesh.shape["sp"], mesh.shape["tp"]),
        mesh=mesh,
        in_specs=in_specs,
        out_specs=P(("grp", "sp", "tp"), None),
        check_vma=False,
    )
```

```python
import functools

import jax
import jax.numpy as jnp
import numpy as np
from jax import lax
from jax.experimental import pallas as pl
from jax.experimental.pallas import tpu as pltpu
from jax.sharding import PartitionSpec as P

HEADS = 16
KV_HEADS = 8
HD = 64
GRID_W = 64
WIN = 128
SPAN = 4
LATEST = 2
LANES = 128
COLS = 512

epsilon = 1e-06
rope_base = 10000.0
neg_large = -1e30
MESH = pl.DeviceIdType.MESH
f32 = jnp.float32
bf16 = jnp.bfloat16


def rope_tables(grid_rows):
    lane = np.arange(LANES)
    d = lane % HD
    freq = rope_base ** (-(d % 16) / 16.0)
    is_row = d < HD // 2
    sign = np.where(d % 32 < 16, -1.0, 1.0)
    is_key = lane < HD

    def table(count, own):
        angle = np.arange(count)[:, None] * freq[None, :]
        c = np.where(own, np.cos(angle), 0.0)
        s = np.where(own, np.sin(angle) * sign, 0.0)
        scale = HD**-0.5
        ck = np.where(is_key, c, 0.0)
        sk = np.where(is_key, s, 0.0)
        return np.concatenate([c * scale, s * scale, ck, sk], axis=1)

    rows = table(grid_rows, is_row)
    cols = table(GRID_W, ~is_row)
    cols[:, 2 * LANES : 3 * LANES] += np.where(is_key, 0.0, 1.0)
    return rows.astype(np.float32), cols.astype(np.float32)


def kernel(
    n_sp,
    n_tp,
    latent,
    context,
    cond_in,
    gain_in,
    shift_w,
    scale_w,
    gate_w,
    q_w,
    k_t,
    v_t,
    o_w,
    sink_in,
    row_tab,
    col_tab,
    out,
    rows,
    w,
    kvt,
    ow,
    mw,
    ctx_rows,
    cg,
    cown,
    cpair,
    mpair,
    mall,
    msum,
    mt,
    inv,
    a_vec,
    s_vec,
    g_vec,
    qrot,
    kv,
    ctx,
    att,
    ysend,
    yrecv,
    rt,
    ct,
    cond,
    gain,
    sink,
    hello,
    load_sem,
    pair_send,
    pair_recv,
    m_send,
    m_recv,
    tot_send,
    tot_recv,
    c_send,
    p_recv,
    b_recv,
    bl_send,
    bm_send,
    ag_send,
    ag_recv,
    sib_send,
    sib_recv,
    x_send,
    x_recv,
    xs_send,
    xs_recv,
    h_send,
    h_recv,
    t_send,
    t_recv,
    tsib_send,
    tsib_recv,
    y_send,
    y_recv,
):
    n_x = n_tp // 2
    z = lax.axis_index("sp")
    t = lax.axis_index("tp")
    x = t // 2
    c = t % 2
    xr = (x + 1) % n_x
    xl = (x + n_x - 1) % n_x
    xo = (x + 2) % n_x
    sib = x * 2 + (1 - c)
    t_r, t_l, t_o = xr * 2 + c, xl * 2 + c, xo * 2 + c
    group = latent.shape[0]
    count = n_tp * group
    depth = latent.shape[1]
    chunks = group // 16
    width = shift_w.shape[1]
    per = width // LANES

    late = (z == 0) & (x == 0)
    center = 1

    started = []

    def send(src, dst, ss, rs, dev, keep=True):
        copy = pltpu.make_async_remote_copy(
            src_ref=src, dst_ref=dst, send_sem=ss, recv_sem=rs, device_id=dev, device_id_type=MESH
        )
        copy.start()
        if keep:
            started.append(copy)

    def recv(dst, rs, dev):
        pltpu.make_async_remote_copy(
            src_ref=dst, dst_ref=dst, send_sem=rs, recv_sem=rs, device_id=dev, device_id_type=MESH
        ).wait_recv()

    def sent(src, ss, dev):
        pltpu.make_async_remote_copy(
            src_ref=src, dst_ref=src, send_sem=ss, recv_sem=ss, device_id=dev, device_id_type=MESH
        ).wait_send()

    def each(lo, hi, body):
        def step(i, carry):
            body(i)
            return carry

        lax.fori_loop(lo, hi, step, 0)

    barrier = pltpu.get_barrier_semaphore()

    def greet(dev):
        pl.semaphore_signal(barrier, inc=1, device_id=dev, device_id_type=MESH)

    @pl.when(c == 1)
    def _():
        for who in (sib, t_r, t_l):
            greet({"tp": who})

    lead = SPAN * (z // SPAN) + center
    members = [(z // SPAN) * SPAN + j for j in range(SPAN) if j != center]
    teams = n_sp // SPAN
    team = z // SPAN

    @pl.when((c == 0) & (z == center))
    def _():
        each(0, center, lambda i: greet({"sp": i}))
        each(center + 1, n_sp, lambda i: greet({"sp": i}))

    @pl.when((c == 0) & (z == lead))
    def _():
        for i in members:
            greet({"sp": i})
        each(team + 1, teams, lambda i: greet({"sp": SPAN * i + center}))

    grid_rows = count // GRID_W
    loads = {}

    def load(name, src, dst):
        copy = pltpu.make_async_copy(src, dst, load_sem.at[len(loads)])
        copy.start()
        loads[name] = copy

    load("cond", cond_in, cond)
    load("m0", shift_w, mw.at[0])
    load("m1", scale_w, mw.at[1])
    load("m2", gate_w, mw.at[2])
    load("rows", latent, rows.at[t])
    load("gain", gain_in, gain)
    load("kw", k_t, kvt.at[pl.ds(0, HD)])
    load("vw", v_t, kvt.at[pl.ds(HD, HD)])
    load("ctx", context, ctx_rows)
    load("qw", q_w, w.at[:, pl.ds(0, LANES)])
    load("rt", row_tab.at[pl.ds(pl.multiple_of(z * grid_rows, 8), grid_rows)], rt)
    load("ct", col_tab, ct)
    load("sink", sink_in, sink)
    load("ow", o_w, ow)

    def contact():
        pl.semaphore_wait(barrier, c * 2 + (1 - c) * (1 + jnp.where(z == center, 0, 1) + jnp.where(z == lead, team, 1)))

    def modulation():
        loads["cond"].wait()
        cv = cond[...].astype(f32)
        lifted = jnp.broadcast_to((cv / (1.0 + jnp.exp(-cv))).astype(bf16), (16, cv.shape[1]))
        for i in range(3):
            loads["m%d" % i].wait()
            part = jnp.dot(lifted, mw[i], preferred_element_type=f32)
            for j in range(per):
                mpair[c, per * i + j : per * i + j + 1, :] = part[0:1, j * LANES : (j + 1) * LANES]
        mpair[c, 3 * per : 16, :] = jnp.zeros((16 - 3 * per, LANES), f32)

    n_ctx = ctx_rows.shape[0]

    def own_context():
        for name in ("kw", "vw", "gain", "ctx"):
            loads[name].wait()
        for i in range(depth // COLS):
            w[i * COLS : (i + 1) * COLS, LANES : 2 * LANES] = kvt[:, i * COLS : (i + 1) * COLS].T
        sq = jnp.zeros((n_ctx, LANES), f32)
        for i in range(depth // LANES):
            v = ctx_rows[:, i * LANES : (i + 1) * LANES].astype(f32)
            sq = sq + v * v
        cinv = lax.rsqrt(jnp.sum(sq, axis=1, keepdims=True) * (1.0 / depth) + epsilon)
        acc = jnp.zeros((n_ctx, LANES), f32)
        for i in range(depth // COLS):
            part = slice(i * COLS, (i + 1) * COLS)
            v = ctx_rows[:, part].astype(f32) * cinv * gain[:, part]
            acc = acc + jnp.dot(v.astype(bf16), w[part, LANES : 2 * LANES], preferred_element_type=f32)
        cown[...] = acc.astype(bf16)

    def row_stats(g):
        sq = jnp.zeros((group, LANES), f32)
        for i in range(depth // LANES):
            v = rows[g, :, i * LANES : (i + 1) * LANES].astype(f32)
            sq = sq + v * v
        r = lax.rsqrt(jnp.sum(sq, axis=1, keepdims=True) * (1.0 / depth) + epsilon)
        inv[g] = jnp.broadcast_to(r, (group, LANES))

    @pl.when(z == 0)
    def _():
        kv[:WIN, :] = jnp.zeros((WIN, LANES), bf16)

    @pl.when(z == n_sp - 1)
    def _():
        kv[WIN + count :, :] = jnp.zeros((WIN, LANES), bf16)

    def piece(g, q):
        return rows.at[g, pl.ds(16 * q, 16)]

    zero_l, zero_r, zero_o = t_l - c, t_r - c, t_o - c

    def meet():
        pl.semaphore_wait(hello, 1)
        send(mpair.at[1], mpair.at[1], pair_send.at[0], pair_recv.at[0], {"tp": sib}, False)

    def hand_context():
        send(cown, cpair.at[1], pair_send.at[1], pair_recv.at[1], {"tp": sib}, False)

    def sibling_rows():
        recv(rows.at[sib], sib_recv.at[sib], {"tp": sib})
        for q in range(chunks):
            send(piece(sib, q), piece(sib, q), ag_send.at[2, q], ag_recv.at[2, q], {"tp": t_r}, False)
            send(piece(sib, q), piece(sib, q), ag_send.at[3, q], ag_recv.at[3, q], {"tp": t_l}, False)

    def hand(groups):
        for g in groups:
            send(rows.at[g], rows.at[g], sib_send.at[g], sib_recv.at[g], {"tp": sib}, False)

    def exchange():
        for n, who in enumerate((t_r, t_l, t_o)):
            send(mt.at[x], mt.at[x], x_send.at[n], x_recv.at[x], {"tp": who}, False)
        for who, xx in ((t_r, xr), (t_l, xl), (t_o, xo)):
            recv(mt.at[xx], x_recv.at[xx], {"tp": who})

    def own_block(k, i):
        return cg.at[k, pl.ds(SPAN * i, SPAN)]

    @pl.when(c == 1)
    def _():
        loads["rows"].wait()
        contact()
        for q in range(chunks):
            send(piece(t, q), piece(t, q), ag_send.at[0, q], ag_recv.at[0, q], {"tp": t_r}, False)
            send(piece(t, q), piece(t, q), ag_send.at[1, q], ag_recv.at[1, q], {"tp": t_l}, False)
        modulation()
        pl.when(~late)(meet)
        own_context()
        pl.when(~late)(hand_context)
        pl.when(~late)(sibling_rows)
        for q in range(chunks):
            recv(piece(t_r, q), ag_recv.at[1, q], {"tp": t_r})
            send(piece(t_r, q), piece(t_r, q), ag_send.at[4, q], ag_recv.at[4, q], {"tp": t_l}, False)
        for q in range(chunks):
            recv(piece(t_l, q), ag_recv.at[0, q], {"tp": t_l})
        pl.when(~late)(functools.partial(hand, (t, t_r, t_l)))
        row_stats(t)
        row_stats(t_l)
        row_stats(t_r)
        for q in range(chunks):
            recv(piece(zero_l, q), ag_recv.at[2, q], {"tp": t_l})
            send(piece(zero_l, q), piece(zero_l, q), ag_send.at[5, q], ag_recv.at[5, q], {"tp": t_r}, False)
        for q in range(chunks):
            recv(piece(zero_r, q), ag_recv.at[3, q], {"tp": t_r})
        pl.when(~late)(functools.partial(hand, (zero_l, zero_r)))
        row_stats(zero_l)
        row_stats(zero_r)
        for q in range(chunks):
            recv(piece(t_o, q), ag_recv.at[4, q], {"tp": t_r})
        pl.when(~late)(functools.partial(hand, (t_o,)))
        row_stats(t_o)
        for q in range(chunks):
            recv(piece(zero_o, q), ag_recv.at[5, q], {"tp": t_l})
        pl.when(~late)(functools.partial(hand, (zero_o,)))
        row_stats(zero_o)

        @pl.when(late)
        def _():
            meet()
            hand_context()
            sibling_rows()
            hand((t, t_r, t_l, zero_l, zero_r, t_o, zero_o))

        row_stats(sib)
        recv(mt.at[x], xs_recv, {"tp": sib})
        exchange()

    @pl.when(c == 0)
    def _():
        modulation()
        loads["rows"].wait()
        contact()
        pl.semaphore_signal(hello, inc=1, device_id={"tp": sib}, device_id_type=MESH)
        send(rows.at[t], rows.at[t], sib_send.at[t], sib_recv.at[t], {"tp": sib}, False)
        recv(mpair.at[1], pair_recv.at[0], {"tp": sib})

        @pl.when(z != center)
        def _():
            send(mpair, mall.at[z], m_send.at[0], m_recv.at[z], {"sp": center}, False)

        @pl.when(z == center)
        def _():
            mall[center] = mpair[...]

        own_context()
        cpair[0] = cown[...]
        row_stats(t)
        recv(cpair.at[1], pair_recv.at[1], {"tp": sib})

        def block(i):
            return cg.at[:, pl.ds(SPAN * i, SPAN)]

        def tell_sum():
            def take(i):
                recv(mall.at[i], m_recv.at[i], {"sp": i})

            each(0, center, take)
            each(center + 1, n_sp, take)
            tot = mall[0]
            for i in range(1, n_sp):
                tot = tot + mall[i]
            msum[...] = tot

            def tell(i):
                send(msum, mt.at[x], tot_send.at[i], tot_recv, {"sp": i}, False)

            each(0, center, tell)
            each(center + 1, n_sp, tell)
            mt[x] = tot

        def sum_in():
            recv(mt.at[x], tot_recv, {"sp": center})

        def early_rows():
            for g in (sib, t_r + 1, t_l + 1, t_o + 1, t_r, t_l, t_o):
                recv(rows.at[g], sib_recv.at[g], {"tp": sib})
                row_stats(g)

        @pl.when(z != lead)
        def _():
            send(cpair, cg.at[:, z], c_send.at[0], p_recv.at[z % SPAN], {"sp": lead}, False)

        def hand_block(i):
            for n, who in enumerate(members):
                for k in range(2):
                    send(own_block(k, i), own_block(k, i), bm_send.at[k, n, i], b_recv.at[i], {"sp": who, "tp": t + k}, False)
            send(own_block(1, i), own_block(1, i), bm_send.at[0, SPAN - 1, i], b_recv.at[i], {"tp": sib}, False)

        def give(i):
            send(block(team), block(team), bl_send.at[i], b_recv.at[team], {"sp": SPAN * i + center}, False)

        def got(i):
            recv(block(i), b_recv.at[i], {"sp": SPAN * i + center})

        def answer(i):
            got(i)
            give(i)
            hand_block(i)

        def follow(i):
            got(i)
            hand_block(i)

        tail = jnp.where(z == center, teams - LATEST, teams)

        @pl.when(z == lead)
        def _():
            for k in range(2):
                cg[k, z] = cpair[k]
            for n, i in enumerate(members):
                recv(cg.at[:, i], p_recv.at[n + (1 if n >= center else 0)], {"sp": i})
            each(0, team, give)
            hand_block(team)
            each(team + 1, tail, answer)

        early_rows()
        pl.when(z == center)(tell_sum)
        pl.when(z != center)(sum_in)
        send(mt.at[x], mt.at[x], xs_send, xs_recv, {"tp": sib}, False)

        @pl.when(z == lead)
        def _():
            each(tail, teams, answer)
            each(0, team, follow)

        exchange()

    for j in range(n_tp):
        for i in range(per):
            part = slice(j * width + i * LANES, j * width + (i + 1) * LANES)
            s_vec[:, part] = mt[j // 2, j % 2, i : i + 1, :]
            a_vec[:, part] = gain[:, part] * (1.0 + mt[j // 2, j % 2, per + i : per + i + 1, :])
            g_vec[:, part] = mt[j // 2, j % 2, 2 * per + i : 2 * per + i + 1, :]
    for name in ("rt", "ct", "qw", "ow", "sink"):
        loads[name].wait()

    lane = lax.broadcasted_iota(jnp.int32, (1, LANES), 1)
    first = lane % 32 < 16

    def swapped(v):
        return jnp.where(first, pltpu.roll(v, LANES - 16, 1), pltpu.roll(v, 16, 1))

    def project(gs):
        acc = jnp.zeros((len(gs) * group, 2 * LANES), f32)
        for i in range(depth // COLS):
            part = slice(i * COLS, (i + 1) * COLS)
            a = a_vec[:, part]
            s = s_vec[:, part]
            tiles = []
            for g in gs:
                r = jnp.concatenate([inv[g]] * (COLS // LANES), axis=1)
                tiles.append((rows[g, :, part].astype(f32) * r * a + s).astype(bf16))
            acc = acc + jnp.dot(jnp.concatenate(tiles, axis=0), w[part, :], preferred_element_type=f32)
        for n, g in enumerate(gs):
            fac = rt[g : g + 1, :] + ct[...]
            vq = acc[n * group : (n + 1) * group, :LANES]
            vk = acc[n * group : (n + 1) * group, LANES:]
            q2 = vq * fac[:, :LANES] + swapped(vq) * fac[:, LANES : 2 * LANES]
            k2 = vk * fac[:, 2 * LANES : 3 * LANES] + swapped(vk) * fac[:, 3 * LANES :]
            qrot[g * group : (g + 1) * group, :] = q2.astype(bf16)
            kv[WIN + g * group : WIN + (g + 1) * group, :] = k2.astype(bf16)

    project((0, 1, n_tp - 2, n_tp - 1))

    @pl.when(z > 0)
    def _():
        send(kv.at[pl.ds(WIN, WIN)], kv.at[pl.ds(WIN + count, WIN)], h_send.at[0], h_recv.at[0], {"sp": z - 1}, False)

    @pl.when(z < n_sp - 1)
    def _():
        send(kv.at[pl.ds(count, WIN)], kv.at[pl.ds(0, WIN)], h_send.at[1], h_recv.at[1], {"sp": z + 1}, False)

    project(tuple(range(2, n_tp - 2)))

    @pl.when((c == 1) | (z != lead))
    def _():
        for i in range(n_sp // SPAN):
            recv(own_block(c, i), b_recv.at[i], {"sp": lead, "tp": t - c})

    for j in range(n_sp):
        ctx[pl.ds(j * n_ctx, n_ctx), :] = cg[c, j]
    rows2 = 2 * WIN
    qi = lax.broadcasted_iota(jnp.int32, (rows2, WIN), 0) % WIN
    ki = lax.broadcasted_iota(jnp.int32, (rows2, WIN), 1)
    head1 = lax.broadcasted_iota(jnp.int32, (rows2, 1), 0) >= WIN
    sink_col = jnp.where(head1, sink[0:1, 1:2], sink[0:1, 0:1])
    is_key = lane < HD
    contract = (((1,), (1,)), ((), ()))
    blocks = count // WIN

    def attend(b):
        qb = qrot[b * WIN : (b + 1) * WIN, :].astype(f32)
        q0 = jnp.where(is_key, qb, 0.0).astype(bf16)
        q1 = jnp.where(is_key, pltpu.roll(qb, HD, 1), 0.0).astype(bf16)
        qq = jnp.concatenate([q0, q1], axis=0)
        band = kv[b * WIN : (b + 3) * WIN, :]
        whole = ctx[...]
        s_band = lax.dot_general(qq, band, contract, preferred_element_type=f32)
        s_ctx = lax.dot_general(qq, whole, contract, preferred_element_type=f32)
        left = ki >= qi
        right = ki <= qi
        if b == 0:
            left = left & (z > 0)
        if b == blocks - 1:
            right = right & (z < n_sp - 1)
        s0 = jnp.where(left, s_band[:, :WIN], neg_large)
        s1 = s_band[:, WIN : 2 * WIN]
        s2 = jnp.where(right, s_band[:, 2 * WIN :], neg_large)
        top = jnp.maximum(jnp.maximum(s0, s1), s2)
        for i in range(whole.shape[0] // LANES):
            top = jnp.maximum(top, s_ctx[:, i * LANES : (i + 1) * LANES])
        m = jnp.maximum(jnp.max(top, axis=1, keepdims=True), sink_col)
        e0 = jnp.exp(s0 - m)
        e1 = jnp.exp(s1 - m)
        e2 = jnp.exp(s2 - m)
        ec = jnp.exp(s_ctx - m)
        tot = e0 + e1 + e2
        for i in range(whole.shape[0] // LANES):
            tot = tot + ec[:, i * LANES : (i + 1) * LANES]
        den = jnp.sum(tot, axis=1, keepdims=True) + jnp.exp(sink_col - m)
        r = 1.0 / den
        p_band = jnp.concatenate([e0, e1, e2], axis=1) * r
        o = jnp.dot(p_band.astype(bf16), band, preferred_element_type=f32) + jnp.dot(
            (ec * r).astype(bf16), whole, preferred_element_type=f32
        )
        res = jnp.where(is_key, pltpu.roll(o[:WIN], HD, 1), o[WIN:]).astype(bf16)
        att[t, b * WIN : (b + 1) * WIN, :] = res

    def att_piece(who, b):
        return att.at[who, pl.ds(b * WIN, WIN)]

    def att_send(b):
        mine = att_piece(t, b)
        send(mine, mine, t_send.at[2, b], t_recv.at[2, b], {"tp": t_o})
        send(mine, mine, t_send.at[0, b], t_recv.at[0, b], {"tp": t_r})
        send(mine, mine, t_send.at[1, b], t_recv.at[1, b], {"tp": t_l})
        send(mine, mine, tsib_send.at[0, b], tsib_recv.at[0, b], {"tp": sib})

    def att_take(b):
        for role, who in ((0, t_l), (1, t_r), (2, t_o)):
            got = att_piece(who, b)
            recv(got, t_recv.at[role, b], {"tp": who})
            send(got, got, tsib_send.at[1 + role, b], tsib_recv.at[1 + role, b], {"tp": sib})

    order = [*range(1, blocks - 1), 0, blocks - 1]
    for n, b in enumerate(order):
        if n == blocks - 2:
            @pl.when(z < n_sp - 1)
            def _():
                recv(kv.at[pl.ds(WIN + count, WIN)], h_recv.at[0], {"sp": z + 1})

            @pl.when(z > 0)
            def _():
                recv(kv.at[pl.ds(0, WIN)], h_recv.at[1], {"sp": z - 1})

        attend(b)
        att_send(b)
        if n >= 2:
            att_take(order[n - 2])
    att_take(order[-2])
    att_take(order[-1])
    for b in order:
        for role, xx in ((0, x), (1, xl), (2, xr), (3, xo)):
            recv(att_piece(xx * 2 + 1 - c, b), tsib_recv.at[role, b], {"tp": sib})

    before = len(started)
    here = pl.ds(pl.multiple_of(t * width, LANES), width)
    for n, xx in enumerate((xo, xr, xl, x)):
        part = pl.ds(pl.multiple_of(xx * WIN, WIN), WIN)
        y = jnp.zeros((WIN, width), f32)
        for i in range(n_x):
            lhs = jnp.concatenate([att[2 * i, part, :], att[2 * i + 1, part, :]], axis=1)
            y = y + jnp.dot(lhs, ow[2 * i * LANES : 2 * (i + 1) * LANES, :], preferred_element_type=f32)
        ysend[2 * n] = y[:group].astype(bf16)
        ysend[2 * n + 1] = y[group:].astype(bf16)
        if n < 3:
            for k in range(2):
                send(ysend.at[2 * n + k], yrecv.at[:, here], y_send.at[2 * n + k], y_recv.at[2 * n + c], {"tp": xx * 2 + k})
        else:
            send(ysend.at[2 * n + 1 - c], yrecv.at[:, here], y_send.at[6], y_recv.at[6], {"tp": sib})
            yrecv[:, here] = ysend[2 * n + c]
    for n, who in enumerate((t_r, t_l, t_o)):
        sent(mt.at[x], x_send.at[n], {"tp": who})

    for copy in started[:before]:
        copy.wait_send()

    @pl.when(z > 0)
    def _():
        sent(kv.at[pl.ds(WIN, WIN)], h_send.at[0], {"sp": z - 1})

    @pl.when(z < n_sp - 1)
    def _():
        sent(kv.at[pl.ds(count, WIN)], h_send.at[1], {"sp": z + 1})

    @pl.when(c == 1)
    def _():
        sent(mpair.at[1], pair_send.at[0], {"tp": sib})
        sent(cown, pair_send.at[1], {"tp": sib})
        for q in range(chunks):
            for n, (g, who) in enumerate(
                ((t, t_r), (t, t_l), (sib, t_r), (sib, t_l), (t_r, t_l), (zero_l, t_r))
            ):
                sent(piece(g, q), ag_send.at[n, q], {"tp": who})
        for g in (t, t_r, t_l, zero_l, zero_r, t_o, zero_o):
            sent(rows.at[g], sib_send.at[g], {"tp": sib})
    @pl.when(c == 0)
    def _():
        sent(rows.at[t], sib_send.at[t], {"tp": sib})
        sent(mt.at[x], xs_send, {"tp": sib})

        def told(i):
            sent(msum, tot_send.at[i], {"sp": i})

        @pl.when(z == center)
        def _():
            each(0, center, told)
            each(center + 1, n_sp, told)

        @pl.when(z != lead)
        def _():
            sent(cpair, c_send.at[0], {"sp": lead})

        @pl.when(z == lead)
        def _():
            def given(i):
                sent(cg.at[:, pl.ds(SPAN * team, SPAN)], bl_send.at[i], {"sp": SPAN * i + center})

            each(0, team, given)
            each(team + 1, teams, given)

            def handed(i):
                for n, who in enumerate(members):
                    for k in range(2):
                        sent(own_block(k, i), bm_send.at[k, n, i], {"sp": who})
                sent(own_block(1, i), bm_send.at[0, SPAN - 1, i], {"tp": sib})

            each(0, teams, handed)

        @pl.when(z != center)
        def _():
            sent(mpair, m_send.at[0], {"sp": center})

    for n, xx in enumerate((xo, xl, xr)):
        for k in range(2):
            cols = pl.ds(pl.multiple_of((xx * 2 + k) * width, LANES), width)
            recv(yrecv.at[:, cols], y_recv.at[2 * n + k], {"tp": xx * 2 + k})
    recv(yrecv.at[:, pl.ds(pl.multiple_of(sib * width, LANES), width)], y_recv.at[6], {"tp": sib})
    for i in range(depth // COLS):
        part = slice(i * COLS, (i + 1) * COLS)
        out[:, part] = (
            rows[t, :, part].astype(f32) + g_vec[:, part] * yrecv[:, part].astype(f32)
        ).astype(bf16)
    for copy in started[before:]:
        copy.wait_send()


def local(n_sp, n_tp, latent, context, conditioning, norm_gain, *rest):
    shift_w, scale_w, gate_w, q_w, k_w, v_w, o_w, sink = rest
    group, depth = latent.shape
    n_ctx = context.shape[0]
    count = n_tp * group
    width = shift_w.shape[1]
    blocks = count // WIN
    chunks = group // 16
    row_tab, col_tab = rope_tables(n_sp * count // GRID_W)
    any_space = pl.BlockSpec(memory_space=pl.ANY)
    vmem = pl.BlockSpec(memory_space=pltpu.VMEM)
    dma = pltpu.SemaphoreType.DMA
    return pl.pallas_call(
        functools.partial(kernel, n_sp, n_tp),
        out_shape=jax.ShapeDtypeStruct((group, depth), bf16),
        in_specs=[any_space] * 14,
        out_specs=vmem,
        scratch_shapes=[
            pltpu.VMEM((n_tp, group, depth), bf16),
            pltpu.VMEM((depth, 2 * LANES), bf16),
            pltpu.VMEM((2 * HD, depth), bf16),
            pltpu.VMEM(o_w.shape, bf16),
            pltpu.VMEM((3, *shift_w.shape), bf16),
            pltpu.VMEM((n_ctx, depth), bf16),
            pltpu.VMEM((2, n_sp, n_ctx, LANES), bf16),
            pltpu.VMEM((n_ctx, LANES), bf16),
            pltpu.VMEM((2, n_ctx, LANES), bf16),
            pltpu.VMEM((2, 16, LANES), f32),
            pltpu.VMEM((n_sp, 2, 16, LANES), f32),
            pltpu.VMEM((2, 16, LANES), f32),
            pltpu.VMEM((n_tp // 2, 2, 16, LANES), f32),
            pltpu.VMEM((n_tp, group, LANES), f32),
            pltpu.VMEM((1, depth), f32),
            pltpu.VMEM((1, depth), f32),
            pltpu.VMEM((1, depth), f32),
            pltpu.VMEM((count, LANES), bf16),
            pltpu.VMEM((count + 2 * WIN, LANES), bf16),
            pltpu.VMEM((n_sp * n_ctx, LANES), bf16),
            pltpu.VMEM((n_tp, count, LANES), bf16),
            pltpu.VMEM((n_tp, group, width), bf16),
            pltpu.VMEM((group, depth), bf16),
            pltpu.VMEM((count // GRID_W, 4 * LANES), f32),
            pltpu.VMEM((GRID_W, 4 * LANES), f32),
            pltpu.VMEM((1, conditioning.shape[0]), bf16),
            pltpu.VMEM((1, depth), f32),
            pltpu.VMEM((1, sink.shape[0]), f32),
            pltpu.SemaphoreType.REGULAR,
            dma((16,)),
            dma((3,)),
            dma((3,)),
            dma((1,)),
            dma((n_sp,)),
            dma((n_sp,)),
            dma,
            dma((1,)),
            dma((SPAN,)),
            dma((n_sp // SPAN,)),
            dma((n_sp // SPAN,)),
            dma((2, SPAN, n_sp // SPAN)),
            dma((6, chunks)),
            dma((6, chunks)),
            dma((n_tp,)),
            dma((n_tp,)),
            dma((3,)),
            dma((n_tp // 2,)),
            dma,
            dma,
            dma((2,)),
            dma((2,)),
            dma((3, blocks)),
            dma((3, blocks)),
            dma((4, blocks)),
            dma((4, blocks)),
            dma((8,)),
            dma((8,)),
        ],
        compiler_params=pltpu.CompilerParams(
            collective_id=0, has_side_effects=True, vmem_limit_bytes=56 * 1024 * 1024
        ),
    )(
        latent,
        context,
        conditioning.reshape(1, -1),
        norm_gain.reshape(1, -1),
        shift_w,
        scale_w,
        gate_w,
        q_w,
        k_w.T,
        v_w.T,
        o_w,
        sink.reshape(1, -1),
        jnp.asarray(row_tab),
        jnp.asarray(col_tab),
    )


def solution(mesh):
    in_specs = (
        P(("grp", "sp", "tp"), None),
        P(("grp", "sp"), None),
        P(("grp", "sp")),
        P(),
        P("sp", "tp"),
        P("sp", "tp"),
        P("sp", "tp"),
        P(None, "tp"),
        P(None, "tp"),
        P(None, "tp"),
        P(None, "tp"),
        P("tp"),
    )
    return jax.shard_map(
        functools.partial(local, mesh.shape["sp"], mesh.shape["tp"]),
        mesh=mesh,
        in_specs=in_specs,
        out_specs=P(("grp", "sp", "tp"), None),
        check_vma=False,
    )
```

```python
import functools

import jax
import jax.numpy as jnp
import numpy as np
from jax import lax
from jax.experimental import pallas as pl
from jax.experimental.pallas import tpu as pltpu
from jax.sharding import PartitionSpec as P

HEADS = 16
KV_HEADS = 8
HD = 64
GRID_W = 64
WIN = 128
SPAN = 4
LATEST = 4
LANES = 128
COLS = 512

epsilon = 1e-06
rope_base = 10000.0
neg_large = -1e30
MESH = pl.DeviceIdType.MESH
f32 = jnp.float32
bf16 = jnp.bfloat16


def rope_tables(grid_rows):
    lane = np.arange(LANES)
    d = lane % HD
    freq = rope_base ** (-(d % 16) / 16.0)
    is_row = d < HD // 2
    sign = np.where(d % 32 < 16, -1.0, 1.0)
    is_key = lane < HD

    def table(count, own):
        angle = np.arange(count)[:, None] * freq[None, :]
        c = np.where(own, np.cos(angle), 0.0)
        s = np.where(own, np.sin(angle) * sign, 0.0)
        scale = HD**-0.5
        ck = np.where(is_key, c, 0.0)
        sk = np.where(is_key, s, 0.0)
        return np.concatenate([c * scale, s * scale, ck, sk], axis=1)

    rows = table(grid_rows, is_row)
    cols = table(GRID_W, ~is_row)
    cols[:, 2 * LANES : 3 * LANES] += np.where(is_key, 0.0, 1.0)
    return rows.astype(np.float32), cols.astype(np.float32)


def kernel(
    n_sp,
    n_tp,
    latent,
    context,
    cond_in,
    gain_in,
    shift_w,
    scale_w,
    gate_w,
    q_w,
    k_t,
    v_t,
    o_w,
    sink_in,
    row_tab,
    col_tab,
    out,
    gate_out,
    rows,
    w,
    kvt,
    ow,
    mw,
    ctx_rows,
    cg,
    cown,
    cpair,
    mpair,
    mall,
    msum,
    mt,
    inv,
    a_vec,
    s_vec,
    g_vec,
    qrot,
    kv,
    ctx,
    att,
    ysend,
    rt,
    ct,
    cond,
    gain,
    sink,
    hello,
    load_sem,
    pair_send,
    pair_recv,
    m_send,
    m_recv,
    tot_send,
    tot_recv,
    c_send,
    p_recv,
    b_recv,
    bl_send,
    bm_send,
    ag_send,
    ag_recv,
    sib_send,
    sib_recv,
    x_send,
    x_recv,
    xs_send,
    xs_recv,
    h_send,
    h_recv,
    t_send,
    t_recv,
    tsib_send,
    tsib_recv,
    y_send,
    y_recv,
):
    n_x = n_tp // 2
    z = lax.axis_index("sp")
    t = lax.axis_index("tp")
    x = t // 2
    c = t % 2
    xr = (x + 1) % n_x
    xl = (x + n_x - 1) % n_x
    xo = (x + 2) % n_x
    sib = x * 2 + (1 - c)
    t_r, t_l, t_o = xr * 2 + c, xl * 2 + c, xo * 2 + c
    group = latent.shape[0]
    count = n_tp * group
    depth = latent.shape[1]
    chunks = group // 16
    width = shift_w.shape[1]
    per = width // LANES

    late = (z == 0) & (x == 0)
    center = 1

    started = []

    def send(src, dst, ss, rs, dev, keep=True):
        copy = pltpu.make_async_remote_copy(
            src_ref=src, dst_ref=dst, send_sem=ss, recv_sem=rs, device_id=dev, device_id_type=MESH
        )
        copy.start()
        if keep:
            started.append(copy)

    def recv(dst, rs, dev):
        pltpu.make_async_remote_copy(
            src_ref=dst, dst_ref=dst, send_sem=rs, recv_sem=rs, device_id=dev, device_id_type=MESH
        ).wait_recv()

    def sent(src, ss, dev):
        pltpu.make_async_remote_copy(
            src_ref=src, dst_ref=src, send_sem=ss, recv_sem=ss, device_id=dev, device_id_type=MESH
        ).wait_send()

    def each(lo, hi, body):
        def step(i, carry):
            body(i)
            return carry

        lax.fori_loop(lo, hi, step, 0)

    barrier = pltpu.get_barrier_semaphore()

    def greet(dev):
        pl.semaphore_signal(barrier, inc=1, device_id=dev, device_id_type=MESH)

    @pl.when(c == 1)
    def _():
        for who in (sib, t_r, t_l):
            greet({"tp": who})

    lead = SPAN * (z // SPAN) + center
    members = [(z // SPAN) * SPAN + j for j in range(SPAN) if j != center]
    teams = n_sp // SPAN
    team = z // SPAN

    @pl.when((c == 0) & (z == center))
    def _():
        each(0, center, lambda i: greet({"sp": i}))
        each(center + 1, n_sp, lambda i: greet({"sp": i}))

    @pl.when((c == 0) & (z == lead))
    def _():
        for i in members:
            greet({"sp": i})
        each(team + 1, teams, lambda i: greet({"sp": SPAN * i + center}))

    grid_rows = count // GRID_W
    loads = {}

    def load(name, src, dst):
        copy = pltpu.make_async_copy(src, dst, load_sem.at[len(loads)])
        copy.start()
        loads[name] = copy

    load("cond", cond_in, cond)
    load("m0", shift_w, mw.at[0])
    load("m1", scale_w, mw.at[1])
    load("m2", gate_w, mw.at[2])
    load("rows", latent, rows.at[t])
    load("gain", gain_in, gain)
    load("kw", k_t, kvt.at[pl.ds(0, HD)])
    load("vw", v_t, kvt.at[pl.ds(HD, HD)])
    load("ctx", context, ctx_rows)
    load("qw", q_w, w.at[:, pl.ds(0, LANES)])
    load("rt", row_tab.at[pl.ds(pl.multiple_of(z * grid_rows, 8), grid_rows)], rt)
    load("ct", col_tab, ct)
    load("sink", sink_in, sink)
    load("ow", o_w, ow)

    def contact():
        pl.semaphore_wait(barrier, c * 2 + (1 - c) * (1 + jnp.where(z == center, 0, 1) + jnp.where(z == lead, team, 1)))

    def modulation():
        loads["cond"].wait()
        cv = cond[...].astype(f32)
        lifted = jnp.broadcast_to((cv / (1.0 + jnp.exp(-cv))).astype(bf16), (16, cv.shape[1]))
        for i in range(3):
            loads["m%d" % i].wait()
            part = jnp.dot(lifted, mw[i], preferred_element_type=f32)
            for j in range(per):
                mpair[c, per * i + j : per * i + j + 1, :] = part[0:1, j * LANES : (j + 1) * LANES]
        mpair[c, 3 * per : 16, :] = jnp.zeros((16 - 3 * per, LANES), f32)

    n_ctx = ctx_rows.shape[0]

    def own_context():
        for name in ("kw", "vw", "gain", "ctx"):
            loads[name].wait()
        for i in range(depth // COLS):
            w[i * COLS : (i + 1) * COLS, LANES : 2 * LANES] = kvt[:, i * COLS : (i + 1) * COLS].T
        sq = jnp.zeros((n_ctx, LANES), f32)
        for i in range(depth // LANES):
            v = ctx_rows[:, i * LANES : (i + 1) * LANES].astype(f32)
            sq = sq + v * v
        cinv = lax.rsqrt(jnp.sum(sq, axis=1, keepdims=True) * (1.0 / depth) + epsilon)
        acc = jnp.zeros((n_ctx, LANES), f32)
        for i in range(depth // COLS):
            part = slice(i * COLS, (i + 1) * COLS)
            v = ctx_rows[:, part].astype(f32) * cinv * gain[:, part]
            acc = acc + jnp.dot(v.astype(bf16), w[part, LANES : 2 * LANES], preferred_element_type=f32)
        cown[...] = acc.astype(bf16)

    def row_stats(g):
        sq = jnp.zeros((group, LANES), f32)
        for i in range(depth // LANES):
            v = rows[g, :, i * LANES : (i + 1) * LANES].astype(f32)
            sq = sq + v * v
        r = lax.rsqrt(jnp.sum(sq, axis=1, keepdims=True) * (1.0 / depth) + epsilon)
        inv[g] = jnp.broadcast_to(r, (group, LANES))

    @pl.when(z == 0)
    def _():
        kv[:WIN, :] = jnp.zeros((WIN, LANES), bf16)

    @pl.when(z == n_sp - 1)
    def _():
        kv[WIN + count :, :] = jnp.zeros((WIN, LANES), bf16)

    def piece(g, q):
        return rows.at[g, pl.ds(16 * q, 16)]

    zero_l, zero_r, zero_o = t_l - c, t_r - c, t_o - c

    def meet():
        pl.semaphore_wait(hello, 1)
        send(mpair.at[1], mpair.at[1], pair_send.at[0], pair_recv.at[0], {"tp": sib}, False)

    def hand_context():
        send(cown, cpair.at[1], pair_send.at[1], pair_recv.at[1], {"tp": sib}, False)

    def sibling_rows():
        recv(rows.at[sib], sib_recv.at[sib], {"tp": sib})
        for q in range(chunks):
            send(piece(sib, q), piece(sib, q), ag_send.at[2, q], ag_recv.at[2, q], {"tp": t_r}, False)
            send(piece(sib, q), piece(sib, q), ag_send.at[3, q], ag_recv.at[3, q], {"tp": t_l}, False)

    def hand(groups):
        for g in groups:
            send(rows.at[g], rows.at[g], sib_send.at[g], sib_recv.at[g], {"tp": sib}, False)

    def exchange():
        for n, who in enumerate((t_r, t_l, t_o)):
            send(mt.at[x], mt.at[x], x_send.at[n], x_recv.at[x], {"tp": who}, False)
        for who, xx in ((t_r, xr), (t_l, xl), (t_o, xo)):
            recv(mt.at[xx], x_recv.at[xx], {"tp": who})

    def own_block(k, i):
        return cg.at[k, pl.ds(SPAN * i, SPAN)]

    @pl.when(c == 1)
    def _():
        loads["rows"].wait()
        contact()
        for q in range(chunks):
            send(piece(t, q), piece(t, q), ag_send.at[0, q], ag_recv.at[0, q], {"tp": t_r}, False)
            send(piece(t, q), piece(t, q), ag_send.at[1, q], ag_recv.at[1, q], {"tp": t_l}, False)
        modulation()
        pl.when(~late)(meet)
        own_context()
        pl.when(~late)(hand_context)
        pl.when(~late)(sibling_rows)
        for q in range(chunks):
            recv(piece(t_r, q), ag_recv.at[1, q], {"tp": t_r})
            send(piece(t_r, q), piece(t_r, q), ag_send.at[4, q], ag_recv.at[4, q], {"tp": t_l}, False)
        for q in range(chunks):
            recv(piece(t_l, q), ag_recv.at[0, q], {"tp": t_l})
        pl.when(~late)(functools.partial(hand, (t, t_r, t_l)))
        row_stats(t)
        row_stats(t_l)
        row_stats(t_r)
        for q in range(chunks):
            recv(piece(zero_l, q), ag_recv.at[2, q], {"tp": t_l})
            send(piece(zero_l, q), piece(zero_l, q), ag_send.at[5, q], ag_recv.at[5, q], {"tp": t_r}, False)
        for q in range(chunks):
            recv(piece(zero_r, q), ag_recv.at[3, q], {"tp": t_r})
        pl.when(~late)(functools.partial(hand, (zero_l, zero_r)))
        row_stats(zero_l)
        row_stats(zero_r)
        for q in range(chunks):
            recv(piece(t_o, q), ag_recv.at[4, q], {"tp": t_r})
        pl.when(~late)(functools.partial(hand, (t_o,)))
        row_stats(t_o)
        for q in range(chunks):
            recv(piece(zero_o, q), ag_recv.at[5, q], {"tp": t_l})
        pl.when(~late)(functools.partial(hand, (zero_o,)))
        row_stats(zero_o)

        @pl.when(late)
        def _():
            meet()
            hand_context()
            sibling_rows()
            hand((t, t_r, t_l, zero_l, zero_r, t_o, zero_o))

        row_stats(sib)
        recv(mt.at[x], xs_recv, {"tp": sib})
        exchange()

    @pl.when(c == 0)
    def _():
        modulation()
        loads["rows"].wait()
        contact()
        pl.semaphore_signal(hello, inc=1, device_id={"tp": sib}, device_id_type=MESH)
        send(rows.at[t], rows.at[t], sib_send.at[t], sib_recv.at[t], {"tp": sib}, False)
        recv(mpair.at[1], pair_recv.at[0], {"tp": sib})

        @pl.when(z != center)
        def _():
            send(mpair, mall.at[z], m_send.at[0], m_recv.at[z], {"sp": center}, False)

        @pl.when(z == center)
        def _():
            mall[center] = mpair[...]

        own_context()
        cpair[0] = cown[...]
        row_stats(t)
        recv(cpair.at[1], pair_recv.at[1], {"tp": sib})

        def block(i):
            return cg.at[:, pl.ds(SPAN * i, SPAN)]

        def tell_sum():
            def take(i):
                recv(mall.at[i], m_recv.at[i], {"sp": i})

            each(0, center, take)
            each(center + 1, n_sp, take)
            tot = mall[0]
            for i in range(1, n_sp):
                tot = tot + mall[i]
            msum[...] = tot

            def tell(i):
                send(msum, mt.at[x], tot_send.at[i], tot_recv, {"sp": i}, False)

            each(0, center, tell)
            each(center + 1, n_sp, tell)
            mt[x] = tot

        def sum_in():
            recv(mt.at[x], tot_recv, {"sp": center})

        def early_rows():
            for g in (sib, t_r + 1, t_l + 1, t_o + 1, t_r, t_l, t_o):
                recv(rows.at[g], sib_recv.at[g], {"tp": sib})
                row_stats(g)

        @pl.when(z != lead)
        def _():
            send(cpair, cg.at[:, z], c_send.at[0], p_recv.at[z % SPAN], {"sp": lead}, False)

        def hand_block(i):
            for n, who in enumerate(members):
                for k in range(2):
                    send(own_block(k, i), own_block(k, i), bm_send.at[k, n, i], b_recv.at[i], {"sp": who, "tp": t + k}, False)
            send(own_block(1, i), own_block(1, i), bm_send.at[0, SPAN - 1, i], b_recv.at[i], {"tp": sib}, False)

        def give(i):
            send(block(team), block(team), bl_send.at[i], b_recv.at[team], {"sp": SPAN * i + center}, False)

        def got(i):
            recv(block(i), b_recv.at[i], {"sp": SPAN * i + center})

        def answer(i):
            got(i)
            give(i)
            hand_block(i)

        def follow(i):
            got(i)
            hand_block(i)

        tail = jnp.where(z == center, teams - LATEST, teams)
        pl.when(z == center)(early_rows)

        @pl.when(z == lead)
        def _():
            for k in range(2):
                cg[k, z] = cpair[k]
            for n, i in enumerate(members):
                recv(cg.at[:, i], p_recv.at[n + (1 if n >= center else 0)], {"sp": i})
            each(0, team, give)
            hand_block(team)
            each(team + 1, tail, answer)

        pl.when(z != center)(early_rows)
        pl.when(z == center)(tell_sum)
        pl.when(z != center)(sum_in)
        send(mt.at[x], mt.at[x], xs_send, xs_recv, {"tp": sib}, False)

        @pl.when(z == lead)
        def _():
            each(tail, teams, answer)
            each(0, team, follow)

        exchange()

    for j in range(n_tp):
        for i in range(per):
            part = slice(j * width + i * LANES, j * width + (i + 1) * LANES)
            s_vec[:, part] = mt[j // 2, j % 2, i : i + 1, :]
            a_vec[:, part] = gain[:, part] * (1.0 + mt[j // 2, j % 2, per + i : per + i + 1, :])
            g_vec[:, part] = mt[j // 2, j % 2, 2 * per + i : 2 * per + i + 1, :]
    gates = pltpu.make_async_copy(g_vec, gate_out, load_sem.at[15])
    gates.start()
    for name in ("rt", "ct", "qw", "ow", "sink"):
        loads[name].wait()

    lane = lax.broadcasted_iota(jnp.int32, (1, LANES), 1)
    first = lane % 32 < 16

    def swapped(v):
        return jnp.where(first, pltpu.roll(v, LANES - 16, 1), pltpu.roll(v, 16, 1))

    def project(gs):
        acc = jnp.zeros((len(gs) * group, 2 * LANES), f32)
        for i in range(depth // COLS):
            part = slice(i * COLS, (i + 1) * COLS)
            a = a_vec[:, part]
            s = s_vec[:, part]
            tiles = []
            for g in gs:
                r = jnp.concatenate([inv[g]] * (COLS // LANES), axis=1)
                tiles.append((rows[g, :, part].astype(f32) * r * a + s).astype(bf16))
            acc = acc + jnp.dot(jnp.concatenate(tiles, axis=0), w[part, :], preferred_element_type=f32)
        for n, g in enumerate(gs):
            fac = rt[g : g + 1, :] + ct[...]
            vq = acc[n * group : (n + 1) * group, :LANES]
            vk = acc[n * group : (n + 1) * group, LANES:]
            q2 = vq * fac[:, :LANES] + swapped(vq) * fac[:, LANES : 2 * LANES]
            k2 = vk * fac[:, 2 * LANES : 3 * LANES] + swapped(vk) * fac[:, 3 * LANES :]
            qrot[g * group : (g + 1) * group, :] = q2.astype(bf16)
            kv[WIN + g * group : WIN + (g + 1) * group, :] = k2.astype(bf16)

    project((0, 1, n_tp - 2, n_tp - 1))

    @pl.when(z > 0)
    def _():
        send(kv.at[pl.ds(WIN, WIN)], kv.at[pl.ds(WIN + count, WIN)], h_send.at[0], h_recv.at[0], {"sp": z - 1}, False)

    @pl.when(z < n_sp - 1)
    def _():
        send(kv.at[pl.ds(count, WIN)], kv.at[pl.ds(0, WIN)], h_send.at[1], h_recv.at[1], {"sp": z + 1}, False)

    project(tuple(range(2, n_tp - 2)))

    @pl.when((c == 1) | (z != lead))
    def _():
        for i in range(n_sp // SPAN):
            recv(own_block(c, i), b_recv.at[i], {"sp": lead, "tp": t - c})

    for j in range(n_sp):
        ctx[pl.ds(j * n_ctx, n_ctx), :] = cg[c, j]
    rows2 = 2 * WIN
    qi = lax.broadcasted_iota(jnp.int32, (rows2, WIN), 0) % WIN
    ki = lax.broadcasted_iota(jnp.int32, (rows2, WIN), 1)
    head1 = lax.broadcasted_iota(jnp.int32, (rows2, 1), 0) >= WIN
    sink_col = jnp.where(head1, sink[0:1, 1:2], sink[0:1, 0:1])
    is_key = lane < HD
    contract = (((1,), (1,)), ((), ()))
    blocks = count // WIN

    def attend(b):
        qb = qrot[b * WIN : (b + 1) * WIN, :].astype(f32)
        q0 = jnp.where(is_key, qb, 0.0).astype(bf16)
        q1 = jnp.where(is_key, pltpu.roll(qb, HD, 1), 0.0).astype(bf16)
        qq = jnp.concatenate([q0, q1], axis=0)
        band = kv[b * WIN : (b + 3) * WIN, :]
        whole = ctx[...]
        s_band = lax.dot_general(qq, band, contract, preferred_element_type=f32)
        s_ctx = lax.dot_general(qq, whole, contract, preferred_element_type=f32)
        left = ki >= qi
        right = ki <= qi
        if b == 0:
            left = left & (z > 0)
        if b == blocks - 1:
            right = right & (z < n_sp - 1)
        s0 = jnp.where(left, s_band[:, :WIN], neg_large)
        s1 = s_band[:, WIN : 2 * WIN]
        s2 = jnp.where(right, s_band[:, 2 * WIN :], neg_large)
        top = jnp.maximum(jnp.maximum(s0, s1), s2)
        for i in range(whole.shape[0] // LANES):
            top = jnp.maximum(top, s_ctx[:, i * LANES : (i + 1) * LANES])
        m = jnp.maximum(jnp.max(top, axis=1, keepdims=True), sink_col)
        e0 = jnp.exp(s0 - m)
        e1 = jnp.exp(s1 - m)
        e2 = jnp.exp(s2 - m)
        ec = jnp.exp(s_ctx - m)
        tot = e0 + e1 + e2
        for i in range(whole.shape[0] // LANES):
            tot = tot + ec[:, i * LANES : (i + 1) * LANES]
        den = jnp.sum(tot, axis=1, keepdims=True) + jnp.exp(sink_col - m)
        r = 1.0 / den
        p_band = jnp.concatenate([e0, e1, e2], axis=1) * r
        o = jnp.dot(p_band.astype(bf16), band, preferred_element_type=f32) + jnp.dot(
            (ec * r).astype(bf16), whole, preferred_element_type=f32
        )
        res = jnp.where(is_key, pltpu.roll(o[:WIN], HD, 1), o[WIN:]).astype(bf16)
        att[t, b * WIN : (b + 1) * WIN, :] = res

    def att_piece(who, b):
        return att.at[who, pl.ds(b * WIN, WIN)]

    def att_send(b):
        mine = att_piece(t, b)
        send(mine, mine, t_send.at[2, b], t_recv.at[2, b], {"tp": t_o})
        send(mine, mine, t_send.at[0, b], t_recv.at[0, b], {"tp": t_r})
        send(mine, mine, t_send.at[1, b], t_recv.at[1, b], {"tp": t_l})
        send(mine, mine, tsib_send.at[0, b], tsib_recv.at[0, b], {"tp": sib})

    def att_take(b):
        for role, who in ((0, t_l), (1, t_r), (2, t_o)):
            got = att_piece(who, b)
            recv(got, t_recv.at[role, b], {"tp": who})
            send(got, got, tsib_send.at[1 + role, b], tsib_recv.at[1 + role, b], {"tp": sib})

    order = [*range(1, blocks - 1), 0, blocks - 1]
    for n, b in enumerate(order):
        if n == blocks - 2:
            @pl.when(z < n_sp - 1)
            def _():
                recv(kv.at[pl.ds(WIN + count, WIN)], h_recv.at[0], {"sp": z + 1})

            @pl.when(z > 0)
            def _():
                recv(kv.at[pl.ds(0, WIN)], h_recv.at[1], {"sp": z - 1})

        attend(b)
        att_send(b)
        if n >= 2:
            att_take(order[n - 2])
    att_take(order[-2])
    att_take(order[-1])
    for b in order:
        for role, xx in ((0, x), (1, xl), (2, xr), (3, xo)):
            recv(att_piece(xx * 2 + 1 - c, b), tsib_recv.at[role, b], {"tp": sib})

    before = len(started)
    here = pl.ds(pl.multiple_of(t * width, LANES), width)
    for n, xx in enumerate((xo, xr, xl, x)):
        part = pl.ds(pl.multiple_of(xx * WIN, WIN), WIN)
        y = jnp.zeros((WIN, width), f32)
        for i in range(n_x):
            lhs = jnp.concatenate([att[2 * i, part, :], att[2 * i + 1, part, :]], axis=1)
            y = y + jnp.dot(lhs, ow[2 * i * LANES : 2 * (i + 1) * LANES, :], preferred_element_type=f32)
        ysend[2 * n] = y[:group].astype(bf16)
        ysend[2 * n + 1] = y[group:].astype(bf16)
        if n < 3:
            for k in range(2):
                send(ysend.at[2 * n + k], out.at[:, here], y_send.at[2 * n + k], y_recv.at[2 * n + c], {"tp": xx * 2 + k})
        else:
            send(ysend.at[2 * n + 1 - c], out.at[:, here], y_send.at[6], y_recv.at[6], {"tp": sib})
            keep = pltpu.make_async_copy(ysend.at[2 * n + c], out.at[:, here], load_sem.at[14])
            keep.start()
    for n, who in enumerate((t_r, t_l, t_o)):
        sent(mt.at[x], x_send.at[n], {"tp": who})

    for copy in started[:before]:
        copy.wait_send()

    @pl.when(z > 0)
    def _():
        sent(kv.at[pl.ds(WIN, WIN)], h_send.at[0], {"sp": z - 1})

    @pl.when(z < n_sp - 1)
    def _():
        sent(kv.at[pl.ds(count, WIN)], h_send.at[1], {"sp": z + 1})

    @pl.when(c == 1)
    def _():
        sent(mpair.at[1], pair_send.at[0], {"tp": sib})
        sent(cown, pair_send.at[1], {"tp": sib})
        for q in range(chunks):
            for n, (g, who) in enumerate(
                ((t, t_r), (t, t_l), (sib, t_r), (sib, t_l), (t_r, t_l), (zero_l, t_r))
            ):
                sent(piece(g, q), ag_send.at[n, q], {"tp": who})
        for g in (t, t_r, t_l, zero_l, zero_r, t_o, zero_o):
            sent(rows.at[g], sib_send.at[g], {"tp": sib})
    @pl.when(c == 0)
    def _():
        sent(rows.at[t], sib_send.at[t], {"tp": sib})
        sent(mt.at[x], xs_send, {"tp": sib})

        def told(i):
            sent(msum, tot_send.at[i], {"sp": i})

        @pl.when(z == center)
        def _():
            each(0, center, told)
            each(center + 1, n_sp, told)

        @pl.when(z != lead)
        def _():
            sent(cpair, c_send.at[0], {"sp": lead})

        @pl.when(z == lead)
        def _():
            def given(i):
                sent(cg.at[:, pl.ds(SPAN * team, SPAN)], bl_send.at[i], {"sp": SPAN * i + center})

            each(0, team, given)
            each(team + 1, teams, given)

            def handed(i):
                for n, who in enumerate(members):
                    for k in range(2):
                        sent(own_block(k, i), bm_send.at[k, n, i], {"sp": who})
                sent(own_block(1, i), bm_send.at[0, SPAN - 1, i], {"tp": sib})

            each(0, teams, handed)

        @pl.when(z != center)
        def _():
            sent(mpair, m_send.at[0], {"sp": center})

    for n, xx in enumerate((xo, xl, xr)):
        for k in range(2):
            cols = pl.ds(pl.multiple_of((xx * 2 + k) * width, LANES), width)
            recv(out.at[:, cols], y_recv.at[2 * n + k], {"tp": xx * 2 + k})
    recv(out.at[:, pl.ds(pl.multiple_of(sib * width, LANES), width)], y_recv.at[6], {"tp": sib})
    keep.wait()
    gates.wait()
    for copy in started[before:]:
        copy.wait_send()


def local(n_sp, n_tp, latent, context, conditioning, norm_gain, *rest):
    shift_w, scale_w, gate_w, q_w, k_w, v_w, o_w, sink = rest
    group, depth = latent.shape
    n_ctx = context.shape[0]
    count = n_tp * group
    width = shift_w.shape[1]
    blocks = count // WIN
    chunks = group // 16
    row_tab, col_tab = rope_tables(n_sp * count // GRID_W)
    any_space = pl.BlockSpec(memory_space=pl.ANY)
    dma = pltpu.SemaphoreType.DMA
    blended, gate = pl.pallas_call(
        functools.partial(kernel, n_sp, n_tp),
        out_shape=(jax.ShapeDtypeStruct((group, depth), bf16), jax.ShapeDtypeStruct((1, depth), f32)),
        in_specs=[any_space] * 14,
        out_specs=(any_space, any_space),
        scratch_shapes=[
            pltpu.VMEM((n_tp, group, depth), bf16),
            pltpu.VMEM((depth, 2 * LANES), bf16),
            pltpu.VMEM((2 * HD, depth), bf16),
            pltpu.VMEM(o_w.shape, bf16),
            pltpu.VMEM((3, *shift_w.shape), bf16),
            pltpu.VMEM((n_ctx, depth), bf16),
            pltpu.VMEM((2, n_sp, n_ctx, LANES), bf16),
            pltpu.VMEM((n_ctx, LANES), bf16),
            pltpu.VMEM((2, n_ctx, LANES), bf16),
            pltpu.VMEM((2, 16, LANES), f32),
            pltpu.VMEM((n_sp, 2, 16, LANES), f32),
            pltpu.VMEM((2, 16, LANES), f32),
            pltpu.VMEM((n_tp // 2, 2, 16, LANES), f32),
            pltpu.VMEM((n_tp, group, LANES), f32),
            pltpu.VMEM((1, depth), f32),
            pltpu.VMEM((1, depth), f32),
            pltpu.VMEM((1, depth), f32),
            pltpu.VMEM((count, LANES), bf16),
            pltpu.VMEM((count + 2 * WIN, LANES), bf16),
            pltpu.VMEM((n_sp * n_ctx, LANES), bf16),
            pltpu.VMEM((n_tp, count, LANES), bf16),
            pltpu.VMEM((n_tp, group, width), bf16),
            pltpu.VMEM((count // GRID_W, 4 * LANES), f32),
            pltpu.VMEM((GRID_W, 4 * LANES), f32),
            pltpu.VMEM((1, conditioning.shape[0]), bf16),
            pltpu.VMEM((1, depth), f32),
            pltpu.VMEM((1, sink.shape[0]), f32),
            pltpu.SemaphoreType.REGULAR,
            dma((16,)),
            dma((3,)),
            dma((3,)),
            dma((1,)),
            dma((n_sp,)),
            dma((n_sp,)),
            dma,
            dma((1,)),
            dma((SPAN,)),
            dma((n_sp // SPAN,)),
            dma((n_sp // SPAN,)),
            dma((2, SPAN, n_sp // SPAN)),
            dma((6, chunks)),
            dma((6, chunks)),
            dma((n_tp,)),
            dma((n_tp,)),
            dma((3,)),
            dma((n_tp // 2,)),
            dma,
            dma,
            dma((2,)),
            dma((2,)),
            dma((3, blocks)),
            dma((3, blocks)),
            dma((4, blocks)),
            dma((4, blocks)),
            dma((8,)),
            dma((8,)),
        ],
        compiler_params=pltpu.CompilerParams(
            collective_id=0, has_side_effects=True, vmem_limit_bytes=56 * 1024 * 1024
        ),
    )(
        latent,
        context,
        conditioning.reshape(1, -1),
        norm_gain.reshape(1, -1),
        shift_w,
        scale_w,
        gate_w,
        q_w,
        k_w.T,
        v_w.T,
        o_w,
        sink.reshape(1, -1),
        jnp.asarray(row_tab),
        jnp.asarray(col_tab),
    )
    return (latent.astype(f32) + gate * blended.astype(f32)).astype(bf16)


def solution(mesh):
    in_specs = (
        P(("grp", "sp", "tp"), None),
        P(("grp", "sp"), None),
        P(("grp", "sp")),
        P(),
        P("sp", "tp"),
        P("sp", "tp"),
        P("sp", "tp"),
        P(None, "tp"),
        P(None, "tp"),
        P(None, "tp"),
        P(None, "tp"),
        P("tp"),
    )
    return jax.shard_map(
        functools.partial(local, mesh.shape["sp"], mesh.shape["tp"]),
        mesh=mesh,
        in_specs=in_specs,
        out_specs=P(("grp", "sp", "tp"), None),
        check_vma=False,
    )
```

```python
import functools

import jax
import jax.numpy as jnp
import numpy as np
from jax import lax
from jax.experimental import pallas as pl
from jax.experimental.pallas import tpu as pltpu
from jax.sharding import PartitionSpec as P

HEADS = 16
KV_HEADS = 8
HD = 64
GRID_W = 64
WIN = 128
SPAN = 4
LATEST = 4
LANES = 128
COLS = 512

epsilon = 1e-06
rope_base = 10000.0
neg_large = -1e30
MESH = pl.DeviceIdType.MESH
f32 = jnp.float32
bf16 = jnp.bfloat16


def rope_tables(grid_rows):
    lane = np.arange(LANES)
    d = lane % HD
    freq = rope_base ** (-(d % 16) / 16.0)
    is_row = d < HD // 2
    sign = np.where(d % 32 < 16, -1.0, 1.0)
    is_key = lane < HD

    def table(count, own):
        angle = np.arange(count)[:, None] * freq[None, :]
        c = np.where(own, np.cos(angle), 0.0)
        s = np.where(own, np.sin(angle) * sign, 0.0)
        scale = HD**-0.5
        ck = np.where(is_key, c, 0.0)
        sk = np.where(is_key, s, 0.0)
        return np.concatenate([c * scale, s * scale, ck, sk], axis=1)

    rows = table(grid_rows, is_row)
    cols = table(GRID_W, ~is_row)
    cols[:, 2 * LANES : 3 * LANES] += np.where(is_key, 0.0, 1.0)
    return rows.astype(np.float32), cols.astype(np.float32)


def kernel(
    n_sp,
    n_tp,
    latent,
    context,
    cond_in,
    gain_in,
    shift_w,
    scale_w,
    gate_w,
    q_w,
    k_t,
    v_t,
    o_w,
    sink_in,
    row_tab,
    col_tab,
    out,
    gate_out,
    rows,
    w,
    kvt,
    ow,
    mw,
    ctx_rows,
    cg,
    cown,
    cpair,
    mpair,
    mall,
    msum,
    mt,
    inv,
    a_vec,
    s_vec,
    g_vec,
    qrot,
    kv,
    ctx,
    att,
    ysend,
    rt,
    ct,
    cond,
    gain,
    sink,
    hello,
    load_sem,
    pair_send,
    pair_recv,
    m_send,
    m_recv,
    tot_send,
    tot_recv,
    c_send,
    p_recv,
    b_recv,
    bl_send,
    bm_send,
    ag_send,
    ag_recv,
    sib_send,
    sib_recv,
    x_send,
    x_recv,
    h_send,
    h_recv,
    t_send,
    t_recv,
    tsib_send,
    tsib_recv,
    y_send,
    y_recv,
):
    n_x = n_tp // 2
    z = lax.axis_index("sp")
    t = lax.axis_index("tp")
    x = t // 2
    c = t % 2
    xr = (x + 1) % n_x
    xl = (x + n_x - 1) % n_x
    xo = (x + 2) % n_x
    sib = x * 2 + (1 - c)
    t_r, t_l, t_o = xr * 2 + c, xl * 2 + c, xo * 2 + c
    group = latent.shape[0]
    count = n_tp * group
    depth = latent.shape[1]
    chunks = group // 16
    width = shift_w.shape[1]
    per = width // LANES

    late = (z == 0) & (x == 0)
    center = 1

    started = []

    def send(src, dst, ss, rs, dev, keep=True):
        copy = pltpu.make_async_remote_copy(
            src_ref=src, dst_ref=dst, send_sem=ss, recv_sem=rs, device_id=dev, device_id_type=MESH
        )
        copy.start()
        if keep:
            started.append(copy)

    def recv(dst, rs, dev):
        pltpu.make_async_remote_copy(
            src_ref=dst, dst_ref=dst, send_sem=rs, recv_sem=rs, device_id=dev, device_id_type=MESH
        ).wait_recv()

    def sent(src, ss, dev):
        pltpu.make_async_remote_copy(
            src_ref=src, dst_ref=src, send_sem=ss, recv_sem=ss, device_id=dev, device_id_type=MESH
        ).wait_send()

    def each(lo, hi, body):
        def step(i, carry):
            body(i)
            return carry

        lax.fori_loop(lo, hi, step, 0)

    barrier = pltpu.get_barrier_semaphore()

    def greet(dev):
        pl.semaphore_signal(barrier, inc=1, device_id=dev, device_id_type=MESH)

    @pl.when(c == 1)
    def _():
        for who in (sib, t_l):
            greet({"tp": who})

    lead = SPAN * (z // SPAN) + center
    members = [(z // SPAN) * SPAN + j for j in range(SPAN) if j != center]
    teams = n_sp // SPAN
    team = z // SPAN

    @pl.when((c == 0) & (z == center))
    def _():
        each(0, center, lambda i: greet({"sp": i}))
        each(center + 1, n_sp, lambda i: greet({"sp": i}))

    @pl.when((c == 0) & (z == lead))
    def _():
        for i in members:
            greet({"sp": i})
        each(team + 1, teams, lambda i: greet({"sp": SPAN * i + center}))

    grid_rows = count // GRID_W
    loads = {}

    def load(name, src, dst):
        copy = pltpu.make_async_copy(src, dst, load_sem.at[len(loads)])
        copy.start()
        loads[name] = copy

    load("cond", cond_in, cond)
    load("m0", shift_w, mw.at[0])
    load("m1", scale_w, mw.at[1])
    load("m2", gate_w, mw.at[2])
    load("rows", latent, rows.at[t])
    load("gain", gain_in, gain)
    load("kw", k_t, kvt.at[pl.ds(0, HD)])
    load("vw", v_t, kvt.at[pl.ds(HD, HD)])
    load("ctx", context, ctx_rows)
    load("qw", q_w, w.at[:, pl.ds(0, LANES)])
    load("rt", row_tab.at[pl.ds(pl.multiple_of(z * grid_rows, 8), grid_rows)], rt)
    load("ct", col_tab, ct)
    load("sink", sink_in, sink)
    load("ow", o_w, ow)

    def contact():
        pl.semaphore_wait(barrier, 1 + jnp.where(z == center, 0, 1) + jnp.where(z == lead, team, 1))

    def modulation():
        loads["cond"].wait()
        cv = cond[...].astype(f32)
        lifted = jnp.broadcast_to((cv / (1.0 + jnp.exp(-cv))).astype(bf16), (16, cv.shape[1]))
        for i in range(3):
            loads["m%d" % i].wait()
            part = jnp.dot(lifted, mw[i], preferred_element_type=f32)
            for j in range(per):
                mpair[c, per * i + j : per * i + j + 1, :] = part[0:1, j * LANES : (j + 1) * LANES]
        mpair[c, 3 * per : 16, :] = jnp.zeros((16 - 3 * per, LANES), f32)

    n_ctx = ctx_rows.shape[0]

    def own_context():
        for name in ("kw", "vw", "gain", "ctx"):
            loads[name].wait()
        for i in range(depth // COLS):
            w[i * COLS : (i + 1) * COLS, LANES : 2 * LANES] = kvt[:, i * COLS : (i + 1) * COLS].T
        sq = jnp.zeros((n_ctx, LANES), f32)
        for i in range(depth // LANES):
            v = ctx_rows[:, i * LANES : (i + 1) * LANES].astype(f32)
            sq = sq + v * v
        cinv = lax.rsqrt(jnp.sum(sq, axis=1, keepdims=True) * (1.0 / depth) + epsilon)
        acc = jnp.zeros((n_ctx, LANES), f32)
        for i in range(depth // COLS):
            part = slice(i * COLS, (i + 1) * COLS)
            v = ctx_rows[:, part].astype(f32) * cinv * gain[:, part]
            acc = acc + jnp.dot(v.astype(bf16), w[part, LANES : 2 * LANES], preferred_element_type=f32)
        cown[...] = acc.astype(bf16)

    def row_stats(g):
        sq = jnp.zeros((group, LANES), f32)
        for i in range(depth // LANES):
            v = rows[g, :, i * LANES : (i + 1) * LANES].astype(f32)
            sq = sq + v * v
        r = lax.rsqrt(jnp.sum(sq, axis=1, keepdims=True) * (1.0 / depth) + epsilon)
        inv[g] = jnp.broadcast_to(r, (group, LANES))

    @pl.when(z == 0)
    def _():
        kv[:WIN, :] = jnp.zeros((WIN, LANES), bf16)

    @pl.when(z == n_sp - 1)
    def _():
        kv[WIN + count :, :] = jnp.zeros((WIN, LANES), bf16)

    def piece(g, q):
        return rows.at[g, pl.ds(16 * q, 16)]

    zero_l, zero_r, zero_o = t_l - c, t_r - c, t_o - c

    def meet():
        pl.semaphore_wait(hello, 1)
        send(mpair.at[1], mpair.at[1], pair_send.at[0], pair_recv.at[0], {"tp": sib}, False)

    def hand_context():
        send(cown, cpair.at[1], pair_send.at[1], pair_recv.at[1], {"tp": sib}, False)

    def sibling_rows():
        recv(rows.at[sib], sib_recv.at[sib], {"tp": sib})
        for q in range(chunks):
            send(piece(sib, q), piece(sib, q), ag_send.at[2], ag_recv.at[2, q], {"tp": t_r}, False)
            send(piece(sib, q), piece(sib, q), ag_send.at[3], ag_recv.at[3, q], {"tp": t_l}, False)

    def hand(groups):
        for g in groups:
            send(rows.at[g], rows.at[g], sib_send.at[g], sib_recv.at[g], {"tp": sib}, False)

    def own_block(k, i):
        return cg.at[k, pl.ds(SPAN * i, SPAN)]

    @pl.when(c == 1)
    def _():
        modulation()
        loads["rows"].wait()
        pl.semaphore_wait(barrier, 1)
        pl.when(~late & (z >= n_sp // 2))(meet)
        for q in range(chunks):
            send(piece(t, q), piece(t, q), ag_send.at[0], ag_recv.at[0, q], {"tp": t_r}, False)
        own_context()
        recv(piece(t_l, 0), ag_recv.at[0, 0], {"tp": t_l})
        for q in range(chunks):
            send(piece(t, q), piece(t, q), ag_send.at[1], ag_recv.at[1, q], {"tp": t_l}, False)
        pl.when(~late & (z < n_sp // 2))(meet)
        pl.when(~late)(hand_context)
        pl.when(~late)(sibling_rows)
        for q in range(chunks):
            recv(piece(t_r, q), ag_recv.at[1, q], {"tp": t_r})
            send(piece(t_r, q), piece(t_r, q), ag_send.at[4], ag_recv.at[4, q], {"tp": t_l}, False)
        for q in range(1, chunks):
            recv(piece(t_l, q), ag_recv.at[0, q], {"tp": t_l})
        pl.when(~late)(functools.partial(hand, (t, t_r, t_l)))
        row_stats(t)
        row_stats(t_l)
        row_stats(t_r)
        for q in range(chunks):
            recv(piece(zero_l, q), ag_recv.at[2, q], {"tp": t_l})
            send(piece(zero_l, q), piece(zero_l, q), ag_send.at[5], ag_recv.at[5, q], {"tp": t_r}, False)
        for q in range(chunks):
            recv(piece(zero_r, q), ag_recv.at[3, q], {"tp": t_r})
        pl.when(~late)(functools.partial(hand, (zero_l, zero_r)))
        row_stats(zero_l)
        row_stats(zero_r)
        for q in range(chunks):
            recv(piece(t_o, q), ag_recv.at[4, q], {"tp": t_r})
        pl.when(~late)(functools.partial(hand, (t_o,)))
        row_stats(t_o)
        for q in range(chunks):
            recv(piece(zero_o, q), ag_recv.at[5, q], {"tp": t_l})
        pl.when(~late)(functools.partial(hand, (zero_o,)))
        row_stats(zero_o)

        @pl.when(late)
        def _():
            meet()
            hand_context()
            sibling_rows()
            hand((t, t_r, t_l, zero_l, zero_r, t_o, zero_o))

        row_stats(sib)
        recv(mt.at[x], x_recv.at[x], {"tp": sib})
        for n, (xx, who) in enumerate(((xr, zero_r), (xl, zero_l), (xo, zero_o))):
            recv(mt.at[xx], x_recv.at[xx], {"tp": who})
            send(mt.at[xx], mt.at[xx], x_send.at[n], x_recv.at[xx], {"tp": sib}, False)

    @pl.when(c == 0)
    def _():
        modulation()
        loads["rows"].wait()
        contact()
        pl.semaphore_signal(hello, inc=1, device_id={"tp": sib}, device_id_type=MESH)
        send(rows.at[t], rows.at[t], sib_send.at[t], sib_recv.at[t], {"tp": sib}, False)
        recv(mpair.at[1], pair_recv.at[0], {"tp": sib})

        @pl.when(z != center)
        def _():
            send(mpair, mall.at[z - jnp.where(z > center, 1, 0)], m_send.at[0], m_recv, {"sp": center}, False)

        own_context()
        cpair[0] = cown[...]
        row_stats(t)
        recv(cpair.at[1], pair_recv.at[1], {"tp": sib})

        def block(i):
            return cg.at[:, pl.ds(SPAN * i, SPAN)]

        def tell_sum():
            recv(mall, m_recv, {"sp": 0})
            tot = mpair[...]
            for i in range(n_sp - 1):
                tot = tot + mall[i]
            msum[...] = tot

            def tell(i):
                send(msum, mt.at[x], tot_send, tot_recv, {"sp": i}, False)

            each(0, center, tell)
            each(center + 1, n_sp, tell)
            mt[x] = tot

        def sum_in():
            recv(mt.at[x], tot_recv, {"sp": center})

        def rows_in(groups):
            for g in groups:
                recv(rows.at[g], sib_recv.at[g], {"tp": sib})
                row_stats(g)

        def early_rows():
            rows_in((sib, t_r + 1, t_l + 1))

        @pl.when(z != lead)
        def _():
            send(cpair, cg.at[:, z], c_send.at[0], p_recv.at[z % SPAN], {"sp": lead}, False)

        def hand_block(i):
            for n, who in enumerate(members):
                for k in range(2):
                    send(own_block(k, i), own_block(k, i), bm_send.at[2 * n + k], b_recv.at[i], {"sp": who, "tp": t + k}, False)
            send(own_block(1, i), own_block(1, i), bm_send.at[2 * SPAN - 2], b_recv.at[i], {"tp": sib}, False)

        def give(i):
            send(block(team), block(team), bl_send.at[i], b_recv.at[team], {"sp": SPAN * i + center}, False)

        def got(i):
            recv(block(i), b_recv.at[i], {"sp": SPAN * i + center})

        def answer(i):
            got(i)
            give(i)
            hand_block(i)

        def follow(i):
            got(i)
            hand_block(i)

        tail = jnp.where(z == center, teams - LATEST, teams)
        pl.when(z == center)(early_rows)

        @pl.when(z == lead)
        def _():
            for k in range(2):
                cg[k, z] = cpair[k]
            for n, i in enumerate(members):
                recv(cg.at[:, i], p_recv.at[n + (1 if n >= center else 0)], {"sp": i})
            each(0, team, give)
            hand_block(team)
            each(team + 1, tail, answer)

        pl.when(z != center)(early_rows)
        pl.when(z == center)(tell_sum)
        pl.when(z != center)(sum_in)
        for n, who in enumerate((sib, t_o + 1, t_r + 1, t_l + 1)):
            send(mt.at[x], mt.at[x], x_send.at[n], x_recv.at[x], {"tp": who}, False)

        @pl.when(z == lead)
        def _():
            each(tail, teams, answer)
            each(0, team, follow)

        rows_in((t_o + 1, t_r, t_l, t_o))
        for xx in (xr, xl, xo):
            recv(mt.at[xx], x_recv.at[xx], {"tp": sib})

    for j in range(n_tp):
        for i in range(per):
            part = slice(j * width + i * LANES, j * width + (i + 1) * LANES)
            s_vec[:, part] = mt[j // 2, j % 2, i : i + 1, :]
            a_vec[:, part] = gain[:, part] * (1.0 + mt[j // 2, j % 2, per + i : per + i + 1, :])
            g_vec[:, part] = mt[j // 2, j % 2, 2 * per + i : 2 * per + i + 1, :]
    gates = pltpu.make_async_copy(g_vec, gate_out, load_sem.at[15])
    gates.start()
    for name in ("rt", "ct", "qw", "ow", "sink"):
        loads[name].wait()

    lane = lax.broadcasted_iota(jnp.int32, (1, LANES), 1)
    first = lane % 32 < 16

    def swapped(v):
        return jnp.where(first, pltpu.roll(v, LANES - 16, 1), pltpu.roll(v, 16, 1))

    def project(gs):
        acc = jnp.zeros((len(gs) * group, 2 * LANES), f32)
        for i in range(depth // COLS):
            part = slice(i * COLS, (i + 1) * COLS)
            a = a_vec[:, part]
            s = s_vec[:, part]
            tiles = []
            for g in gs:
                r = jnp.concatenate([inv[g]] * (COLS // LANES), axis=1)
                tiles.append((rows[g, :, part].astype(f32) * r * a + s).astype(bf16))
            acc = acc + jnp.dot(jnp.concatenate(tiles, axis=0), w[part, :], preferred_element_type=f32)
        for n, g in enumerate(gs):
            fac = rt[g : g + 1, :] + ct[...]
            vq = acc[n * group : (n + 1) * group, :LANES]
            vk = acc[n * group : (n + 1) * group, LANES:]
            q2 = vq * fac[:, :LANES] + swapped(vq) * fac[:, LANES : 2 * LANES]
            k2 = vk * fac[:, 2 * LANES : 3 * LANES] + swapped(vk) * fac[:, 3 * LANES :]
            qrot[g * group : (g + 1) * group, :] = q2.astype(bf16)
            kv[WIN + g * group : WIN + (g + 1) * group, :] = k2.astype(bf16)

    project((0, 1, n_tp - 2, n_tp - 1))

    @pl.when(z > 0)
    def _():
        send(kv.at[pl.ds(WIN, WIN)], kv.at[pl.ds(WIN + count, WIN)], h_send.at[0], h_recv.at[0], {"sp": z - 1}, False)

    @pl.when(z < n_sp - 1)
    def _():
        send(kv.at[pl.ds(count, WIN)], kv.at[pl.ds(0, WIN)], h_send.at[1], h_recv.at[1], {"sp": z + 1}, False)

    project(tuple(range(2, n_tp - 2)))

    @pl.when((c == 1) | (z != lead))
    def _():
        for i in range(n_sp // SPAN):
            recv(own_block(c, i), b_recv.at[i], {"sp": lead, "tp": t - c})

    for j in range(n_sp):
        ctx[pl.ds(j * n_ctx, n_ctx), :] = cg[c, j]
    rows2 = 2 * WIN
    qi = lax.broadcasted_iota(jnp.int32, (rows2, WIN), 0) % WIN
    ki = lax.broadcasted_iota(jnp.int32, (rows2, WIN), 1)
    head1 = lax.broadcasted_iota(jnp.int32, (rows2, 1), 0) >= WIN
    sink_col = jnp.where(head1, sink[0:1, 1:2], sink[0:1, 0:1])
    is_key = lane < HD
    contract = (((1,), (1,)), ((), ()))
    blocks = count // WIN

    def attend(b):
        qb = qrot[b * WIN : (b + 1) * WIN, :].astype(f32)
        q0 = jnp.where(is_key, qb, 0.0).astype(bf16)
        q1 = jnp.where(is_key, pltpu.roll(qb, HD, 1), 0.0).astype(bf16)
        qq = jnp.concatenate([q0, q1], axis=0)
        band = kv[b * WIN : (b + 3) * WIN, :]
        whole = ctx[...]
        s_band = lax.dot_general(qq, band, contract, preferred_element_type=f32)
        s_ctx = lax.dot_general(qq, whole, contract, preferred_element_type=f32)
        left = ki >= qi
        right = ki <= qi
        if b == 0:
            left = left & (z > 0)
        if b == blocks - 1:
            right = right & (z < n_sp - 1)
        s0 = jnp.where(left, s_band[:, :WIN], neg_large)
        s1 = s_band[:, WIN : 2 * WIN]
        s2 = jnp.where(right, s_band[:, 2 * WIN :], neg_large)
        top = jnp.maximum(jnp.maximum(s0, s1), s2)
        for i in range(whole.shape[0] // LANES):
            top = jnp.maximum(top, s_ctx[:, i * LANES : (i + 1) * LANES])
        m = jnp.maximum(jnp.max(top, axis=1, keepdims=True), sink_col)
        e0 = jnp.exp(s0 - m)
        e1 = jnp.exp(s1 - m)
        e2 = jnp.exp(s2 - m)
        ec = jnp.exp(s_ctx - m)
        tot = e0 + e1 + e2
        for i in range(whole.shape[0] // LANES):
            tot = tot + ec[:, i * LANES : (i + 1) * LANES]
        den = jnp.sum(tot, axis=1, keepdims=True) + jnp.exp(sink_col - m)
        r = 1.0 / den
        p_band = jnp.concatenate([e0, e1, e2], axis=1) * r
        o = jnp.dot(p_band.astype(bf16), band, preferred_element_type=f32) + jnp.dot(
            (ec * r).astype(bf16), whole, preferred_element_type=f32
        )
        res = jnp.where(is_key, pltpu.roll(o[:WIN], HD, 1), o[WIN:]).astype(bf16)
        att[t, b * WIN : (b + 1) * WIN, :] = res

    def att_piece(who, b):
        return att.at[who, pl.ds(b * WIN, WIN)]

    def att_send(b):
        mine = att_piece(t, b)
        send(mine, mine, t_send.at[2], t_recv.at[2, b], {"tp": t_o}, False)
        send(mine, mine, t_send.at[0], t_recv.at[0, b], {"tp": t_r}, False)
        send(mine, mine, t_send.at[1], t_recv.at[1, b], {"tp": t_l}, False)
        send(mine, mine, tsib_send.at[0], tsib_recv.at[0], {"tp": sib}, False)

    def att_take(b):
        for role, who in ((0, t_l), (1, t_r), (2, t_o)):
            got = att_piece(who, b)
            recv(got, t_recv.at[role, b], {"tp": who})
            send(got, got, tsib_send.at[1 + role], tsib_recv.at[1 + role], {"tp": sib}, False)

    order = [*range(1, blocks - 1), 0, blocks - 1]
    for n, b in enumerate(order):
        if n == blocks - 2:
            @pl.when(z < n_sp - 1)
            def _():
                recv(kv.at[pl.ds(WIN + count, WIN)], h_recv.at[0], {"sp": z + 1})

            @pl.when(z > 0)
            def _():
                recv(kv.at[pl.ds(0, WIN)], h_recv.at[1], {"sp": z - 1})

        attend(b)
        att_send(b)
        if n >= 2:
            att_take(order[n - 2])
    att_take(order[-2])
    att_take(order[-1])
    for role, xx in ((0, x), (1, xl), (2, xr), (3, xo)):
        recv(att.at[xx * 2 + 1 - c], tsib_recv.at[role], {"tp": sib})

    before = len(started)
    here = pl.ds(pl.multiple_of(t * width, LANES), width)
    for n, xx in enumerate((xo, xr, xl, x)):
        part = pl.ds(pl.multiple_of(xx * WIN, WIN), WIN)
        y = jnp.zeros((WIN, width), f32)
        for i in range(n_x):
            lhs = jnp.concatenate([att[2 * i, part, :], att[2 * i + 1, part, :]], axis=1)
            y = y + jnp.dot(lhs, ow[2 * i * LANES : 2 * (i + 1) * LANES, :], preferred_element_type=f32)
        ysend[2 * n] = y[:group].astype(bf16)
        ysend[2 * n + 1] = y[group:].astype(bf16)
        if n < 3:
            for k in range(2):
                send(ysend.at[2 * n + k], out.at[:, here], y_send.at[2 * n + k], y_recv.at[2 * n + c], {"tp": xx * 2 + k})
        else:
            send(ysend.at[2 * n + 1 - c], out.at[:, here], y_send.at[6], y_recv.at[6], {"tp": sib})
            keep = pltpu.make_async_copy(ysend.at[2 * n + c], out.at[:, here], load_sem.at[14])
            keep.start()
    for n, who in enumerate((t_r, t_l, t_o)):
        sent(att.at[t], t_send.at[n], {"tp": who})
    for n, who in enumerate((t, t_l, t_r, t_o)):
        sent(att.at[who], tsib_send.at[n], {"tp": sib})
    for copy in started[:before]:
        copy.wait_send()

    @pl.when(z > 0)
    def _():
        sent(kv.at[pl.ds(WIN, WIN)], h_send.at[0], {"sp": z - 1})

    @pl.when(z < n_sp - 1)
    def _():
        sent(kv.at[pl.ds(count, WIN)], h_send.at[1], {"sp": z + 1})

    @pl.when(c == 1)
    def _():
        for n, xx in enumerate((xr, xl, xo)):
            sent(mt.at[xx], x_send.at[n], {"tp": sib})
        sent(mpair.at[1], pair_send.at[0], {"tp": sib})
        sent(cown, pair_send.at[1], {"tp": sib})
        for n, (g, who) in enumerate(((t, t_r), (t, t_l), (sib, t_r), (sib, t_l), (t_r, t_l), (zero_l, t_r))):
            sent(rows.at[g], ag_send.at[n], {"tp": who})
        for g in (t, t_r, t_l, zero_l, zero_r, t_o, zero_o):
            sent(rows.at[g], sib_send.at[g], {"tp": sib})
    @pl.when(c == 0)
    def _():
        sent(rows.at[t], sib_send.at[t], {"tp": sib})
        for n, who in enumerate((sib, t_o + 1, t_r + 1, t_l + 1)):
            sent(mt.at[x], x_send.at[n], {"tp": who})

        @pl.when(z == center)
        def _():
            sent(mall, tot_send, {"sp": 0})

        @pl.when(z != lead)
        def _():
            sent(cpair, c_send.at[0], {"sp": lead})

        @pl.when(z == lead)
        def _():
            def given(i):
                sent(cg.at[:, pl.ds(SPAN * team, SPAN)], bl_send.at[i], {"sp": SPAN * i + center})

            each(0, team, given)
            each(team + 1, teams, given)

            for n, who in enumerate(members):
                for k in range(2):
                    sent(cg.at[k], bm_send.at[2 * n + k], {"sp": who})
            sent(cg.at[1], bm_send.at[2 * SPAN - 2], {"tp": sib})

        @pl.when(z != center)
        def _():
            sent(mpair, m_send.at[0], {"sp": center})

    for n, xx in enumerate((xo, xl, xr)):
        for k in range(2):
            cols = pl.ds(pl.multiple_of((xx * 2 + k) * width, LANES), width)
            recv(out.at[:, cols], y_recv.at[2 * n + k], {"tp": xx * 2 + k})
    recv(out.at[:, pl.ds(pl.multiple_of(sib * width, LANES), width)], y_recv.at[6], {"tp": sib})
    keep.wait()
    gates.wait()
    for copy in started[before:]:
        copy.wait_send()


def local(n_sp, n_tp, latent, context, conditioning, norm_gain, *rest):
    shift_w, scale_w, gate_w, q_w, k_w, v_w, o_w, sink = rest
    group, depth = latent.shape
    n_ctx = context.shape[0]
    count = n_tp * group
    width = shift_w.shape[1]
    blocks = count // WIN
    chunks = group // 16
    row_tab, col_tab = rope_tables(n_sp * count // GRID_W)
    any_space = pl.BlockSpec(memory_space=pl.ANY)
    dma = pltpu.SemaphoreType.DMA
    blended, gate = pl.pallas_call(
        functools.partial(kernel, n_sp, n_tp),
        out_shape=(jax.ShapeDtypeStruct((group, depth), bf16), jax.ShapeDtypeStruct((1, depth), f32)),
        in_specs=[any_space] * 14,
        out_specs=(any_space, any_space),
        scratch_shapes=[
            pltpu.VMEM((n_tp, group, depth), bf16),
            pltpu.VMEM((depth, 2 * LANES), bf16),
            pltpu.VMEM((2 * HD, depth), bf16),
            pltpu.VMEM(o_w.shape, bf16),
            pltpu.VMEM((3, *shift_w.shape), bf16),
            pltpu.VMEM((n_ctx, depth), bf16),
            pltpu.VMEM((2, n_sp, n_ctx, LANES), bf16),
            pltpu.VMEM((n_ctx, LANES), bf16),
            pltpu.VMEM((2, n_ctx, LANES), bf16),
            pltpu.VMEM((2, 16, LANES), f32),
            pltpu.VMEM((n_sp - 1, 2, 16, LANES), f32),
            pltpu.VMEM((2, 16, LANES), f32),
            pltpu.VMEM((n_tp // 2, 2, 16, LANES), f32),
            pltpu.VMEM((n_tp, group, LANES), f32),
            pltpu.VMEM((1, depth), f32),
            pltpu.VMEM((1, depth), f32),
            pltpu.VMEM((1, depth), f32),
            pltpu.VMEM((count, LANES), bf16),
            pltpu.VMEM((count + 2 * WIN, LANES), bf16),
            pltpu.VMEM((n_sp * n_ctx, LANES), bf16),
            pltpu.VMEM((n_tp, count, LANES), bf16),
            pltpu.VMEM((n_tp, group, width), bf16),
            pltpu.VMEM((count // GRID_W, 4 * LANES), f32),
            pltpu.VMEM((GRID_W, 4 * LANES), f32),
            pltpu.VMEM((1, conditioning.shape[0]), bf16),
            pltpu.VMEM((1, depth), f32),
            pltpu.VMEM((1, sink.shape[0]), f32),
            pltpu.SemaphoreType.REGULAR,
            dma((16,)),
            dma((3,)),
            dma((3,)),
            dma((1,)),
            dma,
            dma,
            dma,
            dma((1,)),
            dma((SPAN,)),
            dma((n_sp // SPAN,)),
            dma((n_sp // SPAN,)),
            dma((2 * SPAN,)),
            dma((6,)),
            dma((6, chunks)),
            dma((n_tp,)),
            dma((n_tp,)),
            dma((4,)),
            dma((n_tp // 2,)),
            dma((2,)),
            dma((2,)),
            dma((3,)),
            dma((3, blocks)),
            dma((4,)),
            dma((4,)),
            dma((8,)),
            dma((8,)),
        ],
        compiler_params=pltpu.CompilerParams(
            collective_id=0, has_side_effects=True, vmem_limit_bytes=56 * 1024 * 1024
        ),
    )(
        latent,
        context,
        conditioning.reshape(1, -1),
        norm_gain.reshape(1, -1),
        shift_w,
        scale_w,
        gate_w,
        q_w,
        k_w.T,
        v_w.T,
        o_w,
        sink.reshape(1, -1),
        jnp.asarray(row_tab),
        jnp.asarray(col_tab),
    )
    return (latent.astype(f32) + gate * blended.astype(f32)).astype(bf16)


def solution(mesh):
    in_specs = (
        P(("grp", "sp", "tp"), None),
        P(("grp", "sp"), None),
        P(("grp", "sp")),
        P(),
        P("sp", "tp"),
        P("sp", "tp"),
        P("sp", "tp"),
        P(None, "tp"),
        P(None, "tp"),
        P(None, "tp"),
        P(None, "tp"),
        P("tp"),
    )
    return jax.shard_map(
        functools.partial(local, mesh.shape["sp"], mesh.shape["tp"]),
        mesh=mesh,
        in_specs=in_specs,
        out_specs=P(("grp", "sp", "tp"), None),
        check_vma=False,
    )
```

```python
import functools

import jax
import jax.numpy as jnp
import numpy as np
from jax import lax
from jax.experimental import pallas as pl
from jax.experimental.pallas import tpu as pltpu
from jax.sharding import PartitionSpec as P

HEADS = 16
KV_HEADS = 8
HD = 64
GRID_W = 64
WIN = 128
SPAN = 4
LATEST = 4
LANES = 128
COLS = 512

epsilon = 1e-06
rope_base = 10000.0
neg_large = -1e30
MESH = pl.DeviceIdType.MESH
f32 = jnp.float32
bf16 = jnp.bfloat16


def rope_tables(grid_rows):
    lane = np.arange(LANES)
    d = lane % HD
    freq = rope_base ** (-(d % 16) / 16.0)
    is_row = d < HD // 2
    sign = np.where(d % 32 < 16, -1.0, 1.0)
    is_key = lane < HD

    def table(count, own):
        angle = np.arange(count)[:, None] * freq[None, :]
        c = np.where(own, np.cos(angle), 0.0)
        s = np.where(own, np.sin(angle) * sign, 0.0)
        scale = HD**-0.5
        ck = np.where(is_key, c, 0.0)
        sk = np.where(is_key, s, 0.0)
        return np.concatenate([c * scale, s * scale, ck, sk], axis=1)

    rows = table(grid_rows, is_row)
    cols = table(GRID_W, ~is_row)
    cols[:, 2 * LANES : 3 * LANES] += np.where(is_key, 0.0, 1.0)
    return rows.astype(np.float32), cols.astype(np.float32)


def kernel(
    n_sp,
    n_tp,
    latent,
    context,
    cond_in,
    gain_in,
    shift_w,
    scale_w,
    gate_w,
    q_w,
    k_t,
    v_t,
    o_w,
    sink_in,
    row_tab,
    col_tab,
    out,
    gate_out,
    rows,
    w,
    kvt,
    ow,
    mw,
    ctx_rows,
    cg,
    cown,
    cpair,
    mpair,
    mall,
    msum,
    mt,
    inv,
    a_vec,
    s_vec,
    g_vec,
    qrot,
    kv,
    ctx,
    att,
    ysend,
    rt,
    ct,
    cond,
    gain,
    sink,
    hello,
    load_sem,
    pair_send,
    pair_recv,
    m_send,
    m_recv,
    tot_send,
    tot_recv,
    c_send,
    p_recv,
    b_recv,
    bl_send,
    bm_send,
    ag_send,
    ag_recv,
    sib_send,
    sib_recv,
    x_send,
    x_recv,
    h_send,
    h_recv,
    t_send,
    t_recv,
    tsib_send,
    tsib_recv,
    y_send,
    y_recv,
):
    n_x = n_tp // 2
    z = lax.axis_index("sp")
    t = lax.axis_index("tp")
    x = t // 2
    c = t % 2
    xr = (x + 1) % n_x
    xl = (x + n_x - 1) % n_x
    xo = (x + 2) % n_x
    sib = x * 2 + (1 - c)
    t_r, t_l, t_o = xr * 2 + c, xl * 2 + c, xo * 2 + c
    group = latent.shape[0]
    count = n_tp * group
    depth = latent.shape[1]
    chunks = group // 16
    width = shift_w.shape[1]
    per = width // LANES

    late = (z == 0) & (x == 0)
    center = 1

    started = []

    def send(src, dst, ss, rs, dev, keep=True):
        copy = pltpu.make_async_remote_copy(
            src_ref=src, dst_ref=dst, send_sem=ss, recv_sem=rs, device_id=dev, device_id_type=MESH
        )
        copy.start()
        if keep:
            started.append(copy)

    def recv(dst, rs, dev):
        pltpu.make_async_remote_copy(
            src_ref=dst, dst_ref=dst, send_sem=rs, recv_sem=rs, device_id=dev, device_id_type=MESH
        ).wait_recv()

    def sent(src, ss, dev):
        pltpu.make_async_remote_copy(
            src_ref=src, dst_ref=src, send_sem=ss, recv_sem=ss, device_id=dev, device_id_type=MESH
        ).wait_send()

    def each(lo, hi, body):
        def step(i, carry):
            body(i)
            return carry

        lax.fori_loop(lo, hi, step, 0)

    barrier = pltpu.get_barrier_semaphore()

    def greet(dev):
        pl.semaphore_signal(barrier, inc=1, device_id=dev, device_id_type=MESH)

    @pl.when(c == 1)
    def _():
        for who in (sib, t_l):
            greet({"tp": who})

    slot = (z + 1) % n_sp
    teams = n_sp // SPAN
    team = slot // SPAN
    lead = SPAN * team + center
    members = [(z + n_sp - 1) % n_sp, (z + 1) % n_sp, (z + n_sp - 2) % n_sp]
    places = (1, 3, 0)

    @pl.when((c == 0) & (z == center))
    def _():
        each(0, center, lambda i: greet({"sp": i}))
        each(center + 1, n_sp, lambda i: greet({"sp": i}))

    @pl.when((c == 0) & (z == lead))
    def _():
        for i in members:
            greet({"sp": i})
        each(team + 1, teams, lambda i: greet({"sp": SPAN * i + center}))

    grid_rows = count // GRID_W
    loads = {}

    def load(name, src, dst):
        copy = pltpu.make_async_copy(src, dst, load_sem.at[len(loads)])
        copy.start()
        loads[name] = copy

    load("cond", cond_in, cond)
    load("m0", shift_w, mw.at[0])
    load("m1", scale_w, mw.at[1])
    load("m2", gate_w, mw.at[2])
    load("rows", latent, rows.at[t])
    load("gain", gain_in, gain)
    load("kw", k_t, kvt.at[pl.ds(0, HD)])
    load("vw", v_t, kvt.at[pl.ds(HD, HD)])
    load("ctx", context, ctx_rows)
    load("qw", q_w, w.at[:, pl.ds(0, LANES)])
    load("rt", row_tab.at[pl.ds(pl.multiple_of(z * grid_rows, 8), grid_rows)], rt)
    load("ct", col_tab, ct)
    load("sink", sink_in, sink)
    load("ow", o_w, ow)

    def contact():
        pl.semaphore_wait(barrier, 1 + jnp.where(z == center, 0, 1) + jnp.where(z == lead, team, 1))

    def modulation():
        loads["cond"].wait()
        cv = cond[...].astype(f32)
        lifted = jnp.broadcast_to((cv / (1.0 + jnp.exp(-cv))).astype(bf16), (16, cv.shape[1]))
        for i in range(3):
            loads["m%d" % i].wait()
            part = jnp.dot(lifted, mw[i], preferred_element_type=f32)
            for j in range(per):
                mpair[c, per * i + j : per * i + j + 1, :] = part[0:1, j * LANES : (j + 1) * LANES]
        mpair[c, 3 * per : 16, :] = jnp.zeros((16 - 3 * per, LANES), f32)

    n_ctx = ctx_rows.shape[0]

    def own_context():
        for name in ("kw", "vw", "gain", "ctx"):
            loads[name].wait()
        for i in range(depth // COLS):
            w[i * COLS : (i + 1) * COLS, LANES : 2 * LANES] = kvt[:, i * COLS : (i + 1) * COLS].T
        sq = jnp.zeros((n_ctx, LANES), f32)
        for i in range(depth // LANES):
            v = ctx_rows[:, i * LANES : (i + 1) * LANES].astype(f32)
            sq = sq + v * v
        cinv = lax.rsqrt(jnp.sum(sq, axis=1, keepdims=True) * (1.0 / depth) + epsilon)
        acc = jnp.zeros((n_ctx, LANES), f32)
        for i in range(depth // COLS):
            part = slice(i * COLS, (i + 1) * COLS)
            v = ctx_rows[:, part].astype(f32) * cinv * gain[:, part]
            acc = acc + jnp.dot(v.astype(bf16), w[part, LANES : 2 * LANES], preferred_element_type=f32)
        cown[...] = acc.astype(bf16)

    def row_stats(g):
        sq = jnp.zeros((group, LANES), f32)
        for i in range(depth // LANES):
            v = rows[g, :, i * LANES : (i + 1) * LANES].astype(f32)
            sq = sq + v * v
        r = lax.rsqrt(jnp.sum(sq, axis=1, keepdims=True) * (1.0 / depth) + epsilon)
        inv[g] = jnp.broadcast_to(r, (group, LANES))

    @pl.when(z == 0)
    def _():
        kv[:WIN, :] = jnp.zeros((WIN, LANES), bf16)

    @pl.when(z == n_sp - 1)
    def _():
        kv[WIN + count :, :] = jnp.zeros((WIN, LANES), bf16)

    def piece(g, q):
        return rows.at[g, pl.ds(16 * q, 16)]

    zero_l, zero_r, zero_o = t_l - c, t_r - c, t_o - c

    def meet():
        pl.semaphore_wait(hello, 1)
        send(mpair.at[1], mpair.at[1], pair_send.at[0], pair_recv.at[0], {"tp": sib}, False)

    def hand_context():
        send(cown, cpair.at[1], pair_send.at[1], pair_recv.at[1], {"tp": sib}, False)

    def sibling_rows():
        recv(rows.at[sib], sib_recv.at[sib], {"tp": sib})
        for q in range(chunks):
            send(piece(sib, q), piece(sib, q), ag_send.at[2], ag_recv.at[2, q], {"tp": t_r}, False)
            send(piece(sib, q), piece(sib, q), ag_send.at[3], ag_recv.at[3, q], {"tp": t_l}, False)

    def hand(groups):
        for g in groups:
            send(rows.at[g], rows.at[g], sib_send.at[g], sib_recv.at[g], {"tp": sib}, False)

    def own_block(k, i):
        return cg.at[k, pl.ds(SPAN * i, SPAN)]

    @pl.when(c == 1)
    def _():
        modulation()
        loads["rows"].wait()
        pl.semaphore_wait(barrier, 1)
        pl.when(~late & (z >= n_sp // 2))(meet)
        for q in range(chunks):
            send(piece(t, q), piece(t, q), ag_send.at[0], ag_recv.at[0, q], {"tp": t_r}, False)
        own_context()
        pl.when(~late & (z >= n_sp // 2))(hand_context)
        recv(piece(t_l, 0), ag_recv.at[0, 0], {"tp": t_l})
        for q in range(chunks):
            send(piece(t, q), piece(t, q), ag_send.at[1], ag_recv.at[1, q], {"tp": t_l}, False)
        pl.when(~late & (z < n_sp // 2))(meet)
        pl.when(~late & (z < n_sp // 2))(hand_context)
        pl.when(~late)(sibling_rows)
        for q in range(chunks):
            recv(piece(t_r, q), ag_recv.at[1, q], {"tp": t_r})
            send(piece(t_r, q), piece(t_r, q), ag_send.at[4], ag_recv.at[4, q], {"tp": t_l}, False)
        for q in range(1, chunks):
            recv(piece(t_l, q), ag_recv.at[0, q], {"tp": t_l})
        pl.when(~late)(functools.partial(hand, (t, t_r, t_l)))
        row_stats(t)
        row_stats(t_l)
        row_stats(t_r)
        for q in range(chunks):
            recv(piece(zero_l, q), ag_recv.at[2, q], {"tp": t_l})
            send(piece(zero_l, q), piece(zero_l, q), ag_send.at[5], ag_recv.at[5, q], {"tp": t_r}, False)
        for q in range(chunks):
            recv(piece(zero_r, q), ag_recv.at[3, q], {"tp": t_r})
        pl.when(~late)(functools.partial(hand, (zero_l, zero_r)))
        row_stats(zero_l)
        row_stats(zero_r)
        for q in range(chunks):
            recv(piece(t_o, q), ag_recv.at[4, q], {"tp": t_r})
        pl.when(~late)(functools.partial(hand, (t_o,)))
        row_stats(t_o)
        for q in range(chunks):
            recv(piece(zero_o, q), ag_recv.at[5, q], {"tp": t_l})
        pl.when(~late)(functools.partial(hand, (zero_o,)))
        row_stats(zero_o)

        @pl.when(late)
        def _():
            meet()
            hand_context()
            sibling_rows()
            hand((t, t_r, t_l, zero_l, zero_r, t_o, zero_o))

        row_stats(sib)
        recv(mt.at[x], x_recv.at[x], {"tp": sib})
        for n, (xx, who) in enumerate(((xr, zero_r), (xl, zero_l), (xo, zero_o))):
            recv(mt.at[xx], x_recv.at[xx], {"tp": who})
            send(mt.at[xx], mt.at[xx], x_send.at[n], x_recv.at[xx], {"tp": sib}, False)

    @pl.when(c == 0)
    def _():
        modulation()
        loads["rows"].wait()
        contact()
        pl.semaphore_signal(hello, inc=1, device_id={"tp": sib}, device_id_type=MESH)
        send(rows.at[t], rows.at[t], sib_send.at[t], sib_recv.at[t], {"tp": sib}, False)
        recv(mpair.at[1], pair_recv.at[0], {"tp": sib})

        @pl.when(z != center)
        def _():
            send(mpair, mall.at[z - jnp.where(z > center, 1, 0)], m_send.at[0], m_recv, {"sp": center}, False)

        own_context()
        cpair[0] = cown[...]
        row_stats(t)
        recv(cpair.at[1], pair_recv.at[1], {"tp": sib})

        def block(i):
            return cg.at[:, pl.ds(SPAN * i, SPAN)]

        def tell_sum():
            recv(mall, m_recv, {"sp": 0})
            tot = mpair[...]
            for i in range(n_sp - 1):
                tot = tot + mall[i]
            msum[...] = tot

            def tell(i):
                send(msum, mt.at[x], tot_send, tot_recv, {"sp": i}, False)

            each(0, center, tell)
            each(center + 1, n_sp, tell)
            mt[x] = tot

        def sum_in():
            recv(mt.at[x], tot_recv, {"sp": center})

        def rows_in(groups):
            for g in groups:
                recv(rows.at[g], sib_recv.at[g], {"tp": sib})
                row_stats(g)

        def early_rows():
            rows_in((sib, t_r + 1, t_l + 1))

        @pl.when(z != lead)
        def _():
            send(cpair, cg.at[:, slot], c_send.at[0], p_recv.at[slot % SPAN], {"sp": lead}, False)

        def hand_near(i):
            for n, who in enumerate(members[:2]):
                for k in range(2):
                    send(own_block(k, i), own_block(k, i), bm_send.at[2 * n + k], b_recv.at[i], {"sp": who, "tp": t + k}, False)
            send(own_block(1, i), own_block(1, i), bm_send.at[2 * SPAN - 2], b_recv.at[i], {"tp": sib}, False)

        def hand_far(i):
            for k in range(2):
                send(own_block(k, i), own_block(k, i), bm_send.at[4 + k], b_recv.at[i], {"sp": members[2], "tp": t + k}, False)

        def hand_block(i):
            hand_near(i)
            hand_far(i)

        def member_in(n):
            recv(cg.at[:, SPAN * team + places[n]], p_recv.at[places[n]], {"sp": members[n]})

        def give(i):
            send(block(team), block(team), bl_send.at[i], b_recv.at[team], {"sp": SPAN * i + center}, False)

        def got(i):
            recv(block(i), b_recv.at[i], {"sp": SPAN * i + center})

        def answer(i):
            got(i)
            give(i)
            hand_block(i)

        def follow(i):
            got(i)
            hand_block(i)

        def near_in(i):
            got(i)
            hand_near(i)

        def late_in(i):
            got(i)
            give(i)
            hand_near(i)

        @pl.when(z == lead)
        def _():
            for k in range(2):
                cg[k, slot] = cpair[k]
            member_in(1)
            member_in(0)

        @pl.when(z == center)
        def _():
            early_rows()
            each(1, teams - LATEST, near_in)
            member_in(2)
            hand_near(0)

        @pl.when((z == lead) & (z != center))
        def _():
            member_in(2)
            each(0, team, give)
            hand_block(team)
            each(team + 1, teams, answer)

        pl.when(z != center)(early_rows)
        pl.when(z == center)(tell_sum)
        pl.when(z != center)(sum_in)
        for n, who in enumerate((sib, t_o + 1, t_r + 1, t_l + 1)):
            send(mt.at[x], mt.at[x], x_send.at[n], x_recv.at[x], {"tp": who}, False)

        @pl.when(z == center)
        def _():
            each(teams - LATEST, teams, late_in)
            each(1, teams - LATEST, give)
            each(0, teams, hand_far)

        @pl.when((z == lead) & (z != center))
        def _():
            each(0, team, follow)

        rows_in((t_o + 1, t_r, t_l, t_o))
        for xx in (xr, xl, xo):
            recv(mt.at[xx], x_recv.at[xx], {"tp": sib})

    for j in range(n_tp):
        for i in range(per):
            part = slice(j * width + i * LANES, j * width + (i + 1) * LANES)
            s_vec[:, part] = mt[j // 2, j % 2, i : i + 1, :]
            a_vec[:, part] = gain[:, part] * (1.0 + mt[j // 2, j % 2, per + i : per + i + 1, :])
            g_vec[:, part] = mt[j // 2, j % 2, 2 * per + i : 2 * per + i + 1, :]
    gates = pltpu.make_async_copy(g_vec, gate_out, load_sem.at[15])
    gates.start()
    for name in ("rt", "ct", "qw", "ow", "sink"):
        loads[name].wait()

    lane = lax.broadcasted_iota(jnp.int32, (1, LANES), 1)
    first = lane % 32 < 16

    def swapped(v):
        return jnp.where(first, pltpu.roll(v, LANES - 16, 1), pltpu.roll(v, 16, 1))

    def project(gs):
        acc = jnp.zeros((len(gs) * group, 2 * LANES), f32)
        for i in range(depth // COLS):
            part = slice(i * COLS, (i + 1) * COLS)
            a = a_vec[:, part]
            s = s_vec[:, part]
            tiles = []
            for g in gs:
                r = jnp.concatenate([inv[g]] * (COLS // LANES), axis=1)
                tiles.append((rows[g, :, part].astype(f32) * r * a + s).astype(bf16))
            acc = acc + jnp.dot(jnp.concatenate(tiles, axis=0), w[part, :], preferred_element_type=f32)
        for n, g in enumerate(gs):
            fac = rt[g : g + 1, :] + ct[...]
            vq = acc[n * group : (n + 1) * group, :LANES]
            vk = acc[n * group : (n + 1) * group, LANES:]
            q2 = vq * fac[:, :LANES] + swapped(vq) * fac[:, LANES : 2 * LANES]
            k2 = vk * fac[:, 2 * LANES : 3 * LANES] + swapped(vk) * fac[:, 3 * LANES :]
            qrot[g * group : (g + 1) * group, :] = q2.astype(bf16)
            kv[WIN + g * group : WIN + (g + 1) * group, :] = k2.astype(bf16)

    project((0, 1, n_tp - 2, n_tp - 1))

    @pl.when(z > 0)
    def _():
        send(kv.at[pl.ds(WIN, WIN)], kv.at[pl.ds(WIN + count, WIN)], h_send.at[0], h_recv.at[0], {"sp": z - 1}, False)

    @pl.when(z < n_sp - 1)
    def _():
        send(kv.at[pl.ds(count, WIN)], kv.at[pl.ds(0, WIN)], h_send.at[1], h_recv.at[1], {"sp": z + 1}, False)

    project(tuple(range(2, n_tp - 2)))

    @pl.when((c == 1) | (z != lead))
    def _():
        for i in range(n_sp // SPAN):
            recv(own_block(c, i), b_recv.at[i], {"sp": lead, "tp": t - c})

    for j in range(n_sp):
        ctx[pl.ds(j * n_ctx, n_ctx), :] = cg[c, j]
    rows2 = 2 * WIN
    qi = lax.broadcasted_iota(jnp.int32, (rows2, WIN), 0) % WIN
    ki = lax.broadcasted_iota(jnp.int32, (rows2, WIN), 1)
    head1 = lax.broadcasted_iota(jnp.int32, (rows2, 1), 0) >= WIN
    sink_col = jnp.where(head1, sink[0:1, 1:2], sink[0:1, 0:1])
    is_key = lane < HD
    contract = (((1,), (1,)), ((), ()))
    blocks = count // WIN

    def attend(b):
        qb = qrot[b * WIN : (b + 1) * WIN, :].astype(f32)
        q0 = jnp.where(is_key, qb, 0.0).astype(bf16)
        q1 = jnp.where(is_key, pltpu.roll(qb, HD, 1), 0.0).astype(bf16)
        qq = jnp.concatenate([q0, q1], axis=0)
        band = kv[b * WIN : (b + 3) * WIN, :]
        whole = ctx[...]
        s_band = lax.dot_general(qq, band, contract, preferred_element_type=f32)
        s_ctx = lax.dot_general(qq, whole, contract, preferred_element_type=f32)
        left = ki >= qi
        right = ki <= qi
        if b == 0:
            left = left & (z > 0)
        if b == blocks - 1:
            right = right & (z < n_sp - 1)
        s0 = jnp.where(left, s_band[:, :WIN], neg_large)
        s1 = s_band[:, WIN : 2 * WIN]
        s2 = jnp.where(right, s_band[:, 2 * WIN :], neg_large)
        top = jnp.maximum(jnp.maximum(s0, s1), s2)
        for i in range(whole.shape[0] // LANES):
            top = jnp.maximum(top, s_ctx[:, i * LANES : (i + 1) * LANES])
        m = jnp.maximum(jnp.max(top, axis=1, keepdims=True), sink_col)
        e0 = jnp.exp(s0 - m)
        e1 = jnp.exp(s1 - m)
        e2 = jnp.exp(s2 - m)
        ec = jnp.exp(s_ctx - m)
        tot = e0 + e1 + e2
        for i in range(whole.shape[0] // LANES):
            tot = tot + ec[:, i * LANES : (i + 1) * LANES]
        den = jnp.sum(tot, axis=1, keepdims=True) + jnp.exp(sink_col - m)
        r = 1.0 / den
        p_band = jnp.concatenate([e0, e1, e2], axis=1) * r
        o = jnp.dot(p_band.astype(bf16), band, preferred_element_type=f32) + jnp.dot(
            (ec * r).astype(bf16), whole, preferred_element_type=f32
        )
        res = jnp.where(is_key, pltpu.roll(o[:WIN], HD, 1), o[WIN:]).astype(bf16)
        att[t, b * WIN : (b + 1) * WIN, :] = res

    def att_piece(who, b):
        return att.at[who, pl.ds(b * WIN, WIN)]

    def att_send(b):
        mine = att_piece(t, b)
        send(mine, mine, t_send.at[2], t_recv.at[2, b], {"tp": t_o}, False)
        send(mine, mine, t_send.at[0], t_recv.at[0, b], {"tp": t_r}, False)
        send(mine, mine, t_send.at[1], t_recv.at[1, b], {"tp": t_l}, False)
        send(mine, mine, tsib_send.at[0], tsib_recv.at[0], {"tp": sib}, False)

    def att_take(b):
        for role, who in ((0, t_l), (1, t_r), (2, t_o)):
            got = att_piece(who, b)
            recv(got, t_recv.at[role, b], {"tp": who})
            send(got, got, tsib_send.at[1 + role], tsib_recv.at[1 + role], {"tp": sib}, False)

    order = [*range(1, blocks - 1), 0, blocks - 1]
    for n, b in enumerate(order):
        if n == blocks - 2:
            @pl.when(z < n_sp - 1)
            def _():
                recv(kv.at[pl.ds(WIN + count, WIN)], h_recv.at[0], {"sp": z + 1})

            @pl.when(z > 0)
            def _():
                recv(kv.at[pl.ds(0, WIN)], h_recv.at[1], {"sp": z - 1})

        attend(b)
        att_send(b)
        if n >= 2:
            att_take(order[n - 2])
    att_take(order[-2])
    att_take(order[-1])
    for role, xx in ((0, x), (1, xl), (2, xr), (3, xo)):
        recv(att.at[xx * 2 + 1 - c], tsib_recv.at[role], {"tp": sib})

    before = len(started)
    here = pl.ds(pl.multiple_of(t * width, LANES), width)
    for n, xx in enumerate((xo, xr, xl, x)):
        part = pl.ds(pl.multiple_of(xx * WIN, WIN), WIN)
        y = jnp.zeros((WIN, width), f32)
        for i in range(n_x):
            lhs = jnp.concatenate([att[2 * i, part, :], att[2 * i + 1, part, :]], axis=1)
            y = y + jnp.dot(lhs, ow[2 * i * LANES : 2 * (i + 1) * LANES, :], preferred_element_type=f32)
        ysend[2 * n] = y[:group].astype(bf16)
        ysend[2 * n + 1] = y[group:].astype(bf16)
        if n < 3:
            for k in range(2):
                send(ysend.at[2 * n + k], out.at[:, here], y_send.at[2 * n + k], y_recv.at[2 * n + c], {"tp": xx * 2 + k})
        else:
            send(ysend.at[2 * n + 1 - c], out.at[:, here], y_send.at[6], y_recv.at[6], {"tp": sib})
            keep = pltpu.make_async_copy(ysend.at[2 * n + c], out.at[:, here], load_sem.at[14])
            keep.start()
    for n, who in enumerate((t_r, t_l, t_o)):
        sent(att.at[t], t_send.at[n], {"tp": who})
    for n, who in enumerate((t, t_l, t_r, t_o)):
        sent(att.at[who], tsib_send.at[n], {"tp": sib})
    for copy in started[:before]:
        copy.wait_send()

    @pl.when(z > 0)
    def _():
        sent(kv.at[pl.ds(WIN, WIN)], h_send.at[0], {"sp": z - 1})

    @pl.when(z < n_sp - 1)
    def _():
        sent(kv.at[pl.ds(count, WIN)], h_send.at[1], {"sp": z + 1})

    @pl.when(c == 1)
    def _():
        for n, xx in enumerate((xr, xl, xo)):
            sent(mt.at[xx], x_send.at[n], {"tp": sib})
        sent(mpair.at[1], pair_send.at[0], {"tp": sib})
        sent(cown, pair_send.at[1], {"tp": sib})
        for n, (g, who) in enumerate(((t, t_r), (t, t_l), (sib, t_r), (sib, t_l), (t_r, t_l), (zero_l, t_r))):
            sent(rows.at[g], ag_send.at[n], {"tp": who})
        for g in (t, t_r, t_l, zero_l, zero_r, t_o, zero_o):
            sent(rows.at[g], sib_send.at[g], {"tp": sib})
    @pl.when(c == 0)
    def _():
        sent(rows.at[t], sib_send.at[t], {"tp": sib})
        for n, who in enumerate((sib, t_o + 1, t_r + 1, t_l + 1)):
            sent(mt.at[x], x_send.at[n], {"tp": who})

        @pl.when(z == center)
        def _():
            sent(mall, tot_send, {"sp": 0})

        @pl.when(z != lead)
        def _():
            sent(cpair, c_send.at[0], {"sp": lead})

        @pl.when(z == lead)
        def _():
            def given(i):
                sent(cg.at[:, pl.ds(SPAN * team, SPAN)], bl_send.at[i], {"sp": SPAN * i + center})

            each(0, team, given)
            each(team + 1, teams, given)

            for n, who in enumerate(members):
                for k in range(2):
                    sent(cg.at[k], bm_send.at[2 * n + k], {"sp": who})
            sent(cg.at[1], bm_send.at[2 * SPAN - 2], {"tp": sib})

        @pl.when(z != center)
        def _():
            sent(mpair, m_send.at[0], {"sp": center})

    for n, xx in enumerate((xo, xl, xr)):
        for k in range(2):
            cols = pl.ds(pl.multiple_of((xx * 2 + k) * width, LANES), width)
            recv(out.at[:, cols], y_recv.at[2 * n + k], {"tp": xx * 2 + k})
    recv(out.at[:, pl.ds(pl.multiple_of(sib * width, LANES), width)], y_recv.at[6], {"tp": sib})
    keep.wait()
    gates.wait()
    for copy in started[before:]:
        copy.wait_send()


def local(n_sp, n_tp, latent, context, conditioning, norm_gain, *rest):
    shift_w, scale_w, gate_w, q_w, k_w, v_w, o_w, sink = rest
    group, depth = latent.shape
    n_ctx = context.shape[0]
    count = n_tp * group
    width = shift_w.shape[1]
    blocks = count // WIN
    chunks = group // 16
    row_tab, col_tab = rope_tables(n_sp * count // GRID_W)
    any_space = pl.BlockSpec(memory_space=pl.ANY)
    dma = pltpu.SemaphoreType.DMA
    blended, gate = pl.pallas_call(
        functools.partial(kernel, n_sp, n_tp),
        out_shape=(jax.ShapeDtypeStruct((group, depth), bf16), jax.ShapeDtypeStruct((1, depth), f32)),
        in_specs=[any_space] * 14,
        out_specs=(any_space, any_space),
        scratch_shapes=[
            pltpu.VMEM((n_tp, group, depth), bf16),
            pltpu.VMEM((depth, 2 * LANES), bf16),
            pltpu.VMEM((2 * HD, depth), bf16),
            pltpu.VMEM(o_w.shape, bf16),
            pltpu.VMEM((3, *shift_w.shape), bf16),
            pltpu.VMEM((n_ctx, depth), bf16),
            pltpu.VMEM((2, n_sp, n_ctx, LANES), bf16),
            pltpu.VMEM((n_ctx, LANES), bf16),
            pltpu.VMEM((2, n_ctx, LANES), bf16),
            pltpu.VMEM((2, 16, LANES), f32),
            pltpu.VMEM((n_sp - 1, 2, 16, LANES), f32),
            pltpu.VMEM((2, 16, LANES), f32),
            pltpu.VMEM((n_tp // 2, 2, 16, LANES), f32),
            pltpu.VMEM((n_tp, group, LANES), f32),
            pltpu.VMEM((1, depth), f32),
            pltpu.VMEM((1, depth), f32),
            pltpu.VMEM((1, depth), f32),
            pltpu.VMEM((count, LANES), bf16),
            pltpu.VMEM((count + 2 * WIN, LANES), bf16),
            pltpu.VMEM((n_sp * n_ctx, LANES), bf16),
            pltpu.VMEM((n_tp, count, LANES), bf16),
            pltpu.VMEM((n_tp, group, width), bf16),
            pltpu.VMEM((count // GRID_W, 4 * LANES), f32),
            pltpu.VMEM((GRID_W, 4 * LANES), f32),
            pltpu.VMEM((1, conditioning.shape[0]), bf16),
            pltpu.VMEM((1, depth), f32),
            pltpu.VMEM((1, sink.shape[0]), f32),
            pltpu.SemaphoreType.REGULAR,
            dma((16,)),
            dma((3,)),
            dma((3,)),
            dma((1,)),
            dma,
            dma,
            dma,
            dma((1,)),
            dma((SPAN,)),
            dma((n_sp // SPAN,)),
            dma((n_sp // SPAN,)),
            dma((2 * SPAN,)),
            dma((6,)),
            dma((6, chunks)),
            dma((n_tp,)),
            dma((n_tp,)),
            dma((4,)),
            dma((n_tp // 2,)),
            dma((2,)),
            dma((2,)),
            dma((3,)),
            dma((3, blocks)),
            dma((4,)),
            dma((4,)),
            dma((8,)),
            dma((8,)),
        ],
        compiler_params=pltpu.CompilerParams(
            collective_id=0, has_side_effects=True, vmem_limit_bytes=56 * 1024 * 1024
        ),
    )(
        latent,
        context,
        conditioning.reshape(1, -1),
        norm_gain.reshape(1, -1),
        shift_w,
        scale_w,
        gate_w,
        q_w,
        k_w.T,
        v_w.T,
        o_w,
        sink.reshape(1, -1),
        jnp.asarray(row_tab),
        jnp.asarray(col_tab),
    )
    return (latent.astype(f32) + gate * blended.astype(f32)).astype(bf16)


def solution(mesh):
    in_specs = (
        P(("grp", "sp", "tp"), None),
        P(("grp", "sp"), None),
        P(("grp", "sp")),
        P(),
        P("sp", "tp"),
        P("sp", "tp"),
        P("sp", "tp"),
        P(None, "tp"),
        P(None, "tp"),
        P(None, "tp"),
        P(None, "tp"),
        P("tp"),
    )
    return jax.shard_map(
        functools.partial(local, mesh.shape["sp"], mesh.shape["tp"]),
        mesh=mesh,
        in_specs=in_specs,
        out_specs=P(("grp", "sp", "tp"), None),
        check_vma=False,
    )
```

```python
import functools

import jax
import jax.numpy as jnp
import numpy as np
from jax import lax
from jax.experimental import pallas as pl
from jax.experimental.pallas import tpu as pltpu
from jax.sharding import PartitionSpec as P

HEADS = 16
KV_HEADS = 8
HD = 64
GRID_W = 64
WIN = 128
SPAN = 4
LATEST = 4
LANES = 128
COLS = 512

epsilon = 1e-06
rope_base = 10000.0
neg_large = -1e30
MESH = pl.DeviceIdType.MESH
f32 = jnp.float32
bf16 = jnp.bfloat16


def rope_tables(grid_rows):
    lane = np.arange(LANES)
    d = lane % HD
    freq = rope_base ** (-(d % 16) / 16.0)
    is_row = d < HD // 2
    sign = np.where(d % 32 < 16, -1.0, 1.0)
    is_key = lane < HD

    def table(count, own):
        angle = np.arange(count)[:, None] * freq[None, :]
        c = np.where(own, np.cos(angle), 0.0)
        s = np.where(own, np.sin(angle) * sign, 0.0)
        scale = HD**-0.5
        ck = np.where(is_key, c, 0.0)
        sk = np.where(is_key, s, 0.0)
        return np.concatenate([c * scale, s * scale, ck, sk], axis=1)

    rows = table(grid_rows, is_row)
    cols = table(GRID_W, ~is_row)
    cols[:, 2 * LANES : 3 * LANES] += np.where(is_key, 0.0, 1.0)
    return rows.astype(np.float32), cols.astype(np.float32)


def kernel(
    n_sp,
    n_tp,
    latent,
    context,
    cond_in,
    gain_in,
    shift_w,
    scale_w,
    gate_w,
    q_w,
    k_t,
    v_t,
    o_w,
    sink_in,
    row_tab,
    col_tab,
    out,
    gate_out,
    rows,
    w,
    kvt,
    ow,
    mw,
    ctx_rows,
    cg,
    cown,
    cpair,
    mpair,
    mall,
    msum,
    mt,
    inv,
    a_vec,
    s_vec,
    g_vec,
    qrot,
    kv,
    ctx,
    att,
    ysend,
    rt,
    ct,
    cond,
    gain,
    sink,
    hello,
    load_sem,
    pair_send,
    pair_recv,
    m_send,
    m_recv,
    tot_send,
    tot_recv,
    c_send,
    p_recv,
    b_recv,
    bl_send,
    bm_send,
    ag_send,
    ag_recv,
    sib_send,
    sib_recv,
    x_send,
    x_recv,
    h_send,
    h_recv,
    t_send,
    t_recv,
    tsib_send,
    tsib_recv,
    y_send,
    y_recv,
):
    n_x = n_tp // 2
    z = lax.axis_index("sp")
    t = lax.axis_index("tp")
    x = t // 2
    c = t % 2
    xr = (x + 1) % n_x
    xl = (x + n_x - 1) % n_x
    xo = (x + 2) % n_x
    sib = x * 2 + (1 - c)
    t_r, t_l, t_o = xr * 2 + c, xl * 2 + c, xo * 2 + c
    group = latent.shape[0]
    count = n_tp * group
    depth = latent.shape[1]
    chunks = group // 16
    width = shift_w.shape[1]
    per = width // LANES

    late = (z == 0) & (x == 0)
    center = 1

    started = []

    def send(src, dst, ss, rs, dev, keep=True):
        copy = pltpu.make_async_remote_copy(
            src_ref=src, dst_ref=dst, send_sem=ss, recv_sem=rs, device_id=dev, device_id_type=MESH
        )
        copy.start()
        if keep:
            started.append(copy)

    def recv(dst, rs, dev):
        pltpu.make_async_remote_copy(
            src_ref=dst, dst_ref=dst, send_sem=rs, recv_sem=rs, device_id=dev, device_id_type=MESH
        ).wait_recv()

    def sent(src, ss, dev):
        pltpu.make_async_remote_copy(
            src_ref=src, dst_ref=src, send_sem=ss, recv_sem=ss, device_id=dev, device_id_type=MESH
        ).wait_send()

    def each(lo, hi, body):
        def step(i, carry):
            body(i)
            return carry

        lax.fori_loop(lo, hi, step, 0)

    barrier = pltpu.get_barrier_semaphore()

    def greet(dev):
        pl.semaphore_signal(barrier, inc=1, device_id=dev, device_id_type=MESH)

    @pl.when(c == 1)
    def _():
        for who in (sib, t_l):
            greet({"tp": who})

    slot = (z + 1) % n_sp
    teams = n_sp // SPAN
    team = slot // SPAN
    lead = SPAN * team + center
    members = [(z + n_sp - 1) % n_sp, (z + 1) % n_sp, (z + n_sp - 2) % n_sp]
    places = (1, 3, 0)

    @pl.when((c == 0) & (z == center))
    def _():
        each(0, center, lambda i: greet({"sp": i}))
        each(center + 1, n_sp, lambda i: greet({"sp": i}))

    @pl.when((c == 0) & (z == lead))
    def _():
        for i in members:
            greet({"sp": i})
        each(team + 1, teams, lambda i: greet({"sp": SPAN * i + center}))

    grid_rows = count // GRID_W
    loads = {}

    def load(name, src, dst):
        copy = pltpu.make_async_copy(src, dst, load_sem.at[len(loads)])
        copy.start()
        loads[name] = copy

    load("cond", cond_in, cond)
    load("m0", shift_w, mw.at[0])
    load("m1", scale_w, mw.at[1])
    load("m2", gate_w, mw.at[2])
    load("rows", latent, rows.at[t])
    load("gain", gain_in, gain)
    load("kw", k_t, kvt.at[pl.ds(0, HD)])
    load("vw", v_t, kvt.at[pl.ds(HD, HD)])
    load("ctx", context, ctx_rows)
    load("qw", q_w, w.at[:, pl.ds(0, LANES)])
    load("rt", row_tab.at[pl.ds(pl.multiple_of(z * grid_rows, 8), grid_rows)], rt)
    load("ct", col_tab, ct)
    load("sink", sink_in, sink)
    load("ow", o_w, ow)

    def contact():
        pl.semaphore_wait(barrier, 1 + jnp.where(z == center, 0, 1) + jnp.where(z == lead, team, 1))

    def modulation():
        loads["cond"].wait()
        cv = cond[...].astype(f32)
        lifted = jnp.broadcast_to((cv / (1.0 + jnp.exp(-cv))).astype(bf16), (16, cv.shape[1]))
        for i in range(3):
            loads["m%d" % i].wait()
            part = jnp.dot(lifted, mw[i], preferred_element_type=f32)
            for j in range(per):
                mpair[c, per * i + j : per * i + j + 1, :] = part[0:1, j * LANES : (j + 1) * LANES]
        mpair[c, 3 * per : 16, :] = jnp.zeros((16 - 3 * per, LANES), f32)

    n_ctx = ctx_rows.shape[0]

    def own_context():
        for name in ("kw", "vw", "gain", "ctx"):
            loads[name].wait()
        for i in range(depth // COLS):
            w[i * COLS : (i + 1) * COLS, LANES : 2 * LANES] = kvt[:, i * COLS : (i + 1) * COLS].T
        sq = jnp.zeros((n_ctx, LANES), f32)
        for i in range(depth // LANES):
            v = ctx_rows[:, i * LANES : (i + 1) * LANES].astype(f32)
            sq = sq + v * v
        cinv = lax.rsqrt(jnp.sum(sq, axis=1, keepdims=True) * (1.0 / depth) + epsilon)
        acc = jnp.zeros((n_ctx, LANES), f32)
        for i in range(depth // COLS):
            part = slice(i * COLS, (i + 1) * COLS)
            v = ctx_rows[:, part].astype(f32) * cinv * gain[:, part]
            acc = acc + jnp.dot(v.astype(bf16), w[part, LANES : 2 * LANES], preferred_element_type=f32)
        cown[...] = acc.astype(bf16)

    def row_stats(g):
        sq = jnp.zeros((group, LANES), f32)
        for i in range(depth // LANES):
            v = rows[g, :, i * LANES : (i + 1) * LANES].astype(f32)
            sq = sq + v * v
        r = lax.rsqrt(jnp.sum(sq, axis=1, keepdims=True) * (1.0 / depth) + epsilon)
        inv[g] = jnp.broadcast_to(r, (group, LANES))

    @pl.when(z == 0)
    def _():
        kv[:WIN, :] = jnp.zeros((WIN, LANES), bf16)

    @pl.when(z == n_sp - 1)
    def _():
        kv[WIN + count :, :] = jnp.zeros((WIN, LANES), bf16)

    def piece(g, q):
        return rows.at[g, pl.ds(16 * q, 16)]

    zero_l, zero_r, zero_o = t_l - c, t_r - c, t_o - c

    def meet():
        pl.semaphore_wait(hello, 1)
        send(mpair.at[1], mpair.at[1], pair_send.at[0], pair_recv.at[0], {"tp": sib}, False)

    def hand_context():
        send(cown, cpair.at[1], pair_send.at[1], pair_recv.at[1], {"tp": sib}, False)

    def sibling_rows():
        recv(rows.at[sib], sib_recv.at[sib], {"tp": sib})
        for q in range(chunks):
            send(piece(sib, q), piece(sib, q), ag_send.at[2], ag_recv.at[2, q], {"tp": t_r}, False)
            send(piece(sib, q), piece(sib, q), ag_send.at[3], ag_recv.at[3, q], {"tp": t_l}, False)

    def hand(groups):
        for g in groups:
            send(rows.at[g], rows.at[g], sib_send.at[g], sib_recv.at[g], {"tp": sib}, False)

    def own_block(k, i):
        return cg.at[k, pl.ds(SPAN * i, SPAN)]

    def block(i):
        return cg.at[:, pl.ds(SPAN * i, SPAN)]

    def hand_far(i):
        for k in range(2):
            send(own_block(k, i), own_block(k, i), bm_send.at[4 + k], b_recv.at[i], {"sp": members[2], "tp": t + k}, False)

    def give(i):
        send(block(team), block(team), bl_send.at[i], b_recv.at[team], {"sp": SPAN * i + center}, False)

    @pl.when(c == 1)
    def _():
        modulation()
        loads["rows"].wait()
        pl.semaphore_wait(barrier, 1)
        pl.when(~late & (z >= n_sp // 2))(meet)
        for q in range(chunks):
            send(piece(t, q), piece(t, q), ag_send.at[0], ag_recv.at[0, q], {"tp": t_r}, False)
        own_context()
        pl.when(~late & (z >= n_sp // 2))(hand_context)
        recv(piece(t_l, 0), ag_recv.at[0, 0], {"tp": t_l})
        for q in range(chunks):
            send(piece(t, q), piece(t, q), ag_send.at[1], ag_recv.at[1, q], {"tp": t_l}, False)
        pl.when(~late & (z < n_sp // 2))(meet)
        pl.when(~late & (z < n_sp // 2))(hand_context)
        pl.when(~late)(sibling_rows)
        for q in range(chunks):
            recv(piece(t_r, q), ag_recv.at[1, q], {"tp": t_r})
            send(piece(t_r, q), piece(t_r, q), ag_send.at[4], ag_recv.at[4, q], {"tp": t_l}, False)
        for q in range(1, chunks):
            recv(piece(t_l, q), ag_recv.at[0, q], {"tp": t_l})
        pl.when(~late)(functools.partial(hand, (t, t_r, t_l)))
        row_stats(t)
        row_stats(t_l)
        row_stats(t_r)
        for q in range(chunks):
            recv(piece(zero_l, q), ag_recv.at[2, q], {"tp": t_l})
            send(piece(zero_l, q), piece(zero_l, q), ag_send.at[5], ag_recv.at[5, q], {"tp": t_r}, False)
        for q in range(chunks):
            recv(piece(zero_r, q), ag_recv.at[3, q], {"tp": t_r})
        pl.when(~late)(functools.partial(hand, (zero_l, zero_r)))
        row_stats(zero_l)
        row_stats(zero_r)
        for q in range(chunks):
            recv(piece(t_o, q), ag_recv.at[4, q], {"tp": t_r})
        pl.when(~late)(functools.partial(hand, (t_o,)))
        row_stats(t_o)
        for q in range(chunks):
            recv(piece(zero_o, q), ag_recv.at[5, q], {"tp": t_l})
        pl.when(~late)(functools.partial(hand, (zero_o,)))
        row_stats(zero_o)

        @pl.when(late)
        def _():
            meet()
            hand_context()
            sibling_rows()
            hand((t, t_r, t_l, zero_l, zero_r, t_o, zero_o))

        row_stats(sib)
        recv(mt.at[x], x_recv.at[x], {"tp": sib})
        for n, (xx, who) in enumerate(((xr, zero_r), (xl, zero_l), (xo, zero_o))):
            recv(mt.at[xx], x_recv.at[xx], {"tp": who})
            send(mt.at[xx], mt.at[xx], x_send.at[n], x_recv.at[xx], {"tp": sib}, False)

    @pl.when(c == 0)
    def _():
        modulation()
        loads["rows"].wait()
        contact()
        pl.semaphore_signal(hello, inc=1, device_id={"tp": sib}, device_id_type=MESH)
        send(rows.at[t], rows.at[t], sib_send.at[t], sib_recv.at[t], {"tp": sib}, False)
        recv(mpair.at[1], pair_recv.at[0], {"tp": sib})

        @pl.when(z != center)
        def _():
            send(mpair, mall.at[z - jnp.where(z > center, 1, 0)], m_send.at[0], m_recv, {"sp": center}, False)

        own_context()
        cpair[0] = cown[...]
        row_stats(t)
        recv(cpair.at[1], pair_recv.at[1], {"tp": sib})

        def tell_sum():
            recv(mall, m_recv, {"sp": 0})
            tot = mpair[...]
            for i in range(n_sp - 1):
                tot = tot + mall[i]
            msum[...] = tot

            def tell(i):
                send(msum, mt.at[x], tot_send, tot_recv, {"sp": i}, False)

            each(0, center, tell)
            each(center + 1, n_sp, tell)
            mt[x] = tot

        def sum_in():
            recv(mt.at[x], tot_recv, {"sp": center})

        def rows_in(groups):
            for g in groups:
                recv(rows.at[g], sib_recv.at[g], {"tp": sib})
                row_stats(g)

        def early_rows():
            rows_in((sib, t_r + 1, t_l + 1))

        @pl.when(z != lead)
        def _():
            send(cpair, cg.at[:, slot], c_send.at[0], p_recv.at[slot % SPAN], {"sp": lead}, False)

        def hand_near(i):
            for n, who in enumerate(members[:2]):
                for k in range(2):
                    send(own_block(k, i), own_block(k, i), bm_send.at[2 * n + k], b_recv.at[i], {"sp": who, "tp": t + k}, False)
            send(own_block(1, i), own_block(1, i), bm_send.at[2 * SPAN - 2], b_recv.at[i], {"tp": sib}, False)

        def hand_block(i):
            hand_near(i)
            hand_far(i)

        def member_in(n):
            recv(cg.at[:, SPAN * team + places[n]], p_recv.at[places[n]], {"sp": members[n]})

        def got(i):
            recv(block(i), b_recv.at[i], {"sp": SPAN * i + center})

        def answer(i):
            got(i)
            give(i)
            hand_block(i)

        def follow(i):
            got(i)
            hand_block(i)

        def near_in(i):
            got(i)
            hand_near(i)

        @pl.when(z == lead)
        def _():
            for k in range(2):
                cg[k, slot] = cpair[k]
            member_in(1)
            member_in(0)

        @pl.when(z == center)
        def _():
            early_rows()
            each(1, teams - LATEST, near_in)
        @pl.when((z == lead) & (z != center))
        def _():
            member_in(2)
            each(0, team, give)
            hand_block(team)
            each(team + 1, teams, answer)

        pl.when(z != center)(early_rows)
        pl.when(z == center)(tell_sum)
        pl.when(z != center)(sum_in)
        for n, who in enumerate((sib, t_o + 1, t_r + 1, t_l + 1)):
            send(mt.at[x], mt.at[x], x_send.at[n], x_recv.at[x], {"tp": who}, False)

        @pl.when(z == center)
        def _():
            member_in(2)
            hand_near(0)
            each(1, teams - LATEST, give)
            each(teams - LATEST, teams, near_in)

        @pl.when((z == lead) & (z != center))
        def _():
            each(0, team, follow)

        rows_in((t_o + 1, t_r, t_l, t_o))
        for xx in (xr, xl, xo):
            recv(mt.at[xx], x_recv.at[xx], {"tp": sib})

    for j in range(n_tp):
        for i in range(per):
            part = slice(j * width + i * LANES, j * width + (i + 1) * LANES)
            s_vec[:, part] = mt[j // 2, j % 2, i : i + 1, :]
            a_vec[:, part] = gain[:, part] * (1.0 + mt[j // 2, j % 2, per + i : per + i + 1, :])
            g_vec[:, part] = mt[j // 2, j % 2, 2 * per + i : 2 * per + i + 1, :]
    gates = pltpu.make_async_copy(g_vec, gate_out, load_sem.at[15])
    gates.start()
    for name in ("rt", "ct", "qw", "ow", "sink"):
        loads[name].wait()

    lane = lax.broadcasted_iota(jnp.int32, (1, LANES), 1)
    first = lane % 32 < 16

    def swapped(v):
        return jnp.where(first, pltpu.roll(v, LANES - 16, 1), pltpu.roll(v, 16, 1))

    def project(gs):
        acc = jnp.zeros((len(gs) * group, 2 * LANES), f32)
        for i in range(depth // COLS):
            part = slice(i * COLS, (i + 1) * COLS)
            a = a_vec[:, part]
            s = s_vec[:, part]
            tiles = []
            for g in gs:
                r = jnp.concatenate([inv[g]] * (COLS // LANES), axis=1)
                tiles.append((rows[g, :, part].astype(f32) * r * a + s).astype(bf16))
            acc = acc + jnp.dot(jnp.concatenate(tiles, axis=0), w[part, :], preferred_element_type=f32)
        for n, g in enumerate(gs):
            fac = rt[g : g + 1, :] + ct[...]
            vq = acc[n * group : (n + 1) * group, :LANES]
            vk = acc[n * group : (n + 1) * group, LANES:]
            q2 = vq * fac[:, :LANES] + swapped(vq) * fac[:, LANES : 2 * LANES]
            k2 = vk * fac[:, 2 * LANES : 3 * LANES] + swapped(vk) * fac[:, 3 * LANES :]
            qrot[g * group : (g + 1) * group, :] = q2.astype(bf16)
            kv[WIN + g * group : WIN + (g + 1) * group, :] = k2.astype(bf16)

    project((0, 1, n_tp - 2, n_tp - 1))

    @pl.when(z > 0)
    def _():
        send(kv.at[pl.ds(WIN, WIN)], kv.at[pl.ds(WIN + count, WIN)], h_send.at[0], h_recv.at[0], {"sp": z - 1}, False)

    @pl.when(z < n_sp - 1)
    def _():
        send(kv.at[pl.ds(count, WIN)], kv.at[pl.ds(0, WIN)], h_send.at[1], h_recv.at[1], {"sp": z + 1}, False)

    @pl.when((c == 0) & (z == center))
    def _():
        each(teams - LATEST, teams, give)
        each(0, teams, hand_far)

    project(tuple(range(2, n_tp - 2)))

    @pl.when((c == 1) | (z != lead))
    def _():
        for i in range(n_sp // SPAN):
            recv(own_block(c, i), b_recv.at[i], {"sp": lead, "tp": t - c})

    for j in range(n_sp):
        ctx[pl.ds(j * n_ctx, n_ctx), :] = cg[c, j]
    rows2 = 2 * WIN
    qi = lax.broadcasted_iota(jnp.int32, (rows2, WIN), 0) % WIN
    ki = lax.broadcasted_iota(jnp.int32, (rows2, WIN), 1)
    head1 = lax.broadcasted_iota(jnp.int32, (rows2, 1), 0) >= WIN
    sink_col = jnp.where(head1, sink[0:1, 1:2], sink[0:1, 0:1])
    is_key = lane < HD
    contract = (((1,), (1,)), ((), ()))
    blocks = count // WIN

    def attend(b):
        qb = qrot[b * WIN : (b + 1) * WIN, :].astype(f32)
        q0 = jnp.where(is_key, qb, 0.0).astype(bf16)
        q1 = jnp.where(is_key, pltpu.roll(qb, HD, 1), 0.0).astype(bf16)
        qq = jnp.concatenate([q0, q1], axis=0)
        band = kv[b * WIN : (b + 3) * WIN, :]
        whole = ctx[...]
        s_band = lax.dot_general(qq, band, contract, preferred_element_type=f32)
        s_ctx = lax.dot_general(qq, whole, contract, preferred_element_type=f32)
        left = ki >= qi
        right = ki <= qi
        if b == 0:
            left = left & (z > 0)
        if b == blocks - 1:
            right = right & (z < n_sp - 1)
        s0 = jnp.where(left, s_band[:, :WIN], neg_large)
        s1 = s_band[:, WIN : 2 * WIN]
        s2 = jnp.where(right, s_band[:, 2 * WIN :], neg_large)
        top = jnp.maximum(jnp.maximum(s0, s1), s2)
        for i in range(whole.shape[0] // LANES):
            top = jnp.maximum(top, s_ctx[:, i * LANES : (i + 1) * LANES])
        m = jnp.maximum(jnp.max(top, axis=1, keepdims=True), sink_col)
        e0 = jnp.exp(s0 - m)
        e1 = jnp.exp(s1 - m)
        e2 = jnp.exp(s2 - m)
        ec = jnp.exp(s_ctx - m)
        tot = e0 + e1 + e2
        for i in range(whole.shape[0] // LANES):
            tot = tot + ec[:, i * LANES : (i + 1) * LANES]
        den = jnp.sum(tot, axis=1, keepdims=True) + jnp.exp(sink_col - m)
        r = 1.0 / den
        p_band = jnp.concatenate([e0, e1, e2], axis=1) * r
        o = jnp.dot(p_band.astype(bf16), band, preferred_element_type=f32) + jnp.dot(
            (ec * r).astype(bf16), whole, preferred_element_type=f32
        )
        res = jnp.where(is_key, pltpu.roll(o[:WIN], HD, 1), o[WIN:]).astype(bf16)
        att[t, b * WIN : (b + 1) * WIN, :] = res

    def att_piece(who, b):
        return att.at[who, pl.ds(b * WIN, WIN)]

    def att_send(b):
        mine = att_piece(t, b)
        send(mine, mine, t_send.at[2], t_recv.at[2, b], {"tp": t_o}, False)
        send(mine, mine, t_send.at[0], t_recv.at[0, b], {"tp": t_r}, False)
        send(mine, mine, t_send.at[1], t_recv.at[1, b], {"tp": t_l}, False)
        send(mine, mine, tsib_send.at[0], tsib_recv.at[0], {"tp": sib}, False)

    def att_take(b):
        for role, who in ((0, t_l), (1, t_r), (2, t_o)):
            got = att_piece(who, b)
            recv(got, t_recv.at[role, b], {"tp": who})
            send(got, got, tsib_send.at[1 + role], tsib_recv.at[1 + role], {"tp": sib}, False)

    order = [*range(1, blocks - 1), 0, blocks - 1]
    for n, b in enumerate(order):
        if n == blocks - 2:
            @pl.when(z < n_sp - 1)
            def _():
                recv(kv.at[pl.ds(WIN + count, WIN)], h_recv.at[0], {"sp": z + 1})

            @pl.when(z > 0)
            def _():
                recv(kv.at[pl.ds(0, WIN)], h_recv.at[1], {"sp": z - 1})

        attend(b)
        att_send(b)
        if n >= 2:
            att_take(order[n - 2])
    att_take(order[-2])
    att_take(order[-1])
    for role, xx in ((0, x), (1, xl), (2, xr), (3, xo)):
        recv(att.at[xx * 2 + 1 - c], tsib_recv.at[role], {"tp": sib})

    before = len(started)
    here = pl.ds(pl.multiple_of(t * width, LANES), width)
    for n, xx in enumerate((xo, xr, xl, x)):
        part = pl.ds(pl.multiple_of(xx * WIN, WIN), WIN)
        y = jnp.zeros((WIN, width), f32)
        for i in range(n_x):
            lhs = jnp.concatenate([att[2 * i, part, :], att[2 * i + 1, part, :]], axis=1)
            y = y + jnp.dot(lhs, ow[2 * i * LANES : 2 * (i + 1) * LANES, :], preferred_element_type=f32)
        ysend[2 * n] = y[:group].astype(bf16)
        ysend[2 * n + 1] = y[group:].astype(bf16)
        if n < 3:
            for k in range(2):
                send(ysend.at[2 * n + k], out.at[:, here], y_send.at[2 * n + k], y_recv.at[2 * n + c], {"tp": xx * 2 + k})
        else:
            send(ysend.at[2 * n + 1 - c], out.at[:, here], y_send.at[6], y_recv.at[6], {"tp": sib})
            keep = pltpu.make_async_copy(ysend.at[2 * n + c], out.at[:, here], load_sem.at[14])
            keep.start()
    for n, who in enumerate((t_r, t_l, t_o)):
        sent(att.at[t], t_send.at[n], {"tp": who})
    for n, who in enumerate((t, t_l, t_r, t_o)):
        sent(att.at[who], tsib_send.at[n], {"tp": sib})
    for copy in started[:before]:
        copy.wait_send()

    @pl.when(z > 0)
    def _():
        sent(kv.at[pl.ds(WIN, WIN)], h_send.at[0], {"sp": z - 1})

    @pl.when(z < n_sp - 1)
    def _():
        sent(kv.at[pl.ds(count, WIN)], h_send.at[1], {"sp": z + 1})

    @pl.when(c == 1)
    def _():
        for n, xx in enumerate((xr, xl, xo)):
            sent(mt.at[xx], x_send.at[n], {"tp": sib})
        sent(mpair.at[1], pair_send.at[0], {"tp": sib})
        sent(cown, pair_send.at[1], {"tp": sib})
        for n, (g, who) in enumerate(((t, t_r), (t, t_l), (sib, t_r), (sib, t_l), (t_r, t_l), (zero_l, t_r))):
            sent(rows.at[g], ag_send.at[n], {"tp": who})
        for g in (t, t_r, t_l, zero_l, zero_r, t_o, zero_o):
            sent(rows.at[g], sib_send.at[g], {"tp": sib})
    @pl.when(c == 0)
    def _():
        sent(rows.at[t], sib_send.at[t], {"tp": sib})
        for n, who in enumerate((sib, t_o + 1, t_r + 1, t_l + 1)):
            sent(mt.at[x], x_send.at[n], {"tp": who})

        @pl.when(z == center)
        def _():
            sent(mall, tot_send, {"sp": 0})

        @pl.when(z != lead)
        def _():
            sent(cpair, c_send.at[0], {"sp": lead})

        @pl.when(z == lead)
        def _():
            def given(i):
                sent(cg.at[:, pl.ds(SPAN * team, SPAN)], bl_send.at[i], {"sp": SPAN * i + center})

            each(0, team, given)
            each(team + 1, teams, given)

            for n, who in enumerate(members):
                for k in range(2):
                    sent(cg.at[k], bm_send.at[2 * n + k], {"sp": who})
            sent(cg.at[1], bm_send.at[2 * SPAN - 2], {"tp": sib})

        @pl.when(z != center)
        def _():
            sent(mpair, m_send.at[0], {"sp": center})

    for n, xx in enumerate((xo, xl, xr)):
        for k in range(2):
            cols = pl.ds(pl.multiple_of((xx * 2 + k) * width, LANES), width)
            recv(out.at[:, cols], y_recv.at[2 * n + k], {"tp": xx * 2 + k})
    recv(out.at[:, pl.ds(pl.multiple_of(sib * width, LANES), width)], y_recv.at[6], {"tp": sib})
    keep.wait()
    gates.wait()
    for copy in started[before:]:
        copy.wait_send()


def local(n_sp, n_tp, latent, context, conditioning, norm_gain, *rest):
    shift_w, scale_w, gate_w, q_w, k_w, v_w, o_w, sink = rest
    group, depth = latent.shape
    n_ctx = context.shape[0]
    count = n_tp * group
    width = shift_w.shape[1]
    blocks = count // WIN
    chunks = group // 16
    row_tab, col_tab = rope_tables(n_sp * count // GRID_W)
    any_space = pl.BlockSpec(memory_space=pl.ANY)
    dma = pltpu.SemaphoreType.DMA
    blended, gate = pl.pallas_call(
        functools.partial(kernel, n_sp, n_tp),
        out_shape=(jax.ShapeDtypeStruct((group, depth), bf16), jax.ShapeDtypeStruct((1, depth), f32)),
        in_specs=[any_space] * 14,
        out_specs=(any_space, any_space),
        scratch_shapes=[
            pltpu.VMEM((n_tp, group, depth), bf16),
            pltpu.VMEM((depth, 2 * LANES), bf16),
            pltpu.VMEM((2 * HD, depth), bf16),
            pltpu.VMEM(o_w.shape, bf16),
            pltpu.VMEM((3, *shift_w.shape), bf16),
            pltpu.VMEM((n_ctx, depth), bf16),
            pltpu.VMEM((2, n_sp, n_ctx, LANES), bf16),
            pltpu.VMEM((n_ctx, LANES), bf16),
            pltpu.VMEM((2, n_ctx, LANES), bf16),
            pltpu.VMEM((2, 16, LANES), f32),
            pltpu.VMEM((n_sp - 1, 2, 16, LANES), f32),
            pltpu.VMEM((2, 16, LANES), f32),
            pltpu.VMEM((n_tp // 2, 2, 16, LANES), f32),
            pltpu.VMEM((n_tp, group, LANES), f32),
            pltpu.VMEM((1, depth), f32),
            pltpu.VMEM((1, depth), f32),
            pltpu.VMEM((1, depth), f32),
            pltpu.VMEM((count, LANES), bf16),
            pltpu.VMEM((count + 2 * WIN, LANES), bf16),
            pltpu.VMEM((n_sp * n_ctx, LANES), bf16),
            pltpu.VMEM((n_tp, count, LANES), bf16),
            pltpu.VMEM((n_tp, group, width), bf16),
            pltpu.VMEM((count // GRID_W, 4 * LANES), f32),
            pltpu.VMEM((GRID_W, 4 * LANES), f32),
            pltpu.VMEM((1, conditioning.shape[0]), bf16),
            pltpu.VMEM((1, depth), f32),
            pltpu.VMEM((1, sink.shape[0]), f32),
            pltpu.SemaphoreType.REGULAR,
            dma((16,)),
            dma((3,)),
            dma((3,)),
            dma((1,)),
            dma,
            dma,
            dma,
            dma((1,)),
            dma((SPAN,)),
            dma((n_sp // SPAN,)),
            dma((n_sp // SPAN,)),
            dma((2 * SPAN,)),
            dma((6,)),
            dma((6, chunks)),
            dma((n_tp,)),
            dma((n_tp,)),
            dma((4,)),
            dma((n_tp // 2,)),
            dma((2,)),
            dma((2,)),
            dma((3,)),
            dma((3, blocks)),
            dma((4,)),
            dma((4,)),
            dma((8,)),
            dma((8,)),
        ],
        compiler_params=pltpu.CompilerParams(
            collective_id=0, has_side_effects=True, vmem_limit_bytes=56 * 1024 * 1024
        ),
    )(
        latent,
        context,
        conditioning.reshape(1, -1),
        norm_gain.reshape(1, -1),
        shift_w,
        scale_w,
        gate_w,
        q_w,
        k_w.T,
        v_w.T,
        o_w,
        sink.reshape(1, -1),
        jnp.asarray(row_tab),
        jnp.asarray(col_tab),
    )
    return (latent.astype(f32) + gate * blended.astype(f32)).astype(bf16)


def solution(mesh):
    in_specs = (
        P(("grp", "sp", "tp"), None),
        P(("grp", "sp"), None),
        P(("grp", "sp")),
        P(),
        P("sp", "tp"),
        P("sp", "tp"),
        P("sp", "tp"),
        P(None, "tp"),
        P(None, "tp"),
        P(None, "tp"),
        P(None, "tp"),
        P("tp"),
    )
    return jax.shard_map(
        functools.partial(local, mesh.shape["sp"], mesh.shape["tp"]),
        mesh=mesh,
        in_specs=in_specs,
        out_specs=P(("grp", "sp", "tp"), None),
        check_vma=False,
    )
```

```python
import functools

import jax
import jax.numpy as jnp
import numpy as np
from jax import lax
from jax.experimental import pallas as pl
from jax.experimental.pallas import tpu as pltpu
from jax.sharding import PartitionSpec as P

HEADS = 16
KV_HEADS = 8
HD = 64
GRID_W = 64
WIN = 128
SPAN = 4
LATEST = 4
LANES = 128
COLS = 512

epsilon = 1e-06
rope_base = 10000.0
neg_large = -1e30
MESH = pl.DeviceIdType.MESH
f32 = jnp.float32
bf16 = jnp.bfloat16


def rope_tables(grid_rows):
    lane = np.arange(LANES)
    d = lane % HD
    freq = rope_base ** (-(d % 16) / 16.0)
    is_row = d < HD // 2
    sign = np.where(d % 32 < 16, -1.0, 1.0)
    is_key = lane < HD

    def table(count, own):
        angle = np.arange(count)[:, None] * freq[None, :]
        c = np.where(own, np.cos(angle), 0.0)
        s = np.where(own, np.sin(angle) * sign, 0.0)
        scale = HD**-0.5
        ck = np.where(is_key, c, 0.0)
        sk = np.where(is_key, s, 0.0)
        return np.concatenate([c * scale, s * scale, ck, sk], axis=1)

    rows = table(grid_rows, is_row)
    cols = table(GRID_W, ~is_row)
    cols[:, 2 * LANES : 3 * LANES] += np.where(is_key, 0.0, 1.0)
    return rows.astype(np.float32), cols.astype(np.float32)


def kernel(
    n_sp,
    n_tp,
    latent,
    context,
    cond_in,
    gain_in,
    shift_w,
    scale_w,
    gate_w,
    q_w,
    k_t,
    v_t,
    o_w,
    sink_in,
    row_tab,
    col_tab,
    out,
    gate_out,
    rows,
    w,
    kvt,
    ow,
    mw,
    ctx_rows,
    cg,
    cown,
    cpair,
    mpair,
    mall,
    msum,
    mt,
    inv,
    a_vec,
    s_vec,
    g_vec,
    qrot,
    kv,
    ctx,
    att,
    ysend,
    rt,
    ct,
    cond,
    gain,
    sink,
    hello,
    load_sem,
    pair_send,
    pair_recv,
    m_send,
    m_recv,
    tot_send,
    tot_recv,
    c_send,
    p_recv,
    b_recv,
    bl_send,
    bm_send,
    ag_send,
    ag_recv,
    sib_send,
    sib_recv,
    x_send,
    x_recv,
    h_send,
    h_recv,
    t_send,
    t_recv,
    tsib_send,
    tsib_recv,
    y_send,
    y_recv,
):
    n_x = n_tp // 2
    z = lax.axis_index("sp")
    t = lax.axis_index("tp")
    x = t // 2
    c = t % 2
    xr = (x + 1) % n_x
    xl = (x + n_x - 1) % n_x
    xo = (x + 2) % n_x
    sib = x * 2 + (1 - c)
    t_r, t_l, t_o = xr * 2 + c, xl * 2 + c, xo * 2 + c
    group = latent.shape[0]
    count = n_tp * group
    depth = latent.shape[1]
    chunks = group // 16
    width = shift_w.shape[1]
    per = width // LANES

    late = (z == 0) & (x == 0)
    center = 1

    started = []

    def send(src, dst, ss, rs, dev, keep=True):
        copy = pltpu.make_async_remote_copy(
            src_ref=src, dst_ref=dst, send_sem=ss, recv_sem=rs, device_id=dev, device_id_type=MESH
        )
        copy.start()
        if keep:
            started.append(copy)

    def recv(dst, rs, dev):
        pltpu.make_async_remote_copy(
            src_ref=dst, dst_ref=dst, send_sem=rs, recv_sem=rs, device_id=dev, device_id_type=MESH
        ).wait_recv()

    def sent(src, ss, dev):
        pltpu.make_async_remote_copy(
            src_ref=src, dst_ref=src, send_sem=ss, recv_sem=ss, device_id=dev, device_id_type=MESH
        ).wait_send()

    def each(lo, hi, body):
        def step(i, carry):
            body(i)
            return carry

        lax.fori_loop(lo, hi, step, 0)

    barrier = pltpu.get_barrier_semaphore()

    def greet(dev):
        pl.semaphore_signal(barrier, inc=1, device_id=dev, device_id_type=MESH)

    @pl.when(c == 1)
    def _():
        for who in (sib, t_l):
            greet({"tp": who})

    slot = (z + 1) % n_sp
    teams = n_sp // SPAN
    team = slot // SPAN
    lead = SPAN * team + center
    members = [(z + n_sp - 1) % n_sp, (z + 1) % n_sp, (z + n_sp - 2) % n_sp]
    places = (1, 3, 0)

    @pl.when((c == 0) & (z == center))
    def _():
        each(0, center, lambda i: greet({"sp": i}))
        each(center + 1, n_sp, lambda i: greet({"sp": i}))

    @pl.when((c == 0) & (z == lead))
    def _():
        for i in members:
            greet({"sp": i})
        each(team + 1, teams, lambda i: greet({"sp": SPAN * i + center}))

    grid_rows = count // GRID_W
    loads = {}

    def load(name, src, dst):
        copy = pltpu.make_async_copy(src, dst, load_sem.at[len(loads)])
        copy.start()
        loads[name] = copy

    load("cond", cond_in, cond)
    load("m0", shift_w, mw.at[0])
    load("m1", scale_w, mw.at[1])
    load("m2", gate_w, mw.at[2])
    load("rows", latent, rows.at[t])
    load("gain", gain_in, gain)
    load("kw", k_t, kvt.at[pl.ds(0, HD)])
    load("vw", v_t, kvt.at[pl.ds(HD, HD)])
    load("ctx", context, ctx_rows)
    load("qw", q_w, w.at[:, pl.ds(0, LANES)])
    load("rt", row_tab.at[pl.ds(pl.multiple_of(z * grid_rows, 8), grid_rows)], rt)
    load("ct", col_tab, ct)
    load("sink", sink_in, sink)
    load("ow", o_w, ow)

    def contact():
        pl.semaphore_wait(barrier, 1 + jnp.where(z == center, 0, 1) + jnp.where(z == lead, team, 1))

    def modulation():
        loads["cond"].wait()
        cv = cond[...].astype(f32)
        lifted = jnp.broadcast_to((cv / (1.0 + jnp.exp(-cv))).astype(bf16), (16, cv.shape[1]))
        for i in range(3):
            loads["m%d" % i].wait()
            part = jnp.dot(lifted, mw[i], preferred_element_type=f32)
            for j in range(per):
                mpair[c, per * i + j : per * i + j + 1, :] = part[0:1, j * LANES : (j + 1) * LANES]
        mpair[c, 3 * per : 16, :] = jnp.zeros((16 - 3 * per, LANES), f32)

    n_ctx = ctx_rows.shape[0]

    def own_context():
        for name in ("kw", "vw", "gain", "ctx"):
            loads[name].wait()
        for i in range(depth // COLS):
            w[i * COLS : (i + 1) * COLS, LANES : 2 * LANES] = kvt[:, i * COLS : (i + 1) * COLS].T
        sq = jnp.zeros((n_ctx, LANES), f32)
        for i in range(depth // LANES):
            v = ctx_rows[:, i * LANES : (i + 1) * LANES].astype(f32)
            sq = sq + v * v
        cinv = lax.rsqrt(jnp.sum(sq, axis=1, keepdims=True) * (1.0 / depth) + epsilon)
        acc = jnp.zeros((n_ctx, LANES), f32)
        for i in range(depth // COLS):
            part = slice(i * COLS, (i + 1) * COLS)
            v = ctx_rows[:, part].astype(f32) * cinv * gain[:, part]
            acc = acc + jnp.dot(v.astype(bf16), w[part, LANES : 2 * LANES], preferred_element_type=f32)
        cown[...] = acc.astype(bf16)

    def row_stats(g):
        sq = jnp.zeros((group, LANES), f32)
        for i in range(depth // LANES):
            v = rows[g, :, i * LANES : (i + 1) * LANES].astype(f32)
            sq = sq + v * v
        r = lax.rsqrt(jnp.sum(sq, axis=1, keepdims=True) * (1.0 / depth) + epsilon)
        inv[g] = jnp.broadcast_to(r, (group, LANES))

    @pl.when(z == 0)
    def _():
        kv[:WIN, :] = jnp.zeros((WIN, LANES), bf16)

    @pl.when(z == n_sp - 1)
    def _():
        kv[WIN + count :, :] = jnp.zeros((WIN, LANES), bf16)

    def piece(g, q):
        return rows.at[g, pl.ds(16 * q, 16)]

    zero_l, zero_r, zero_o = t_l - c, t_r - c, t_o - c

    def meet():
        pl.semaphore_wait(hello, 1)
        send(mpair.at[1], mpair.at[1], pair_send.at[0], pair_recv.at[0], {"tp": sib}, False)

    def hand_context():
        send(cown, cpair.at[1], pair_send.at[1], pair_recv.at[1], {"tp": sib}, False)

    def sibling_rows():
        recv(rows.at[sib], sib_recv.at[sib], {"tp": sib})
        for q in range(chunks):
            send(piece(sib, q), piece(sib, q), ag_send.at[2], ag_recv.at[2, q], {"tp": t_r}, False)
            send(piece(sib, q), piece(sib, q), ag_send.at[3], ag_recv.at[3, q], {"tp": t_l}, False)

    def hand(groups):
        for g in groups:
            send(rows.at[g], rows.at[g], sib_send.at[g], sib_recv.at[g], {"tp": sib}, False)

    def own_block(k, i):
        return cg.at[k, pl.ds(SPAN * i, SPAN)]

    def block(i):
        return cg.at[:, pl.ds(SPAN * i, SPAN)]

    def hand_far(i):
        for k in range(2):
            send(own_block(k, i), own_block(k, i), bm_send.at[4 + k], b_recv.at[i], {"sp": members[2], "tp": t + k}, False)

    def give(i):
        send(block(team), block(team), bl_send.at[i], b_recv.at[team], {"sp": SPAN * i + center}, False)

    @pl.when(c == 1)
    def _():
        modulation()
        loads["rows"].wait()
        pl.semaphore_wait(barrier, 1)
        pl.when(~late & (z >= n_sp // 2))(meet)
        for q in range(chunks):
            send(piece(t, q), piece(t, q), ag_send.at[0], ag_recv.at[0, q], {"tp": t_r}, False)
        own_context()
        pl.when(~late & (z >= n_sp // 2))(hand_context)
        recv(piece(t_l, 0), ag_recv.at[0, 0], {"tp": t_l})
        for q in range(chunks):
            send(piece(t, q), piece(t, q), ag_send.at[1], ag_recv.at[1, q], {"tp": t_l}, False)
        pl.when(~late & (z < n_sp // 2))(meet)
        pl.when(~late & (z < n_sp // 2))(hand_context)
        pl.when(~late)(sibling_rows)
        for q in range(chunks):
            recv(piece(t_r, q), ag_recv.at[1, q], {"tp": t_r})
            send(piece(t_r, q), piece(t_r, q), ag_send.at[4], ag_recv.at[4, q], {"tp": t_l}, False)
        for q in range(1, chunks):
            recv(piece(t_l, q), ag_recv.at[0, q], {"tp": t_l})
        pl.when(~late)(functools.partial(hand, (t, t_r, t_l)))
        row_stats(t)
        row_stats(t_l)
        row_stats(t_r)
        for q in range(chunks):
            recv(piece(zero_l, q), ag_recv.at[2, q], {"tp": t_l})
            send(piece(zero_l, q), piece(zero_l, q), ag_send.at[5], ag_recv.at[5, q], {"tp": t_r}, False)
        for q in range(chunks):
            recv(piece(zero_r, q), ag_recv.at[3, q], {"tp": t_r})
        pl.when(~late)(functools.partial(hand, (zero_l, zero_r)))
        row_stats(zero_l)
        row_stats(zero_r)
        for q in range(chunks):
            recv(piece(t_o, q), ag_recv.at[4, q], {"tp": t_r})
        pl.when(~late)(functools.partial(hand, (t_o,)))
        row_stats(t_o)
        for q in range(chunks):
            recv(piece(zero_o, q), ag_recv.at[5, q], {"tp": t_l})
        pl.when(~late)(functools.partial(hand, (zero_o,)))
        row_stats(zero_o)

        @pl.when(late)
        def _():
            meet()
            hand_context()
            sibling_rows()
            hand((t, t_r, t_l, zero_l, zero_r, t_o, zero_o))

        row_stats(sib)
        recv(mt.at[x], x_recv.at[x], {"tp": sib})
        for n, (xx, who) in enumerate(((xr, zero_r), (xl, zero_l), (xo, zero_o))):
            recv(mt.at[xx], x_recv.at[xx], {"tp": who})
            send(mt.at[xx], mt.at[xx], x_send.at[n], x_recv.at[xx], {"tp": sib}, False)

    @pl.when(c == 0)
    def _():
        modulation()
        loads["rows"].wait()
        contact()
        pl.semaphore_signal(hello, inc=1, device_id={"tp": sib}, device_id_type=MESH)
        send(rows.at[t], rows.at[t], sib_send.at[t], sib_recv.at[t], {"tp": sib}, False)
        recv(mpair.at[1], pair_recv.at[0], {"tp": sib})

        @pl.when(z != center)
        def _():
            send(mpair, mall.at[z - jnp.where(z > center, 1, 0)], m_send.at[0], m_recv, {"sp": center}, False)

        own_context()
        cpair[0] = cown[...]
        row_stats(t)
        recv(cpair.at[1], pair_recv.at[1], {"tp": sib})

        def tell_sum():
            recv(mall, m_recv, {"sp": 0})
            tot = mpair[...]
            for i in range(n_sp - 1):
                tot = tot + mall[i]
            msum[...] = tot

            def tell(i):
                send(msum, mt.at[x], tot_send, tot_recv, {"sp": i}, False)

            each(0, center, tell)
            each(center + 1, n_sp, tell)
            mt[x] = tot

        def sum_in():
            recv(mt.at[x], tot_recv, {"sp": center})

        def rows_in(groups):
            for g in groups:
                recv(rows.at[g], sib_recv.at[g], {"tp": sib})
                row_stats(g)

        def early_rows():
            rows_in((sib, t_r + 1, t_l + 1))

        @pl.when(z != lead)
        def _():
            send(cpair, cg.at[:, slot], c_send.at[0], p_recv.at[slot % SPAN], {"sp": lead}, False)

        def hand_near(i):
            for n, who in enumerate(members[:2]):
                for k in range(2):
                    send(own_block(k, i), own_block(k, i), bm_send.at[2 * n + k], b_recv.at[i], {"sp": who, "tp": t + k}, False)
            send(own_block(1, i), own_block(1, i), bm_send.at[2 * SPAN - 2], b_recv.at[i], {"tp": sib}, False)

        def hand_block(i):
            hand_near(i)
            hand_far(i)

        def member_in(n):
            recv(cg.at[:, SPAN * team + places[n]], p_recv.at[places[n]], {"sp": members[n]})

        def got(i):
            recv(block(i), b_recv.at[i], {"sp": SPAN * i + center})

        def answer(i):
            got(i)
            give(i)
            hand_block(i)

        def follow(i):
            got(i)
            hand_block(i)

        def near_in(i):
            got(i)
            hand_near(i)

        @pl.when(z == lead)
        def _():
            for k in range(2):
                cg[k, slot] = cpair[k]
            member_in(1)
            member_in(0)

        @pl.when(z == center)
        def _():
            early_rows()
            each(1, teams - LATEST, near_in)
        @pl.when((z == lead) & (z != center))
        def _():
            member_in(2)
            each(0, team, give)
            hand_block(team)
            each(team + 1, teams, answer)

        pl.when(z != center)(early_rows)
        pl.when(z == center)(tell_sum)
        pl.when(z != center)(sum_in)
        for n, who in enumerate((sib, t_o + 1, t_r + 1, t_l + 1)):
            send(mt.at[x], mt.at[x], x_send.at[n], x_recv.at[x], {"tp": who}, False)

        @pl.when(z == center)
        def _():
            member_in(2)
            hand_near(0)
            each(1, teams - LATEST, give)
            each(teams - LATEST, teams, near_in)

        @pl.when((z == lead) & (z != center))
        def _():
            each(0, team, follow)

        rows_in((t_o + 1, t_r, t_l, t_o))
        for xx in (xr, xl, xo):
            recv(mt.at[xx], x_recv.at[xx], {"tp": sib})

    for j in range(n_tp):
        for i in range(per):
            part = slice(j * width + i * LANES, j * width + (i + 1) * LANES)
            s_vec[:, part] = mt[j // 2, j % 2, i : i + 1, :]
            a_vec[:, part] = gain[:, part] * (1.0 + mt[j // 2, j % 2, per + i : per + i + 1, :])
            g_vec[:, part] = mt[j // 2, j % 2, 2 * per + i : 2 * per + i + 1, :]
    gates = pltpu.make_async_copy(g_vec, gate_out, load_sem.at[15])
    gates.start()
    for name in ("rt", "ct", "qw", "ow", "sink"):
        loads[name].wait()

    lane = lax.broadcasted_iota(jnp.int32, (1, LANES), 1)
    first = lane % 32 < 16

    def swapped(v):
        return jnp.where(first, pltpu.roll(v, LANES - 16, 1), pltpu.roll(v, 16, 1))

    def project(gs):
        acc = jnp.zeros((len(gs) * group, 2 * LANES), f32)
        for i in range(depth // COLS):
            part = slice(i * COLS, (i + 1) * COLS)
            a = a_vec[:, part]
            s = s_vec[:, part]
            tiles = []
            for g in gs:
                r = jnp.concatenate([inv[g]] * (COLS // LANES), axis=1)
                tiles.append((rows[g, :, part].astype(f32) * r * a + s).astype(bf16))
            acc = acc + jnp.dot(jnp.concatenate(tiles, axis=0), w[part, :], preferred_element_type=f32)
        for n, g in enumerate(gs):
            fac = rt[g : g + 1, :] + ct[...]
            vq = acc[n * group : (n + 1) * group, :LANES]
            vk = acc[n * group : (n + 1) * group, LANES:]
            q2 = vq * fac[:, :LANES] + swapped(vq) * fac[:, LANES : 2 * LANES]
            k2 = vk * fac[:, 2 * LANES : 3 * LANES] + swapped(vk) * fac[:, 3 * LANES :]
            qrot[g * group : (g + 1) * group, :] = q2.astype(bf16)
            kv[WIN + g * group : WIN + (g + 1) * group, :] = k2.astype(bf16)

    project((0, 1, n_tp - 2, n_tp - 1))

    @pl.when(z > 0)
    def _():
        send(kv.at[pl.ds(WIN, WIN)], kv.at[pl.ds(WIN + count, WIN)], h_send.at[0], h_recv.at[0], {"sp": z - 1}, False)

    @pl.when(z < n_sp - 1)
    def _():
        send(kv.at[pl.ds(count, WIN)], kv.at[pl.ds(0, WIN)], h_send.at[1], h_recv.at[1], {"sp": z + 1}, False)

    @pl.when((c == 0) & (z == center))
    def _():
        each(teams - LATEST, teams, give)
        each(0, teams, hand_far)

    project(tuple(range(2, n_tp - 2)))

    @pl.when((c == 1) | (z != lead))
    def _():
        for i in range(n_sp // SPAN):
            recv(own_block(c, i), b_recv.at[i], {"sp": lead, "tp": t - c})

    for j in range(n_sp):
        ctx[pl.ds(j * n_ctx, n_ctx), :] = cg[c, j]
    rows2 = 2 * WIN
    qi = lax.broadcasted_iota(jnp.int32, (rows2, WIN), 0) % WIN
    ki = lax.broadcasted_iota(jnp.int32, (rows2, WIN), 1)
    head1 = lax.broadcasted_iota(jnp.int32, (rows2, 1), 0) >= WIN
    sink_col = jnp.where(head1, sink[0:1, 1:2], sink[0:1, 0:1])
    is_key = lane < HD
    contract = (((1,), (1,)), ((), ()))
    blocks = count // WIN

    def attend(b):
        qb = qrot[b * WIN : (b + 1) * WIN, :].astype(f32)
        q0 = jnp.where(is_key, qb, 0.0).astype(bf16)
        q1 = jnp.where(is_key, pltpu.roll(qb, HD, 1), 0.0).astype(bf16)
        qq = jnp.concatenate([q0, q1], axis=0)
        band = kv[b * WIN : (b + 3) * WIN, :]
        whole = ctx[...]
        s_band = lax.dot_general(qq, band, contract, preferred_element_type=f32)
        s_ctx = lax.dot_general(qq, whole, contract, preferred_element_type=f32)
        left = ki >= qi
        right = ki <= qi
        if b == 0:
            left = left & (z > 0)
        if b == blocks - 1:
            right = right & (z < n_sp - 1)
        s0 = jnp.where(left, s_band[:, :WIN], neg_large)
        s1 = s_band[:, WIN : 2 * WIN]
        s2 = jnp.where(right, s_band[:, 2 * WIN :], neg_large)
        top = jnp.maximum(jnp.maximum(s0, s1), s2)
        for i in range(whole.shape[0] // LANES):
            top = jnp.maximum(top, s_ctx[:, i * LANES : (i + 1) * LANES])
        m = jnp.maximum(jnp.max(top, axis=1, keepdims=True), sink_col)
        e0 = jnp.exp(s0 - m)
        e1 = jnp.exp(s1 - m)
        e2 = jnp.exp(s2 - m)
        ec = jnp.exp(s_ctx - m)
        tot = e0 + e1 + e2
        for i in range(whole.shape[0] // LANES):
            tot = tot + ec[:, i * LANES : (i + 1) * LANES]
        den = jnp.sum(tot, axis=1, keepdims=True) + jnp.exp(sink_col - m)
        r = 1.0 / den
        p_band = jnp.concatenate([e0, e1, e2], axis=1) * r
        o = jnp.dot(p_band.astype(bf16), band, preferred_element_type=f32) + jnp.dot(
            (ec * r).astype(bf16), whole, preferred_element_type=f32
        )
        res = jnp.where(is_key, pltpu.roll(o[:WIN], HD, 1), o[WIN:]).astype(bf16)
        att[t, b * WIN : (b + 1) * WIN, :] = res

    def att_piece(who, b):
        return att.at[who, pl.ds(b * WIN, WIN)]

    def att_send(b):
        mine = att_piece(t, b)
        send(mine, mine, t_send.at[2], t_recv.at[2, b], {"tp": t_o}, False)
        send(mine, mine, t_send.at[0], t_recv.at[0, b], {"tp": t_r}, False)
        send(mine, mine, t_send.at[1], t_recv.at[1, b], {"tp": t_l}, False)
        send(mine, mine, tsib_send.at[0], tsib_recv.at[0], {"tp": sib}, False)

    def att_take(b):
        for role, who in ((0, t_l), (1, t_r), (2, t_o)):
            got = att_piece(who, b)
            recv(got, t_recv.at[role, b], {"tp": who})
            send(got, got, tsib_send.at[1 + role], tsib_recv.at[1 + role], {"tp": sib}, False)

    order = [*range(1, blocks - 1), 0, blocks - 1]
    for n, b in enumerate(order):
        if n == blocks - 2:
            @pl.when(z < n_sp - 1)
            def _():
                recv(kv.at[pl.ds(WIN + count, WIN)], h_recv.at[0], {"sp": z + 1})

            @pl.when(z > 0)
            def _():
                recv(kv.at[pl.ds(0, WIN)], h_recv.at[1], {"sp": z - 1})

        attend(b)
        att_send(b)
    for b in order:
        att_take(b)
    for role, xx in ((0, x), (1, xl), (2, xr), (3, xo)):
        recv(att.at[xx * 2 + 1 - c], tsib_recv.at[role], {"tp": sib})

    before = len(started)
    here = pl.ds(pl.multiple_of(t * width, LANES), width)
    for n, xx in enumerate((xo, xr, xl, x)):
        part = pl.ds(pl.multiple_of(xx * WIN, WIN), WIN)
        y = jnp.zeros((WIN, width), f32)
        for i in range(n_x):
            lhs = jnp.concatenate([att[2 * i, part, :], att[2 * i + 1, part, :]], axis=1)
            y = y + jnp.dot(lhs, ow[2 * i * LANES : 2 * (i + 1) * LANES, :], preferred_element_type=f32)
        ysend[2 * n] = y[:group].astype(bf16)
        ysend[2 * n + 1] = y[group:].astype(bf16)
        if n < 3:
            for k in range(2):
                send(ysend.at[2 * n + k], out.at[:, here], y_send.at[2 * n + k], y_recv.at[2 * n + c], {"tp": xx * 2 + k})
        else:
            send(ysend.at[2 * n + 1 - c], out.at[:, here], y_send.at[6], y_recv.at[6], {"tp": sib})
            keep = pltpu.make_async_copy(ysend.at[2 * n + c], out.at[:, here], load_sem.at[14])
            keep.start()
    for n, who in enumerate((t_r, t_l, t_o)):
        sent(att.at[t], t_send.at[n], {"tp": who})
    for n, who in enumerate((t, t_l, t_r, t_o)):
        sent(att.at[who], tsib_send.at[n], {"tp": sib})
    for copy in started[:before]:
        copy.wait_send()

    @pl.when(z > 0)
    def _():
        sent(kv.at[pl.ds(WIN, WIN)], h_send.at[0], {"sp": z - 1})

    @pl.when(z < n_sp - 1)
    def _():
        sent(kv.at[pl.ds(count, WIN)], h_send.at[1], {"sp": z + 1})

    @pl.when(c == 1)
    def _():
        for n, xx in enumerate((xr, xl, xo)):
            sent(mt.at[xx], x_send.at[n], {"tp": sib})
        sent(mpair.at[1], pair_send.at[0], {"tp": sib})
        sent(cown, pair_send.at[1], {"tp": sib})
        for n, (g, who) in enumerate(((t, t_r), (t, t_l), (sib, t_r), (sib, t_l), (t_r, t_l), (zero_l, t_r))):
            sent(rows.at[g], ag_send.at[n], {"tp": who})
        for g in (t, t_r, t_l, zero_l, zero_r, t_o, zero_o):
            sent(rows.at[g], sib_send.at[g], {"tp": sib})
    @pl.when(c == 0)
    def _():
        sent(rows.at[t], sib_send.at[t], {"tp": sib})
        for n, who in enumerate((sib, t_o + 1, t_r + 1, t_l + 1)):
            sent(mt.at[x], x_send.at[n], {"tp": who})

        @pl.when(z == center)
        def _():
            sent(mall, tot_send, {"sp": 0})

        @pl.when(z != lead)
        def _():
            sent(cpair, c_send.at[0], {"sp": lead})

        @pl.when(z == lead)
        def _():
            def given(i):
                sent(cg.at[:, pl.ds(SPAN * team, SPAN)], bl_send.at[i], {"sp": SPAN * i + center})

            each(0, team, given)
            each(team + 1, teams, given)

            for n, who in enumerate(members):
                for k in range(2):
                    sent(cg.at[k], bm_send.at[2 * n + k], {"sp": who})
            sent(cg.at[1], bm_send.at[2 * SPAN - 2], {"tp": sib})

        @pl.when(z != center)
        def _():
            sent(mpair, m_send.at[0], {"sp": center})

    for n, xx in enumerate((xo, xl, xr)):
        for k in range(2):
            cols = pl.ds(pl.multiple_of((xx * 2 + k) * width, LANES), width)
            recv(out.at[:, cols], y_recv.at[2 * n + k], {"tp": xx * 2 + k})
    recv(out.at[:, pl.ds(pl.multiple_of(sib * width, LANES), width)], y_recv.at[6], {"tp": sib})
    keep.wait()
    gates.wait()
    for copy in started[before:]:
        copy.wait_send()


def local(n_sp, n_tp, latent, context, conditioning, norm_gain, *rest):
    shift_w, scale_w, gate_w, q_w, k_w, v_w, o_w, sink = rest
    group, depth = latent.shape
    n_ctx = context.shape[0]
    count = n_tp * group
    width = shift_w.shape[1]
    blocks = count // WIN
    chunks = group // 16
    row_tab, col_tab = rope_tables(n_sp * count // GRID_W)
    any_space = pl.BlockSpec(memory_space=pl.ANY)
    dma = pltpu.SemaphoreType.DMA
    blended, gate = pl.pallas_call(
        functools.partial(kernel, n_sp, n_tp),
        out_shape=(jax.ShapeDtypeStruct((group, depth), bf16), jax.ShapeDtypeStruct((1, depth), f32)),
        in_specs=[any_space] * 14,
        out_specs=(any_space, any_space),
        scratch_shapes=[
            pltpu.VMEM((n_tp, group, depth), bf16),
            pltpu.VMEM((depth, 2 * LANES), bf16),
            pltpu.VMEM((2 * HD, depth), bf16),
            pltpu.VMEM(o_w.shape, bf16),
            pltpu.VMEM((3, *shift_w.shape), bf16),
            pltpu.VMEM((n_ctx, depth), bf16),
            pltpu.VMEM((2, n_sp, n_ctx, LANES), bf16),
            pltpu.VMEM((n_ctx, LANES), bf16),
            pltpu.VMEM((2, n_ctx, LANES), bf16),
            pltpu.VMEM((2, 16, LANES), f32),
            pltpu.VMEM((n_sp - 1, 2, 16, LANES), f32),
            pltpu.VMEM((2, 16, LANES), f32),
            pltpu.VMEM((n_tp // 2, 2, 16, LANES), f32),
            pltpu.VMEM((n_tp, group, LANES), f32),
            pltpu.VMEM((1, depth), f32),
            pltpu.VMEM((1, depth), f32),
            pltpu.VMEM((1, depth), f32),
            pltpu.VMEM((count, LANES), bf16),
            pltpu.VMEM((count + 2 * WIN, LANES), bf16),
            pltpu.VMEM((n_sp * n_ctx, LANES), bf16),
            pltpu.VMEM((n_tp, count, LANES), bf16),
            pltpu.VMEM((n_tp, group, width), bf16),
            pltpu.VMEM((count // GRID_W, 4 * LANES), f32),
            pltpu.VMEM((GRID_W, 4 * LANES), f32),
            pltpu.VMEM((1, conditioning.shape[0]), bf16),
            pltpu.VMEM((1, depth), f32),
            pltpu.VMEM((1, sink.shape[0]), f32),
            pltpu.SemaphoreType.REGULAR,
            dma((16,)),
            dma((3,)),
            dma((3,)),
            dma((1,)),
            dma,
            dma,
            dma,
            dma((1,)),
            dma((SPAN,)),
            dma((n_sp // SPAN,)),
            dma((n_sp // SPAN,)),
            dma((2 * SPAN,)),
            dma((6,)),
            dma((6, chunks)),
            dma((n_tp,)),
            dma((n_tp,)),
            dma((4,)),
            dma((n_tp // 2,)),
            dma((2,)),
            dma((2,)),
            dma((3,)),
            dma((3, blocks)),
            dma((4,)),
            dma((4,)),
            dma((8,)),
            dma((8,)),
        ],
        compiler_params=pltpu.CompilerParams(
            collective_id=0, has_side_effects=True, vmem_limit_bytes=56 * 1024 * 1024
        ),
    )(
        latent,
        context,
        conditioning.reshape(1, -1),
        norm_gain.reshape(1, -1),
        shift_w,
        scale_w,
        gate_w,
        q_w,
        k_w.T,
        v_w.T,
        o_w,
        sink.reshape(1, -1),
        jnp.asarray(row_tab),
        jnp.asarray(col_tab),
    )
    return (latent.astype(f32) + gate * blended.astype(f32)).astype(bf16)


def solution(mesh):
    in_specs = (
        P(("grp", "sp", "tp"), None),
        P(("grp", "sp"), None),
        P(("grp", "sp")),
        P(),
        P("sp", "tp"),
        P("sp", "tp"),
        P("sp", "tp"),
        P(None, "tp"),
        P(None, "tp"),
        P(None, "tp"),
        P(None, "tp"),
        P("tp"),
    )
    return jax.shard_map(
        functools.partial(local, mesh.shape["sp"], mesh.shape["tp"]),
        mesh=mesh,
        in_specs=in_specs,
        out_specs=P(("grp", "sp", "tp"), None),
        check_vma=False,
    )
```
